32 devices in a mesh: sp: 8 (over z, y), tp: 4 (over x, core).
Axes of the slice: x: 2, y: 2, z: 4, core: 2. Of those that a mesh axis runs over, the one named last changes fastest.
Arguments:
- residual_entry_input: bfloat16 [8192, 2048], P(('sp', 'tp')), may hold values from -6 to 6
- query_matrix_rows: bfloat16 [8192, 1024], P('sp', 'tp'), may hold values from -6 to 6
- key_matrix_rows: bfloat16 [8192, 1024], P('sp', 'tp'), may hold values from -6 to 6
- value_matrix_rows: bfloat16 [8192, 2048], P('sp', 'tp'), may hold values from -6 to 6
- output_gate_logits: bfloat16 [8192, 2048], P('sp', 'tp'), may hold values from -6 to 6
- input_gate_logits: float32 [8192, 8], P('sp', 'tp'), may hold values from -6 to 6
- forget_gate_logits: float32 [8192, 8], P('sp', 'tp'), may hold values from -8 to 31
- forget_decay_offset: float32 [8192, 8], P('sp', 'tp'), may hold values from -0.7 to 0
- head_norm_gain: float32 [8, 256], P('tp'), may hold values from 0.1 to 1.9
- cell_output_weight: bfloat16 [2048, 2048], P('tp'), may hold values from -0.125 to 0.125
- feedforward_norm_gain: float32 [2048], replicated, may hold values from 0.1 to 1.9
- gate_up_weight: bfloat16 [2048, 5632], P('sp', 'tp'), may hold values from -0.125 to 0.125
- value_up_weight: bfloat16 [2048, 5632], P('sp', 'tp'), may hold values from -0.125 to 0.125
- gate_filter_taps: float32 [3, 5632], P(None, 'tp'), may hold values from -3 to 3
- value_filter_taps: float32 [3, 5632], P(None, 'tp'), may hold values from -3 to 3
- down_projection_weight: bfloat16 [5632, 2048], P('tp', 'sp'), may hold values from -0.078125 to 0.078125
Outputs:
- result: bfloat16 [8192, 2048], P(('sp', 'tp'))
The draws below stay inside these ranges and needn't reach their ends.
All inputs are finite; a program needn't handle non-finite values.
Results may differ from the reference program's by a relative error of at most 0.025.
Values may be sent and summed in bfloat16 or wider, within the bound.
A program may use at most 128 MiB of HBM per device.

```python
import math
import jax
import jax.numpy as jnp
from jax import lax

D = 2048
HEADS = 8
DK = 128
DV = 256
FF = 5632
BLOCK = 128
TOK_DEV = 1024
TOKENS = 8192
HV = 2048
FF_DEV = 1408
N_TP = 4


def draw_forget_gate_logits(key, part):
    key_order = jax.random.fold_in(key, 11)
    key_slow = jax.random.fold_in(key, 12)
    key_fast = jax.random.fold_in(key, 13)
    key_noise = jax.random.fold_in(key, 14)
    order = jax.random.permutation(key_order, HEADS)
    slow_heads = order < HEADS // 2
    slow_rate = math.log(10.0) / (6.0 * TOKENS) * jnp.exp(jax.random.uniform(key_slow, (HEADS,), jnp.float32, math.log(0.5), 0.0))
    fast_rate = 1.0 / 40.0 * jnp.exp(jax.random.uniform(key_fast, (HEADS,), jnp.float32, math.log(0.6), math.log(1.6)))
    head_rate = jnp.where(slow_heads, slow_rate, fast_rate)
    block_index = jnp.arange(TOKENS) // TOK_DEV
    device_factor = (1 + block_index % 2).astype(jnp.float32)
    noise = jnp.clip(jax.random.normal(key_noise, (TOKENS, HEADS), jnp.float32), -4.0, 4.0)
    rate = head_rate[None, :] * device_factor[:, None] * jnp.exp(0.7 * noise)
    capped = jnp.clip(-jnp.log(jnp.expm1(rate)), -6.0, 14.5)
    ratio = capped / 15.0
    return (7.5 * jnp.log((1.0 + ratio) / (1.0 - ratio))).astype(jnp.float32)


def draw_forget_decay_offset(key, part):
    key_where = jax.random.fold_in(key, 21)
    key_depth = jax.random.fold_in(key, 22)
    spots = jax.random.randint(key_where, (2,), 0, TOKENS)
    depth = jax.random.uniform(key_depth, (2, HEADS), jnp.float32, math.log(0.5), math.log(0.8))
    positions = jnp.arange(TOKENS)
    first = jnp.where((positions == spots[0])[:, None], depth[0][None, :], 0.0)
    second = jnp.where((positions == spots[1])[:, None], depth[1][None, :], 0.0)
    return (first + second).astype(jnp.float32)


def steps_of(rng, extent, split, low, top_value):
    def one(axis_at, blocks):
        draws = jax.random.uniform(jax.random.fold_in(jax.random.fold_in(rng, 6), axis_at), (blocks,), jnp.float32, low / len(split), top_value / len(split))
        return jnp.repeat(jnp.exp(draws), extent[axis_at] // blocks).reshape((-1,) + (1,) * (len(extent) - axis_at - 1))

    factor_of = one(*split[0])
    for cut in split[1:]:
        factor_of = factor_of * one(*cut)
    return factor_of


def normal_values(own_key, dims, width, most, cuts=(), kind=jnp.bfloat16):
    array = width * jax.random.normal(own_key, dims, jnp.float32)
    if cuts:
        array = array * steps_of(own_key, dims, cuts, -0.22, 0.18)
    return jnp.clip(array, -most, most).astype(kind)


def setup_inputs(seed: int = 0) -> dict:
    keys = jax.random.split(jax.random.key(seed), 17)
    return {
        "residual_entry_input": normal_values(keys[0], (TOKENS, D), 1.0, 6.0, ((0, 32),)),
        "query_matrix_rows": normal_values(keys[1], (TOKENS, HEADS * DK), 1.0, 6.0, ((0, 8), (1, 4))),
        "key_matrix_rows": normal_values(keys[2], (TOKENS, HEADS * DK), 1.0, 6.0, ((0, 8), (1, 4))),
        "value_matrix_rows": normal_values(keys[3], (TOKENS, HV), 1.0, 6.0, ((0, 8), (1, 4))),
        "output_gate_logits": normal_values(keys[4], (TOKENS, HV), 1.0, 6.0, ((0, 8), (1, 4))),
        "input_gate_logits": normal_values(keys[5], (TOKENS, HEADS), 1.0, 6.0, ((0, 8), (1, 4)), jnp.float32),
        "forget_gate_logits": draw_forget_gate_logits(jax.random.fold_in(keys[16], 71), 0),
        "forget_decay_offset": draw_forget_decay_offset(jax.random.fold_in(keys[16], 71), 0),
        "head_norm_gain": jnp.clip(1.0 + 0.18 * jax.random.normal(keys[8], (HEADS, DV), jnp.float32), 0.1, 1.9),
        "cell_output_weight": normal_values(keys[9], (HV, D), HV ** -0.5, 0.125, ((0, 4),)),
        "feedforward_norm_gain": jnp.clip(1.0 + 0.18 * jax.random.normal(keys[10], (D,), jnp.float32), 0.1, 1.9),
        "gate_up_weight": normal_values(keys[11], (D, FF), D ** -0.5, 0.125, ((0, 8), (1, 4))),
        "value_up_weight": normal_values(keys[12], (D, FF), D ** -0.5, 0.125, ((0, 8), (1, 4))),
        "gate_filter_taps": normal_values(keys[13], (3, FF), 0.577, 3.0, ((1, 4),), jnp.float32),
        "value_filter_taps": normal_values(keys[14], (3, FF), 0.577, 3.0, ((1, 4),), jnp.float32),
        "down_projection_weight": normal_values(keys[15], (FF, D), FF ** -0.5, 0.078125, ((0, 4), (1, 8))),
    }


eps = 1e-06

def gate_log_values(input_gate_logits, forget_gate_logits, forget_decay_offset):
    input_log_value = 15.0 * jnp.tanh(input_gate_logits / 15.0)
    forget_log_sigmoid = jax.nn.log_sigmoid(15.0 * jnp.tanh(forget_gate_logits / 15.0)) + forget_decay_offset
    return (input_log_value, forget_log_sigmoid)

def block_step(state_carry, inputs):
    memory, normer, running = state_carry
    query_block, key_block, value_block, input_block, forget_block = inputs
    length = query_block.shape[0]
    highest = lax.Precision.HIGHEST
    query_scale = DK ** (-0.5)
    query_wide = query_block.astype(jnp.float32)
    key_wide = key_block.astype(jnp.float32)
    value_wide = value_block.astype(jnp.float32)
    causal = jnp.tril(jnp.ones((length, length), dtype=bool))[:, :, None]
    cumulative = jnp.cumsum(forget_block, axis=0)
    logits = cumulative[:, None, :] - cumulative[None, :, :] + input_block[None, :, :]
    logits = jnp.where(causal, logits, -jnp.inf)
    carried = cumulative + running[None, :]
    stable = jnp.maximum(carried, lax.optimization_barrier(jnp.max(logits, axis=1)))
    carry_weight = jnp.exp(carried - stable)
    raw = jnp.einsum('thd,shd->tsh', query_wide, key_wide) * query_scale
    scores = raw * jnp.exp(logits - stable[:, None, :])
    scores_low = scores.astype(jnp.bfloat16).astype(jnp.float32)
    scaled_query = query_wide * query_scale
    numerator = carry_weight[:, :, None] * jnp.einsum('hvd,thd->thv', memory, scaled_query, precision=highest)
    numerator = numerator + jnp.einsum('tsh,shv->thv', scores_low, value_wide)
    denominator = carry_weight * jnp.einsum('hd,thd->th', normer, scaled_query, precision=highest) + lax.optimization_barrier(jnp.sum(scores, axis=1))
    output = numerator / jnp.maximum(jnp.abs(denominator), jnp.exp(-stable))[:, :, None]
    last_sum = cumulative[-1]
    weights_log = last_sum[None, :] - cumulative + input_block
    new_running = jnp.maximum(last_sum + running, lax.optimization_barrier(jnp.max(weights_log, axis=0)))
    decay_factor = jnp.exp(last_sum + running - new_running)
    weighted = key_wide * jnp.exp(weights_log - new_running[None, :])[:, :, None]
    weighted_low = weighted.astype(jnp.bfloat16).astype(jnp.float32)
    memory = decay_factor[:, None, None] * memory + jnp.einsum('shv,shd->hvd', value_wide, weighted_low)
    normer = decay_factor[:, None] * normer + lax.optimization_barrier(jnp.sum(weighted, axis=0))
    return ((memory, normer, new_running), output)

def reference(residual_entry_input, query_matrix_rows, key_matrix_rows, value_matrix_rows, output_gate_logits, input_gate_logits, forget_gate_logits, forget_decay_offset, head_norm_gain, cell_output_weight, feedforward_norm_gain, gate_up_weight, value_up_weight, gate_filter_taps, value_filter_taps, down_projection_weight):
    token_count = query_matrix_rows.shape[0]
    queries = query_matrix_rows.reshape(token_count, HEADS, DK)
    keys_all = key_matrix_rows.reshape(token_count, HEADS, DK)
    values_all = value_matrix_rows.reshape(token_count, HEADS, DV)
    input_log_value, forget_log_sigmoid = gate_log_values(input_gate_logits, forget_gate_logits, forget_decay_offset)
    block_count = token_count // BLOCK

    def blocks(tensor):
        return tensor.reshape((block_count, BLOCK) + tensor.shape[1:])
    initial = (jnp.zeros((HEADS, DV, DK), jnp.float32), jnp.zeros((HEADS, DK), jnp.float32), jnp.zeros((HEADS,), jnp.float32))
    _, outputs = lax.scan(block_step, initial, (blocks(queries), blocks(keys_all), blocks(values_all), blocks(input_log_value), blocks(forget_log_sigmoid)))
    memory_out = outputs.reshape(token_count, HEADS, DV)
    normed = memory_out * lax.rsqrt(lax.optimization_barrier(jnp.mean(memory_out * memory_out, axis=-1, keepdims=True)) + eps) * head_norm_gain[None, :, :]
    gated_rows = (normed.reshape(token_count, HEADS * DV) * jax.nn.sigmoid(output_gate_logits.astype(jnp.float32))).astype(jnp.bfloat16)
    mixed_rows = jnp.dot(gated_rows, cell_output_weight, preferred_element_type=jnp.float32)
    stream = (residual_entry_input.astype(jnp.float32) + mixed_rows).astype(jnp.bfloat16)
    stream_wide = lax.optimization_barrier(stream).astype(jnp.float32)
    normed_rows = (stream_wide * lax.rsqrt(lax.optimization_barrier(jnp.mean(stream_wide * stream_wide, axis=-1, keepdims=True)) + eps) * feedforward_norm_gain[None, :]).astype(jnp.bfloat16)
    padded = jnp.concatenate([jnp.zeros((2, D), jnp.bfloat16), normed_rows], axis=0)
    row_block = min(token_count, 4096)
    pieces = []
    for offset in range(0, token_count, row_block):
        window = padded[offset:offset + row_block + 2]
        up_gate = jnp.dot(window, gate_up_weight, preferred_element_type=jnp.float32)
        up_value = jnp.dot(window, value_up_weight, preferred_element_type=jnp.float32)
        conv_g = gate_filter_taps[0][None, :] * up_gate[:-2] + gate_filter_taps[1][None, :] * up_gate[1:-1] + gate_filter_taps[2][None, :] * up_gate[2:]
        conv_v = value_filter_taps[0][None, :] * up_value[:-2] + value_filter_taps[1][None, :] * up_value[1:-1] + value_filter_taps[2][None, :] * up_value[2:]
        hidden = (jax.nn.silu(conv_g) * conv_v).astype(jnp.bfloat16)
        running_sum = jnp.zeros((row_block, D), jnp.float32)
        for member in range(N_TP):
            lower = member * FF_DEV
            partial_value = jnp.dot(hidden[:, lower:lower + FF_DEV], down_projection_weight[lower:lower + FF_DEV], preferred_element_type=jnp.float32).astype(jnp.bfloat16)
            running_sum = running_sum + lax.optimization_barrier(partial_value).astype(jnp.float32)
        pieces.append((stream_wide[offset:offset + row_block] + running_sum).astype(jnp.bfloat16))
    return jnp.concatenate(pieces, axis=0)
```

```python
import functools

import jax
import jax.numpy as jnp
from jax import lax
from jax.experimental import pallas as pl
from jax.experimental.pallas import tpu as pltpu
from jax.sharding import PartitionSpec as P

BLOCK = 128


eps = 1e-06
neg_large = -1e30


def shifted(x, axis, by):
    count = lax.axis_size(axis)
    pairs = [(i, i + by) for i in range(count) if 0 <= i + by < count]
    return lax.ppermute(x, axis, pairs)


def gate_log_values(input_gate_logits, forget_gate_logits, forget_decay_offset):
    input_log_value = 15.0 * jnp.tanh(input_gate_logits / 15.0)
    forget_log_sigmoid = (
        jax.nn.log_sigmoid(15.0 * jnp.tanh(forget_gate_logits / 15.0)) + forget_decay_offset
    )
    return (input_log_value, forget_log_sigmoid)


STATE_PAD = 16
MESH = pl.DeviceIdType.MESH


def cell_kernel(
    count,
    heads,
    state_ref,
    q_ref,
    k_ref,
    v_ref,
    gate_ref,
    gain_ref,
    rows_ref,
    cols_ref,
    out_ref,
    held,
    memory,
    normer,
    running,
    send_sem,
    recv_sem,
):
    me = lax.axis_index("sp")
    barrier = pltpu.get_barrier_semaphore()
    for d in range(1, count):
        pl.semaphore_signal(
            barrier, inc=1, device_id={"sp": lax.rem(me + d, count)}, device_id_type=MESH
        )
    pl.semaphore_wait(barrier, count - 1)

    def push(d, target, slot):
        return pltpu.make_async_remote_copy(
            src_ref=state_ref,
            dst_ref=held.at[slot],
            send_sem=send_sem.at[d],
            recv_sem=recv_sem.at[d],
            device_id={"sp": target},
            device_id_type=MESH,
        )

    for d in range(1, count):

        @pl.when(me + d < count)
        def _():
            push(d, me + d, me).start()

    memory[...] = jnp.zeros_like(memory)
    normer[...] = jnp.zeros_like(normer)
    running[...] = jnp.full(running.shape, neg_large, jnp.float32)
    for d in range(1, count):

        @pl.when(me - d >= 0)
        def _():
            push(d, lax.rem(me + d, count), me - d).wait_recv()

    key_width = memory.shape[1]
    value_width = memory.shape[2]
    span = key_width + STATE_PAD

    @pl.loop(0, me)
    def _(j):
        for h in range(heads):
            low = h * span
            extra = held[j, low + key_width : low + span, :].astype(jnp.float32)
            total = extra[2:3, :1] + extra[3:4, :1]
            level = extra[4:5, :1] + extra[5:6, :1]
            before = running[h, :1, :1]
            after = jnp.maximum(total + before, level)
            one = jnp.exp(total + before - after)
            two = jnp.exp(level - after)
            memory[h] = one * memory[h] + two * held[j, low : low + key_width, :].astype(
                jnp.float32
            )
            parts = extra[0:1, :key_width] + extra[1:2, :key_width]
            normer[h, :1, :] = one * normer[h, :1, :] + two * parts
            running[h] = jnp.broadcast_to(after, running.shape[1:])

    length = BLOCK
    scale = key_width ** (-0.5)
    at_row = lax.broadcasted_iota(jnp.int32, (length, length), 0)
    at_col = lax.broadcasted_iota(jnp.int32, (length, length), 1)
    causal = at_col <= at_row

    @pl.loop(0, q_ref.shape[0] // length)
    def _(j):
        rows = pl.ds(pl.multiple_of(j * length, length), length)
        lanes = rows_ref[j]
        cols = cols_ref[rows, :]
        for h in range(heads):
            keys = slice(h * key_width, (h + 1) * key_width)
            vals = slice(h * value_width, (h + 1) * value_width)
            q = q_ref[rows, keys]
            k = k_ref[rows, keys]
            v = v_ref[rows, vals]
            before = running[h, :1, :1]
            total = lanes[heads + h : heads + h + 1, :1]
            shifted_log = jnp.where(causal, lanes[h : h + 1, :], -jnp.inf)
            top = jnp.maximum(jnp.max(shifted_log, axis=1, keepdims=True), before)
            raw = (
                lax.dot_general(
                    q, k, (((1,), (1,)), ((), ())), preferred_element_type=jnp.float32
                )
                * scale
            )
            scores = raw * jnp.exp(shifted_log - top)
            carry = jnp.exp(before - top) * scale
            state = memory[h]
            high = state.astype(jnp.bfloat16)
            low = (state - high.astype(jnp.float32)).astype(jnp.bfloat16)
            carried = jnp.dot(q, high, preferred_element_type=jnp.float32) + jnp.dot(
                q, low, preferred_element_type=jnp.float32
            )
            numerator = carry * carried + jnp.dot(
                scores.astype(jnp.bfloat16), v, preferred_element_type=jnp.float32
            )
            denominator = carry * jnp.sum(
                q.astype(jnp.float32) * normer[h, :1, :], axis=1, keepdims=True
            ) + jnp.sum(scores, axis=1, keepdims=True)
            level = cols[:, h : h + 1] + top
            value = numerator / jnp.maximum(jnp.abs(denominator), jnp.exp(-level))
            mean = jnp.mean(value * value, axis=1, keepdims=True)
            normed = value * lax.rsqrt(mean + eps) * gain_ref[h : h + 1, :]
            gated = normed * jax.nn.sigmoid(gate_ref[rows, vals].astype(jnp.float32))
            out_ref[rows, vals] = gated.astype(out_ref.dtype)
            last = jnp.max(jnp.maximum(lanes[h : h + 1, :], before), axis=1, keepdims=True)
            decay = jnp.exp(before - last)
            weighted = k.astype(jnp.float32) * jnp.exp(cols[:, heads + h : heads + h + 1] - last)
            memory[h] = decay * state + lax.dot_general(
                weighted.astype(jnp.bfloat16),
                v,
                (((0,), (0,)), ((), ())),
                preferred_element_type=jnp.float32,
            )
            normer[h, :1, :] = decay * normer[h, :1, :] + jnp.sum(
                weighted, axis=0, keepdims=True
            )
            running[h] = jnp.broadcast_to(last + total, running.shape[1:])

    for d in range(1, count):

        @pl.when(me + d < count)
        def _():
            push(d, me + d, me).wait_send()


def halves(x):
    high = lax.reduce_precision(x, 8, 7)
    return (high.astype(jnp.bfloat16), (x - high).astype(jnp.bfloat16))


def cell_parts(q, k, v, input_log, forget_log):
    heads = input_log.shape[1]
    tokens = q.shape[0]
    key_width = q.shape[1] // heads
    value_width = v.shape[1] // heads
    count = lax.axis_size("sp")
    blocks = tokens // BLOCK
    f = forget_log.reshape(blocks, BLOCK, heads)
    tri = jnp.tril(jnp.ones((BLOCK, BLOCK), jnp.float32))
    within = jnp.einsum("ts,bsh->bth", tri, f, precision=lax.Precision.HIGHEST)
    each = within[:, -1, :]
    later = jnp.triu(jnp.ones((blocks, blocks), jnp.float32), 1)
    after = jnp.einsum("bc,ch->bh", later, each, precision=lax.Precision.HIGHEST)
    total = jnp.sum(each, axis=0)
    shifted_log = input_log.reshape(blocks, BLOCK, heads) - within
    to_end = (shifted_log + (each + after)[:, None, :]).reshape(tokens, heads)
    level = jnp.max(to_end, axis=0)
    weighted = k.reshape(tokens, heads, key_width).astype(jnp.float32) * jnp.exp(to_end - level)[
        :, :, None
    ]
    memory = jnp.einsum(
        "shd,shv->hdv",
        weighted.astype(jnp.bfloat16),
        v.reshape(tokens, heads, value_width),
        preferred_element_type=jnp.float32,
    ).astype(jnp.bfloat16)
    normer = jnp.sum(weighted, axis=0)
    wide = (heads, 1, value_width)
    lines = [
        jnp.pad(part, ((0, 0), (0, value_width - key_width)))[:, None, :]
        for part in halves(normer)
    ]
    for scalar in (total, level):
        lines += [jnp.broadcast_to(part[:, None, None], wide) for part in halves(scalar)]
    lines.append(jnp.zeros((heads, STATE_PAD - len(lines), value_width), jnp.bfloat16))
    span = key_width + STATE_PAD
    state = jnp.concatenate([memory] + lines, axis=1).reshape(heads * span, value_width)
    lanes = jnp.concatenate(
        [
            jnp.transpose(shifted_log, (0, 2, 1)),
            jnp.broadcast_to(each[:, :, None], (blocks, heads, BLOCK)),
        ],
        axis=1,
    )
    cols = jnp.concatenate([within, shifted_log], axis=2).reshape(tokens, 2 * heads)
    return state, lanes, cols


def cell(q, k, v, gates, input_log, forget_log, gain):
    heads = input_log.shape[1]
    key_width = q.shape[1] // heads
    value_width = v.shape[1] // heads
    count = lax.axis_size("sp")
    span = key_width + STATE_PAD
    state, lanes, cols = cell_parts(q, k, v, input_log, forget_log)
    vmem = pl.BlockSpec(memory_space=pltpu.VMEM)
    return pl.pallas_call(
        functools.partial(cell_kernel, count, heads),
        out_shape=jax.ShapeDtypeStruct(v.shape, jnp.bfloat16),
        in_specs=[vmem] * 8,
        out_specs=vmem,
        scratch_shapes=[
            pltpu.VMEM((count, heads * span, value_width), jnp.bfloat16),
            pltpu.VMEM((heads, key_width, value_width), jnp.float32),
            pltpu.VMEM((heads, 8, key_width), jnp.float32),
            pltpu.VMEM((heads, 8, 128), jnp.float32),
            pltpu.SemaphoreType.DMA((count,)),
            pltpu.SemaphoreType.DMA((count,)),
        ],
        compiler_params=pltpu.CompilerParams(
            collective_id=0, has_side_effects=True, vmem_limit_bytes=40 * 1024 * 1024
        ),
        cost_estimate=pl.CostEstimate(
            flops=30_000_000_000, bytes_accessed=8 * v.size, transcendentals=0
        ),
    )(state, q, k, v, gates, gain, lanes, cols)


def rows_kernel(pieces, x_ref, out_ref, own_sem, near_send, near_recv, far_send, far_recv, on_send, on_recv):
    me = lax.axis_index("tp")
    near = me + 1 - 2 * lax.rem(me, 2)
    far = lax.rem(me + 2, 4)
    opposite = lax.rem(near + 2, 4)
    size = x_ref.shape[0]
    step = size // pieces
    barrier = pltpu.get_barrier_semaphore()
    for other in (near, far):
        pl.semaphore_signal(barrier, inc=1, device_id={"tp": other}, device_id_type=MESH)
    pl.semaphore_wait(barrier, 2)

    def at(owner, p):
        return out_ref.at[pl.ds(pl.multiple_of(owner * size + p * step, step), step)]

    def send(src, dst, sems, p, target):
        return pltpu.make_async_remote_copy(
            src_ref=src,
            dst_ref=dst,
            send_sem=sems[0].at[p],
            recv_sem=sems[1].at[p],
            device_id={"tp": target},
            device_id_type=MESH,
        )

    mine = [x_ref.at[pl.ds(p * step, step)] for p in range(pieces)]
    far_out = [send(mine[p], at(me, p), (far_send, far_recv), p, far) for p in range(pieces)]
    near_out = [send(mine[p], at(me, p), (near_send, near_recv), p, near) for p in range(pieces)]
    far_in = [send(mine[p], at(far, p), (far_send, far_recv), p, far) for p in range(pieces)]
    near_in = [send(mine[p], at(near, p), (near_send, near_recv), p, near) for p in range(pieces)]
    onward = [send(at(far, p), at(far, p), (on_send, on_recv), p, near) for p in range(pieces)]
    on_in = [
        send(at(opposite, p), at(opposite, p), (on_send, on_recv), p, near)
        for p in range(pieces)
    ]
    for p in range(pieces):
        far_out[p].start()
    for p in range(pieces):
        near_out[p].start()
    whole = pl.ds(pl.multiple_of(me * size, size), size)
    own = pltpu.make_async_copy(x_ref, out_ref.at[whole], own_sem)
    own.start()
    for p in range(pieces):
        far_in[p].wait_recv()
        onward[p].start()
    own.wait()
    for p in range(pieces):
        near_in[p].wait_recv()
        on_in[p].wait_recv()
    for p in range(pieces):
        far_out[p].wait_send()
        near_out[p].wait_send()
        onward[p].wait_send()


def gather_rows(x):
    if lax.axis_size("tp") != 4:
        return lax.all_gather(x, "tp", axis=0, tiled=True)
    pieces = 4
    vmem = pl.BlockSpec(memory_space=pltpu.VMEM)
    return pl.pallas_call(
        functools.partial(rows_kernel, pieces),
        out_shape=jax.ShapeDtypeStruct((4 * x.shape[0], x.shape[1]), x.dtype),
        in_specs=[vmem],
        out_specs=vmem,
        scratch_shapes=[pltpu.SemaphoreType.DMA] + [pltpu.SemaphoreType.DMA((pieces,))] * 6,
        compiler_params=pltpu.CompilerParams(
            collective_id=1, has_side_effects=True, vmem_limit_bytes=16 * 1024 * 1024
        ),
        cost_estimate=pl.CostEstimate(
            flops=30_000_000_000, bytes_accessed=4 * x.size, transcendentals=0
        ),
    )(x)


def product_kernel(
    pieces,
    x_ref,
    w_ref,
    out_ref,
    pair_out,
    pair_in,
    far_out,
    far_in,
    near_out,
    near_in,
    pair_send,
    pair_recv,
    far_send,
    far_recv,
    near_send,
    near_recv,
):
    me = lax.axis_index("tp")
    near = me + 1 - 2 * lax.rem(me, 2)
    far = lax.rem(me + 2, 4)
    opposite = lax.rem(near + 2, 4)
    size = out_ref.shape[0]
    step = out_ref.shape[1] // pieces
    barrier = pltpu.get_barrier_semaphore()
    for other in (near, far):
        pl.semaphore_signal(barrier, inc=1, device_id={"tp": other}, device_id_type=MESH)
    pl.semaphore_wait(barrier, 2)

    def columns(p):
        return pl.ds(pl.multiple_of(p * step, step), step)

    def term(owner, p):
        rows = pl.ds(pl.multiple_of(owner * size, size), size)
        return jnp.dot(x_ref[rows, :], w_ref[:, columns(p)], preferred_element_type=jnp.float32)

    def send(src, dst, sems, p, target):
        return pltpu.make_async_remote_copy(
            src_ref=src.at[p],
            dst_ref=dst.at[p],
            send_sem=sems[0].at[p],
            recv_sem=sems[1].at[p],
            device_id={"tp": target},
            device_id_type=MESH,
        )

    def pair(p):
        return send(pair_out, pair_in, (pair_send, pair_recv), p, near)

    def across(p):
        return send(far_out, far_in, (far_send, far_recv), p, far)

    def beside(p):
        return send(near_out, near_in, (near_send, near_recv), p, near)

    @pl.loop(0, pieces)
    def _(p):
        pair_out[p] = term(opposite, p).astype(jnp.bfloat16)
        pair(p).start()
        mine = term(far, p)
        pair(p).wait_recv()
        far_out[p] = (mine + pair_in[p].astype(jnp.float32)).astype(jnp.bfloat16)
        across(p).start()

    @pl.loop(0, pieces)
    def _(p):
        near_out[p] = term(near, p).astype(jnp.bfloat16)
        beside(p).start()

    @pl.loop(0, pieces)
    def _(p):
        own = term(me, p)
        beside(p).wait_recv()
        out_ref[:, columns(p)] = own + near_in[p].astype(jnp.float32)

    @pl.loop(0, pieces)
    def _(p):
        across(p).wait_recv()
        out_ref[:, columns(p)] += far_in[p].astype(jnp.float32)

    @pl.loop(0, pieces)
    def _(p):
        pair(p).wait_send()
        across(p).wait_send()
        beside(p).wait_send()


def product_rows(x, w, tag):
    if lax.axis_size("tp") != 4:
        partial = jnp.dot(x, w, preferred_element_type=jnp.float32).astype(jnp.bfloat16)
        return lax.psum_scatter(partial, "tp", scatter_dimension=0, tiled=True).astype(
            jnp.float32
        )
    pieces = 4
    rows, wide = x.shape[0] // 4, w.shape[1]
    vmem = pl.BlockSpec(memory_space=pltpu.VMEM)
    slots = pltpu.VMEM((pieces, rows, wide // pieces), jnp.bfloat16)
    return pl.pallas_call(
        functools.partial(product_kernel, pieces),
        out_shape=jax.ShapeDtypeStruct((rows, wide), jnp.float32),
        in_specs=[vmem] * 2,
        out_specs=vmem,
        scratch_shapes=[slots] * 6 + [pltpu.SemaphoreType.DMA((pieces,))] * 6,
        compiler_params=pltpu.CompilerParams(
            collective_id=tag, has_side_effects=True, vmem_limit_bytes=40 * 1024 * 1024
        ),
        cost_estimate=pl.CostEstimate(
            flops=30_000_000_000, bytes_accessed=2 * w.size, transcendentals=0
        ),
    )(x, w)


def walk_kernel(count, pieces, x_ref, out_ref, own_sem, send_sem, recv_sem):
    me = lax.axis_index("sp")
    odd = lax.rem(me, 2)
    place = me // 2 + odd * (count - 1 - 2 * (me // 2))
    size = x_ref.shape[0]
    step = size // (2 * pieces)

    def index(position):
        position = lax.rem(position + 2 * count, count)
        back = position // (count // 2)
        return (1 - back) * 2 * position + back * (2 * (count - 1 - position) + 1)

    ways = (1, -1)
    barrier = pltpu.get_barrier_semaphore()
    for way in ways:
        pl.semaphore_signal(
            barrier, inc=1, device_id={"sp": index(place + way)}, device_id_type=MESH
        )
    pl.semaphore_wait(barrier, 2)

    def hop(w, t, p, age, own=False):
        inner = (w * pieces + p) * step
        owner = index(place - ways[w] * age)
        dst = out_ref.at[pl.ds(pl.multiple_of(owner * size + inner, step), step)]
        return pltpu.make_async_remote_copy(
            src_ref=x_ref.at[pl.ds(inner, step)] if own else dst,
            dst_ref=dst,
            send_sem=send_sem.at[w, p, t],
            recv_sem=recv_sem.at[w, p, t],
            device_id={"sp": index(place + ways[w])},
            device_id_type=MESH,
        )

    for p in range(pieces):
        for w in range(2):
            hop(w, 0, p, 0, True).start()
    whole = pl.ds(pl.multiple_of(me * size, size), size)
    own = pltpu.make_async_copy(x_ref, out_ref.at[whole], own_sem)
    own.start()

    @pl.loop(1, count - 1)
    def _(t):
        for p in range(pieces):
            for w in range(2):
                hop(w, t - 1, p, t).wait_recv()
                hop(w, t, p, t).start()

    own.wait()
    for p in range(pieces):
        for w in range(2):
            hop(w, count - 2, p, count - 1).wait_recv()
            hop(w, 0, p, 0, True).wait_send()

    @pl.loop(1, count - 1)
    def _(t):
        for p in range(pieces):
            for w in range(2):
                hop(w, t, p, t).wait_send()


def walk_gather(x, pieces):
    count = lax.axis_size("sp")
    if count % 2 or count < 4 or x.shape[0] % (32 * pieces):
        return lax.all_gather(x, "sp", axis=0, tiled=True)
    vmem = pl.BlockSpec(memory_space=pltpu.VMEM)
    return pl.pallas_call(
        functools.partial(walk_kernel, count, pieces),
        out_shape=jax.ShapeDtypeStruct((count * x.shape[0], x.shape[1]), x.dtype),
        in_specs=[vmem],
        out_specs=vmem,
        scratch_shapes=[pltpu.SemaphoreType.DMA]
        + [pltpu.SemaphoreType.DMA((2, pieces, count - 1))] * 2,
        compiler_params=pltpu.CompilerParams(
            collective_id=4, has_side_effects=True, vmem_limit_bytes=16 * 1024 * 1024
        ),
        cost_estimate=pl.CostEstimate(
            flops=30_000_000_000, bytes_accessed=count * x.size, transcendentals=0
        ),
    )(x)


def layer_kernel(
    count,
    heads,
    up_pieces,
    down_pieces,
    logs_ref,
    q_ref,
    k_ref,
    v_ref,
    gate_ref,
    gain_ref,
    wo_ref,
    residual_ref,
    norm_gain_ref,
    gate_taps_ref,
    value_taps_ref,
    gate_w_ref,
    value_w_ref,
    down_w_ref,
    out_ref,
    rows_ref,
    cols_ref,
    state_ref,
    held,
    memory,
    normer,
    running,
    pair_memory,
    pair_normer,
    pair_level,
    handed,
    gated,
    pair_out,
    pair_in,
    far_out,
    far_in,
    near_out,
    near_in,
    total_rows,
    stream,
    group,
    full_up,
    full_down,
    up_tile,
    hidden,
    load_sem,
    state_send,
    state_recv,
    up_send,
    up_recv,
    down_send,
    down_recv,
    first_sem,
    second_sem,
    rows_sem,
    edge_sem,
):
    me = lax.axis_index("sp")
    tp = lax.axis_index("tp")
    near = tp + 1 - 2 * lax.rem(tp, 2)
    far = lax.rem(tp + 2, 4)
    opposite = lax.rem(near + 2, 4)
    odd = lax.rem(me, 2)
    half = count // 2
    place = me // 2 + odd * (count - 1 - 2 * (me // 2))
    tiles = full_up.shape[0]
    up_rows = full_up.shape[1] // count
    up_step = up_rows // (2 * up_pieces)
    down_step = full_down.shape[1] // (2 * down_pieces)
    lane = full_up.shape[2] // 2

    barrier = pltpu.get_barrier_semaphore()
    for d in range(1, count):
        pl.semaphore_signal(
            barrier, inc=1, device_id={"sp": lax.rem(me + d, count)}, device_id_type=MESH
        )
    for other in (near, far):
        pl.semaphore_signal(barrier, inc=1, device_id={"tp": other}, device_id_type=MESH)

    own_up = pl.ds(pl.multiple_of(me * up_rows, up_rows), up_rows)
    loads = []
    for i in range(tiles):
        for a, w_ref in enumerate((gate_w_ref, value_w_ref)):
            loads.append(
                pltpu.make_async_copy(
                    w_ref.at[:, pl.ds(i * lane, lane)],
                    full_up.at[i, own_up, pl.ds(a * lane, lane)],
                    load_sem.at[2 * i + a],
                )
            )
    down_load = pltpu.make_async_copy(down_w_ref, full_down.at[me], load_sem.at[2 * tiles])
    for load in loads:
        load.start()
    down_load.start()

    pl.semaphore_wait(barrier, count + 1)

    step_at = me // 2
    swap = pltpu.make_async_remote_copy(
        src_ref=state_ref,
        dst_ref=held.at[0],
        send_sem=state_send.at[0],
        recv_sem=state_recv.at[0],
        device_id={"sp": me + 1 - 2 * odd},
        device_id_type=MESH,
    )
    hand = pltpu.make_async_remote_copy(
        src_ref=handed,
        dst_ref=held.at[1],
        send_sem=state_send.at[1],
        recv_sem=state_recv.at[1],
        device_id={"sp": lax.rem(me + 2, count)},
        device_id_type=MESH,
    )
    def index(position):
        position = lax.rem(position + 2 * count, count)
        back = position // half
        return (1 - back) * 2 * position + back * (2 * (count - 1 - position) + 1)

    ways = (1, -1)

    def up_hop(w, t, m):
        owner = index(place - ways[w] * t)
        row = owner * up_rows + (w * up_pieces + m) * up_step
        part = full_up.at[:, pl.ds(pl.multiple_of(row, up_step), up_step), :]
        return pltpu.make_async_remote_copy(
            src_ref=part,
            dst_ref=part,
            send_sem=up_send.at[w, m, t],
            recv_sem=up_recv.at[w, m, t],
            device_id={"sp": index(place + ways[w])},
            device_id_type=MESH,
        )

    def down_hop(w, t, m):
        owner = index(place - ways[w] * t)
        row = (w * down_pieces + m) * down_step
        part = full_down.at[owner, pl.ds(pl.multiple_of(row, down_step), down_step), :]
        return pltpu.make_async_remote_copy(
            src_ref=part,
            dst_ref=part,
            send_sem=down_send.at[w, m, t],
            recv_sem=down_recv.at[w, m, t],
            device_id={"sp": index(place + ways[w])},
            device_id_type=MESH,
        )

    up_ticks = (count - 1) * up_pieces
    all_ticks = up_ticks + (count - 1) * down_pieces

    def move(hop, pieces, n):
        t = n // pieces
        m = lax.rem(n, pieces)
        for w in range(2):

            @pl.when(t > 0)
            def _():
                hop(w, t - 1, m).wait_recv()

            hop(w, t, m).start()

    def up_tick(n):
        move(up_hop, up_pieces, n)

    def tick(n):
        @pl.when(n < up_ticks)
        def _():
            up_tick(n)

        @pl.when((n >= up_ticks) & (n < all_ticks))
        def _():
            move(down_hop, down_pieces, n - up_ticks)

    def up_sent(n):
        for w in range(2):
            up_hop(w, n // up_pieces, lax.rem(n, up_pieces)).wait_send()

    for load in loads:
        load.wait()
    down_load.wait()
    for n in range(2):
        up_tick(n)

    key_width = memory.shape[1]
    value_width = memory.shape[2]
    span = key_width + STATE_PAD

    def read_state(ref, h):
        low = h * span
        extra = ref[low + key_width : low + span, :].astype(jnp.float32)
        total = extra[2:3, :1] + extra[3:4, :1]
        level = extra[4:5, :1] + extra[5:6, :1]
        parts = extra[0:1, :key_width] + extra[1:2, :key_width]
        return ref[low : low + key_width, :].astype(jnp.float32), parts, level, total

    def join(first, second, total):
        mem_a, norm_a, level_a = first
        mem_b, norm_b, level_b = second
        after = jnp.maximum(total + level_a, level_b)
        one = jnp.exp(total + level_a - after)
        two = jnp.exp(level_b - after)
        return one * mem_a + two * mem_b, one * norm_a + two * norm_b, after

    def keep(refs, h, values):
        mem, norm, level = values
        refs[0][h] = mem
        refs[1][h, :1, :] = norm
        refs[2][h] = jnp.broadcast_to(level, refs[2].shape[1:])

    carried_refs = (memory, normer, running)

    def write_state(ref, h, mem, norm, level, total):
        low = h * span
        ref[low : low + key_width, :] = mem.astype(jnp.bfloat16)
        lines = jnp.zeros((STATE_PAD, value_width), jnp.float32)
        at_line = lax.broadcasted_iota(jnp.int32, lines.shape, 0)
        norm = jnp.concatenate([norm] * (value_width // key_width), axis=1)
        for i, part in enumerate((norm, total, level)):
            high = part.astype(jnp.bfloat16).astype(jnp.float32)
            lines = jnp.where(at_line == 2 * i, high, lines)
            lines = jnp.where(at_line == 2 * i + 1, part - high, lines)
        ref[low + key_width : low + span, :] = lines.astype(jnp.bfloat16)

    length = BLOCK
    blocks = q_ref.shape[0] // length
    at_row = lax.broadcasted_iota(jnp.int32, (length, length), 0)
    at_col = lax.broadcasted_iota(jnp.int32, (length, length), 1)

    def by_block(first):
        return jnp.concatenate(
            [
                logs_ref[first : first + heads, b * length : (b + 1) * length]
                for b in range(blocks)
            ],
            axis=0,
        )

    within = jnp.dot(
        by_block(heads),
        jnp.where(at_row <= at_col, 1.0, 0.0),
        precision=lax.Precision.HIGHEST,
        preferred_element_type=jnp.float32,
    )
    shifted_all = by_block(0) - within
    each_all = within[:, length - 1 : length]
    after = jnp.zeros((heads, 1), jnp.float32)
    to_end = [None] * blocks
    for b in reversed(range(blocks)):
        part = slice(b * heads, (b + 1) * heads)
        after = after + each_all[part]
        to_end[b] = shifted_all[part] + after
    own_total = after
    own_level = functools.reduce(jnp.maximum, to_end)
    own_level = jnp.max(own_level, axis=1, keepdims=True)
    for b in range(blocks):
        part = slice(b * heads, (b + 1) * heads)
        rows_ref[b, 0 : 2 * heads, :] = jnp.concatenate(
            [shifted_all[part], jnp.broadcast_to(each_all[part], (heads, length))], axis=0
        )
        lines = [within[part], shifted_all[part], jnp.exp(to_end[b] - own_level)]
        lines.append(jnp.zeros((length - 3 * heads, length), jnp.float32))
        cols_ref[b * length : (b + 1) * length, :] = jnp.transpose(
            jnp.concatenate(lines, axis=0)
        )

    memory[...] = jnp.zeros_like(memory)
    normer[...] = jnp.zeros_like(normer)

    @pl.loop(0, blocks)
    def _(j):
        rows = pl.ds(pl.multiple_of(j * length, length), length)
        cols = cols_ref[rows, :]
        for h in range(heads):
            k = k_ref[rows, h * key_width : (h + 1) * key_width]
            v = v_ref[rows, h * value_width : (h + 1) * value_width]
            weighted = k.astype(jnp.float32) * cols[:, 2 * heads + h : 2 * heads + h + 1]
            memory[h] += lax.dot_general(
                weighted.astype(jnp.bfloat16),
                v,
                (((0,), (0,)), ((), ())),
                preferred_element_type=jnp.float32,
            )
            normer[h, :1, :] += jnp.sum(weighted, axis=0, keepdims=True)

    for h in range(heads):
        write_state(
            state_ref,
            h,
            memory[h],
            normer[h, :1, :],
            own_level[h : h + 1, :],
            own_total[h : h + 1, :],
        )
    swap.start()
    swap.wait_recv()

    @pl.when(odd == 0)
    def _():
        for h in range(heads):
            mem_a, norm_a, level_a, total_a = read_state(state_ref, h)
            mem_b, norm_b, level_b, total_b = read_state(held.at[0], h)
            out = join((mem_a, norm_a, level_a), (mem_b, norm_b, level_b), total_b)
            keep((pair_memory, pair_normer, pair_level.at[0]), h, out)
            pair_level[1, h] = jnp.broadcast_to(total_a + total_b, pair_level.shape[2:])

    @pl.when(odd == 1)
    def _():
        for h in range(heads):
            mem_a, norm_a, level_a, total_a = read_state(held.at[0], h)
            mem_b, norm_b, level_b, total_b = read_state(state_ref, h)
            out = join((mem_a, norm_a, level_a), (mem_b, norm_b, level_b), total_b)
            keep((pair_memory, pair_normer, pair_level.at[0]), h, out)
            pair_level[1, h] = jnp.broadcast_to(total_a + total_b, pair_level.shape[2:])

    started = jnp.minimum(FIRST_TICKS + NEXT_TICKS * step_at, up_ticks)

    @pl.loop(2, started)
    def _(n):
        up_sent(n - 2)
        up_tick(n)

    memory[...] = jnp.zeros_like(memory)
    normer[...] = jnp.zeros_like(normer)
    running[...] = jnp.full(running.shape, neg_large, jnp.float32)

    @pl.when(step_at > 0)
    def _():
        hand.wait_recv()
        for h in range(heads):
            mem, parts, level, total = read_state(held.at[1], h)
            keep(carried_refs, h, (mem, parts, level))

    @pl.when(step_at + 1 < half)
    def _():
        for h in range(heads):
            mem, norm, level = join(
                (memory[h], normer[h, :1, :], running[h, :1, :1]),
                (pair_memory[h], pair_normer[h, :1, :], pair_level[0, h, :1, :1]),
                pair_level[1, h, :1, :1],
            )
            write_state(handed, h, mem, norm, level, jnp.zeros_like(level))
        hand.start()

    @pl.when(odd == 1)
    def _():
        for h in range(heads):
            mem, norm, level, total = read_state(held.at[0], h)
            out = join(
                (memory[h], normer[h, :1, :], running[h, :1, :1]), (mem, norm, level), total
            )
            keep(carried_refs, h, out)

    scale = key_width ** (-0.5)
    causal = at_col <= at_row

    @pl.loop(0, blocks)
    def _(j):
        tick(started + j)
        rows = pl.ds(pl.multiple_of(j * length, length), length)
        lanes = rows_ref[j]
        cols = cols_ref[rows, :]
        for h in range(heads):
            keys = slice(h * key_width, (h + 1) * key_width)
            vals = slice(h * value_width, (h + 1) * value_width)
            q = q_ref[rows, keys]
            k = k_ref[rows, keys]
            v = v_ref[rows, vals]
            before = running[h, :1, :1]
            total = lanes[heads + h : heads + h + 1, :1]
            shifted_log = jnp.where(causal, lanes[h : h + 1, :], -jnp.inf)
            top = jnp.maximum(jnp.max(shifted_log, axis=1, keepdims=True), before)
            raw = (
                lax.dot_general(
                    q, k, (((1,), (1,)), ((), ())), preferred_element_type=jnp.float32
                )
                * scale
            )
            scores = raw * jnp.exp(shifted_log - top)
            carry = jnp.exp(before - top) * scale
            state = memory[h]
            high = state.astype(jnp.bfloat16)
            low = (state - high.astype(jnp.float32)).astype(jnp.bfloat16)
            carried = jnp.dot(q, high, preferred_element_type=jnp.float32) + jnp.dot(
                q, low, preferred_element_type=jnp.float32
            )
            numerator = carry * carried + jnp.dot(
                scores.astype(jnp.bfloat16), v, preferred_element_type=jnp.float32
            )
            denominator = carry * jnp.sum(
                q.astype(jnp.float32) * normer[h, :1, :], axis=1, keepdims=True
            ) + jnp.sum(scores, axis=1, keepdims=True)
            level = cols[:, h : h + 1] + top
            value = numerator / jnp.maximum(jnp.abs(denominator), jnp.exp(-level))
            mean = jnp.mean(value * value, axis=1, keepdims=True)
            normed = value * lax.rsqrt(mean + eps) * gain_ref[h : h + 1, :]
            gate = normed * jax.nn.sigmoid(gate_ref[rows, vals].astype(jnp.float32))
            gated[rows, vals] = gate.astype(gated.dtype)
            last = jnp.max(jnp.maximum(lanes[h : h + 1, :], before), axis=1, keepdims=True)
            decay = jnp.exp(before - last)
            weighted = k.astype(jnp.float32) * jnp.exp(cols[:, heads + h : heads + h + 1] - last)
            memory[h] = decay * state + lax.dot_general(
                weighted.astype(jnp.bfloat16),
                v,
                (((0,), (0,)), ((), ())),
                preferred_element_type=jnp.float32,
            )
            normer[h, :1, :] = decay * normer[h, :1, :] + jnp.sum(
                weighted, axis=0, keepdims=True
            )
            running[h] = jnp.broadcast_to(last + total, running.shape[1:])

    size = residual_ref.shape[0]
    slices = pair_out.shape[0]
    wide = pair_out.shape[2]

    def columns(i):
        return pl.ds(pl.multiple_of(i * wide, wide), wide)

    def exchange(src, dst, sems, kind, i, target):
        return pltpu.make_async_remote_copy(
            src_ref=src.at[i],
            dst_ref=dst.at[i],
            send_sem=sems.at[2 * kind, i],
            recv_sem=sems.at[2 * kind + 1, i],
            device_id={"tp": target},
            device_id_type=MESH,
        )

    def pair(sems, i):
        return exchange(pair_out, pair_in, sems, 0, i, near)

    def across(sems, i):
        return exchange(far_out, far_in, sems, 1, i, far)

    def beside(sems, i):
        return exchange(near_out, near_in, sems, 2, i, near)

    def product_slice(x_ref, weight, sems, i):
        def term(owner):
            rows = pl.ds(pl.multiple_of(owner * size, size), size)
            return jnp.dot(x_ref[rows, :], weight(), preferred_element_type=jnp.float32)

        pair_out[i] = term(opposite).astype(jnp.bfloat16)
        pair(sems, i).start()
        onward = term(far)
        near_out[i] = term(near).astype(jnp.bfloat16)
        beside(sems, i).start()
        pair(sems, i).wait_recv()
        far_out[i] = (onward + pair_in[i].astype(jnp.float32)).astype(jnp.bfloat16)
        across(sems, i).start()
        own = term(tp)
        beside(sems, i).wait_recv()
        return own + near_in[i].astype(jnp.float32)

    @pl.loop(0, slices)
    def _(i):
        tick(started + blocks + i)
        total_rows[:, columns(i)] = product_slice(
            gated, lambda: wo_ref[:, columns(i)], first_sem, i
        )

    @pl.loop(0, slices)
    def _(i):
        across(first_sem, i).wait_recv()
        total_rows[:, columns(i)] += far_in[i].astype(jnp.float32)

    pad = group.shape[0] - 4 * size
    row_pieces = rows_sem.shape[1]
    row_step = size // row_pieces

    def at(owner, p):
        row = pad + owner * size + p * row_step
        return group.at[pl.ds(pl.multiple_of(row, pad), row_step)]

    def send_rows(owner, kind, p, target):
        return pltpu.make_async_remote_copy(
            src_ref=at(owner, p),
            dst_ref=at(owner, p),
            send_sem=rows_sem.at[2 * kind, p],
            recv_sem=rows_sem.at[2 * kind + 1, p],
            device_id={"tp": target},
            device_id_type=MESH,
        )

    @pl.when(me == 0)
    def _():
        group[0:pad, :] = jnp.zeros((pad, group.shape[1]), group.dtype)

    @pl.loop(0, row_pieces)
    def _(p):
        rows = pl.ds(pl.multiple_of(p * row_step, row_step), row_step)
        rounded = (residual_ref[rows, :].astype(jnp.float32) + total_rows[rows, :]).astype(
            jnp.bfloat16
        )
        stream[rows, :] = rounded
        x = rounded.astype(jnp.float32)
        normed = x * lax.rsqrt(jnp.mean(x * x, axis=-1, keepdims=True) + eps) * norm_gain_ref[...]
        row = pad + tp * size + p * row_step
        group[pl.ds(pl.multiple_of(row, pad), row_step), :] = normed.astype(jnp.bfloat16)
        send_rows(tp, 0, p, far).start()
        send_rows(tp, 1, p, near).start()

    @pl.loop(0, row_pieces)
    def _(p):
        tick(started + blocks + slices + p)
        send_rows(far, 0, p, far).wait_recv()
        send_rows(far, 2, p, near).start()

    @pl.loop(0, row_pieces)
    def _(p):
        send_rows(near, 1, p, near).wait_recv()
        send_rows(opposite, 2, p, near).wait_recv()

    edge = pltpu.make_async_remote_copy(
        src_ref=group.at[pl.ds(4 * size, pad)],
        dst_ref=group.at[pl.ds(0, pad)],
        send_sem=edge_sem.at[0],
        recv_sem=edge_sem.at[1],
        device_id={"sp": lax.rem(me + 1, count)},
        device_id_type=MESH,
    )

    @pl.when(me + 1 < count)
    def _():
        edge.start()

    reached = jnp.maximum(started + blocks + slices + row_pieces, up_ticks)

    @pl.loop(jnp.minimum(started + blocks + slices + row_pieces, up_ticks), up_ticks)
    def _(n):
        up_tick(n)

    for m in range(up_pieces):
        for w in range(2):
            up_hop(w, count - 2, m).wait_recv()

    @pl.when(me > 0)
    def _():
        edge.wait_recv()

    @pl.loop(0, slices)
    def _(i):
        pair(first_sem, i).wait_send()
        across(first_sem, i).wait_send()
        beside(first_sem, i).wait_send()

    early = up_ticks + half * down_pieces

    @pl.loop(0, tiles)
    def _(i):
        @pl.when(reached + i < early)
        def _():
            tick(reached + i)

        up_tile[...] = jnp.dot(group[...], full_up[i], preferred_element_type=jnp.float32)
        tokens = 4 * size
        at_lane = pl.ds(pl.multiple_of(i * lane, lane), lane)

        def conv(taps_ref, first):
            taps = taps_ref[:, at_lane]
            lanes = slice(first, first + lane)
            return (
                taps[0:1, :] * up_tile[pad - 2 : pad - 2 + tokens, lanes]
                + taps[1:2, :] * up_tile[pad - 1 : pad - 1 + tokens, lanes]
                + taps[2:3, :] * up_tile[pad : pad + tokens, lanes]
            )

        act = jax.nn.silu(conv(gate_taps_ref, 0)) * conv(value_taps_ref, lane)
        hidden[:, at_lane] = act.astype(jnp.bfloat16)

    @pl.loop(jnp.minimum(reached + tiles, early), early)
    def _(n):
        tick(n)

    def owner_of(i):
        k = i // 2
        j = lax.rem(i, 2)
        away = j * (half + k) + (1 - j) * lax.rem(half - k, half)
        return index(place - away)

    @pl.loop(0, half)
    def _(k):
        for m in range(down_pieces):
            tick(early + k * down_pieces + m)

        @pl.when(k == half - 1)
        def _():
            for m in range(down_pieces):
                for w in range(2):
                    down_hop(w, count - 2, m).wait_recv()

        for j in range(2):
            i = 2 * k + j
            owner = owner_of(i)
            total_rows[:, columns(owner)] = product_slice(
                hidden, lambda: full_down[owner], second_sem, i
            )

    @pl.loop(0, slices)
    def _(i):
        across(second_sem, i).wait_recv()
        cols = columns(owner_of(i))
        out_ref[:, cols] = (
            stream[:, cols].astype(jnp.float32)
            + (total_rows[:, cols] + far_in[i].astype(jnp.float32))
        ).astype(out_ref.dtype)

    swap.wait_send()

    @pl.when(step_at + 1 < half)
    def _():
        hand.wait_send()

    @pl.when(me + 1 < count)
    def _():
        edge.wait_send()

    @pl.loop(0, slices)
    def _(i):
        pair(second_sem, i).wait_send()
        across(second_sem, i).wait_send()
        beside(second_sem, i).wait_send()

    @pl.loop(0, row_pieces)
    def _(p):
        send_rows(tp, 0, p, far).wait_send()
        send_rows(tp, 1, p, near).wait_send()
        send_rows(far, 2, p, near).wait_send()

    @pl.loop(started - 2, up_ticks)
    def _(n):
        up_sent(n)

    @pl.loop(0, count - 1)
    def _(t):
        for w in range(2):
            for m in range(down_pieces):
                down_hop(w, t, m).wait_send()


FIRST_TICKS = 4
NEXT_TICKS = 2
UP_PIECES = 4
DOWN_PIECES = 2
PAD_ROWS = 16


def one_kernel_fits(rows, gate_w, down_w):
    count = lax.axis_size("sp")
    return (
        lax.axis_size("tp") == 4
        and count >= 4
        and count % 2 == 0
        and gate_w.shape[0] % (16 * 2 * UP_PIECES) == 0
        and gate_w.shape[1] % 128 == 0
        and down_w.shape[0] % (16 * 2 * DOWN_PIECES) == 0
        and down_w.shape[1] % 128 == 0
        and rows % 64 == 0
    )


def layer(q, k, v, gates, input_log, forget_log, gain, wo, residual, norm_gain, gate_w, value_w, down_w, gate_taps, value_taps):
    count = lax.axis_size("sp")
    heads = input_log.shape[1]
    tokens = q.shape[0]
    key_width = q.shape[1] // heads
    value_width = v.shape[1] // heads
    span = key_width + STATE_PAD
    model = wo.shape[1]
    rows = residual.shape[0]
    lane = 128
    tiles = gate_w.shape[1] // lane
    logs = jnp.concatenate([input_log.T, forget_log.T], axis=0)
    slices, wide = count, down_w.shape[1]
    row_pieces = 4
    vmem = pl.BlockSpec(memory_space=pltpu.VMEM)
    hbm = pl.BlockSpec(memory_space=pl.ANY)
    slots = pltpu.VMEM((slices, rows, wide), jnp.bfloat16)
    dma = pltpu.SemaphoreType.DMA
    return pl.pallas_call(
        functools.partial(layer_kernel, count, heads, UP_PIECES, DOWN_PIECES),
        out_shape=jax.ShapeDtypeStruct(residual.shape, jnp.bfloat16),
        in_specs=[vmem] * 11 + [hbm] * 3,
        out_specs=vmem,
        scratch_shapes=[
            pltpu.VMEM((tokens // BLOCK, 8, BLOCK), jnp.float32),
            pltpu.VMEM((tokens, BLOCK), jnp.float32),
            pltpu.VMEM((heads * span, value_width), jnp.bfloat16),
            pltpu.VMEM((2, heads * span, value_width), jnp.bfloat16),
            pltpu.VMEM((heads, key_width, value_width), jnp.float32),
            pltpu.VMEM((heads, 8, key_width), jnp.float32),
            pltpu.VMEM((heads, 8, 128), jnp.float32),
            pltpu.VMEM((heads, key_width, value_width), jnp.float32),
            pltpu.VMEM((heads, 8, key_width), jnp.float32),
            pltpu.VMEM((2, heads, 8, 128), jnp.float32),
            pltpu.VMEM((heads * span, value_width), jnp.bfloat16),
            pltpu.VMEM((tokens, v.shape[1]), jnp.bfloat16),
        ]
        + [slots] * 6
        + [
            pltpu.VMEM((rows, model), jnp.float32),
            pltpu.VMEM((rows, model), jnp.bfloat16),
            pltpu.VMEM((PAD_ROWS + tokens, model), jnp.bfloat16),
            pltpu.VMEM((tiles, model, 2 * lane), jnp.bfloat16),
            pltpu.VMEM((count,) + down_w.shape, jnp.bfloat16),
            pltpu.VMEM((PAD_ROWS + tokens, 2 * lane), jnp.float32),
            pltpu.VMEM((tokens, down_w.shape[0]), jnp.bfloat16),
            dma((2 * tiles + 1,)),
            dma((2,)),
            dma((2,)),
            dma((2, UP_PIECES, count - 1)),
            dma((2, UP_PIECES, count - 1)),
            dma((2, DOWN_PIECES, count - 1)),
            dma((2, DOWN_PIECES, count - 1)),
            dma((6, slices)),
            dma((6, slices)),
            dma((6, row_pieces)),
            dma((2,)),
        ],
        compiler_params=pltpu.CompilerParams(
            collective_id=0, has_side_effects=True, vmem_limit_bytes=60 * 1024 * 1024
        ),
        cost_estimate=pl.CostEstimate(
            flops=30_000_000_000, bytes_accessed=8 * v.size, transcendentals=0
        ),
    )(
        logs,
        q,
        k,
        v,
        gates,
        gain,
        wo,
        residual,
        norm_gain[None, :],
        gate_taps,
        value_taps,
        gate_w,
        value_w,
        down_w,
    )


def local(
    residual_entry_input,
    query_matrix_rows,
    key_matrix_rows,
    value_matrix_rows,
    output_gate_logits,
    input_gate_logits,
    forget_gate_logits,
    forget_decay_offset,
    head_norm_gain,
    cell_output_weight,
    feedforward_norm_gain,
    gate_up_weight,
    value_up_weight,
    gate_filter_taps,
    value_filter_taps,
    down_projection_weight,
):
    input_log, forget_log = gate_log_values(
        input_gate_logits, forget_gate_logits, forget_decay_offset
    )
    if one_kernel_fits(residual_entry_input.shape[0], gate_up_weight, down_projection_weight):
        return layer(
            query_matrix_rows,
            key_matrix_rows,
            value_matrix_rows,
            output_gate_logits,
            input_log,
            forget_log,
            head_norm_gain,
            cell_output_weight,
            residual_entry_input,
            feedforward_norm_gain,
            gate_up_weight,
            value_up_weight,
            down_projection_weight,
            gate_filter_taps,
            value_filter_taps,
        )
    whole_gate = lax.all_gather(gate_up_weight, "sp", axis=0, tiled=True)
    whole_down = lax.all_gather(down_projection_weight, "sp", axis=1, tiled=True)
    gated_rows = cell(
        query_matrix_rows,
        key_matrix_rows,
        value_matrix_rows,
        output_gate_logits,
        input_log,
        forget_log,
        head_norm_gain,
    )
    mixed_rows = product_rows(gated_rows, cell_output_weight, 2)
    stream_wide = residual_entry_input.astype(jnp.float32) + mixed_rows
    stream = stream_wide.astype(jnp.bfloat16)
    stream_wide = lax.optimization_barrier(stream).astype(jnp.float32)
    normed_rows = (
        stream_wide
        * lax.rsqrt(jnp.mean(stream_wide * stream_wide, axis=-1, keepdims=True) + eps)
        * feedforward_norm_gain[None, :]
    ).astype(jnp.bfloat16)
    group_rows = gather_rows(normed_rows)
    group_rows, value_shard = lax.optimization_barrier((group_rows, value_up_weight))
    whole_value = walk_gather(value_shard, 2)
    earlier_rows = shifted(group_rows[-2:], "sp", 1)
    window = jnp.concatenate([earlier_rows, group_rows], axis=0)
    up_gate = jnp.dot(
        window,
        whole_gate,
        preferred_element_type=jnp.float32,
    )
    up_value = jnp.dot(
        window,
        whole_value,
        preferred_element_type=jnp.float32,
    )
    conv_g = (
        gate_filter_taps[0][None, :] * up_gate[:-2]
        + gate_filter_taps[1][None, :] * up_gate[1:-1]
        + gate_filter_taps[2][None, :] * up_gate[2:]
    )
    conv_v = (
        value_filter_taps[0][None, :] * up_value[:-2]
        + value_filter_taps[1][None, :] * up_value[1:-1]
        + value_filter_taps[2][None, :] * up_value[2:]
    )
    hidden = (jax.nn.silu(conv_g) * conv_v).astype(jnp.bfloat16)
    ffn_rows = product_rows(hidden, whole_down, 3)
    return (stream_wide + ffn_rows).astype(jnp.bfloat16)


def solution(mesh):
    in_specs = (
        P(("sp", "tp"), None),
        P("sp", "tp"),
        P("sp", "tp"),
        P("sp", "tp"),
        P("sp", "tp"),
        P("sp", "tp"),
        P("sp", "tp"),
        P("sp", "tp"),
        P("tp", None),
        P("tp", None),
        P(),
        P("sp", "tp"),
        P("sp", "tp"),
        P(None, "tp"),
        P(None, "tp"),
        P("tp", "sp"),
    )
    out_specs = P(("sp", "tp"), None)
    return jax.shard_map(local, mesh=mesh, in_specs=in_specs, out_specs=out_specs, check_vma=False)
```

```python
import functools

import jax
import jax.numpy as jnp
from jax import lax
from jax.experimental import pallas as pl
from jax.experimental.pallas import tpu as pltpu
from jax.sharding import PartitionSpec as P

BLOCK = 128


eps = 1e-06
neg_large = -1e30


def shifted(x, axis, by):
    count = lax.axis_size(axis)
    pairs = [(i, i + by) for i in range(count) if 0 <= i + by < count]
    return lax.ppermute(x, axis, pairs)


def gate_log_values(input_gate_logits, forget_gate_logits, forget_decay_offset):
    input_log_value = 15.0 * jnp.tanh(input_gate_logits / 15.0)
    forget_log_sigmoid = (
        jax.nn.log_sigmoid(15.0 * jnp.tanh(forget_gate_logits / 15.0)) + forget_decay_offset
    )
    return (input_log_value, forget_log_sigmoid)


STATE_PAD = 16
MESH = pl.DeviceIdType.MESH


def cell_kernel(
    count,
    heads,
    state_ref,
    q_ref,
    k_ref,
    v_ref,
    gate_ref,
    gain_ref,
    rows_ref,
    cols_ref,
    out_ref,
    held,
    memory,
    normer,
    running,
    send_sem,
    recv_sem,
):
    me = lax.axis_index("sp")
    barrier = pltpu.get_barrier_semaphore()
    for d in range(1, count):
        pl.semaphore_signal(
            barrier, inc=1, device_id={"sp": lax.rem(me + d, count)}, device_id_type=MESH
        )
    pl.semaphore_wait(barrier, count - 1)

    def push(d, target, slot):
        return pltpu.make_async_remote_copy(
            src_ref=state_ref,
            dst_ref=held.at[slot],
            send_sem=send_sem.at[d],
            recv_sem=recv_sem.at[d],
            device_id={"sp": target},
            device_id_type=MESH,
        )

    for d in range(1, count):

        @pl.when(me + d < count)
        def _():
            push(d, me + d, me).start()

    memory[...] = jnp.zeros_like(memory)
    normer[...] = jnp.zeros_like(normer)
    running[...] = jnp.full(running.shape, neg_large, jnp.float32)
    for d in range(1, count):

        @pl.when(me - d >= 0)
        def _():
            push(d, lax.rem(me + d, count), me - d).wait_recv()

    key_width = memory.shape[1]
    value_width = memory.shape[2]
    span = key_width + STATE_PAD

    @pl.loop(0, me)
    def _(j):
        for h in range(heads):
            low = h * span
            extra = held[j, low + key_width : low + span, :].astype(jnp.float32)
            total = extra[2:3, :1] + extra[3:4, :1]
            level = extra[4:5, :1] + extra[5:6, :1]
            before = running[h, :1, :1]
            after = jnp.maximum(total + before, level)
            one = jnp.exp(total + before - after)
            two = jnp.exp(level - after)
            memory[h] = one * memory[h] + two * held[j, low : low + key_width, :].astype(
                jnp.float32
            )
            parts = extra[0:1, :key_width] + extra[1:2, :key_width]
            normer[h, :1, :] = one * normer[h, :1, :] + two * parts
            running[h] = jnp.broadcast_to(after, running.shape[1:])

    length = BLOCK
    scale = key_width ** (-0.5)
    at_row = lax.broadcasted_iota(jnp.int32, (length, length), 0)
    at_col = lax.broadcasted_iota(jnp.int32, (length, length), 1)
    causal = at_col <= at_row

    @pl.loop(0, q_ref.shape[0] // length)
    def _(j):
        rows = pl.ds(pl.multiple_of(j * length, length), length)
        lanes = rows_ref[j]
        cols = cols_ref[rows, :]
        for h in range(heads):
            keys = slice(h * key_width, (h + 1) * key_width)
            vals = slice(h * value_width, (h + 1) * value_width)
            q = q_ref[rows, keys]
            k = k_ref[rows, keys]
            v = v_ref[rows, vals]
            before = running[h, :1, :1]
            total = lanes[heads + h : heads + h + 1, :1]
            shifted_log = jnp.where(causal, lanes[h : h + 1, :], -jnp.inf)
            top = jnp.maximum(jnp.max(shifted_log, axis=1, keepdims=True), before)
            raw = (
                lax.dot_general(
                    q, k, (((1,), (1,)), ((), ())), preferred_element_type=jnp.float32
                )
                * scale
            )
            scores = raw * jnp.exp(shifted_log - top)
            carry = jnp.exp(before - top) * scale
            state = memory[h]
            high = state.astype(jnp.bfloat16)
            low = (state - high.astype(jnp.float32)).astype(jnp.bfloat16)
            carried = jnp.dot(q, high, preferred_element_type=jnp.float32) + jnp.dot(
                q, low, preferred_element_type=jnp.float32
            )
            numerator = carry * carried + jnp.dot(
                scores.astype(jnp.bfloat16), v, preferred_element_type=jnp.float32
            )
            denominator = carry * jnp.sum(
                q.astype(jnp.float32) * normer[h, :1, :], axis=1, keepdims=True
            ) + jnp.sum(scores, axis=1, keepdims=True)
            level = cols[:, h : h + 1] + top
            value = numerator / jnp.maximum(jnp.abs(denominator), jnp.exp(-level))
            mean = jnp.mean(value * value, axis=1, keepdims=True)
            normed = value * lax.rsqrt(mean + eps) * gain_ref[h : h + 1, :]
            gated = normed * jax.nn.sigmoid(gate_ref[rows, vals].astype(jnp.float32))
            out_ref[rows, vals] = gated.astype(out_ref.dtype)
            last = jnp.max(jnp.maximum(lanes[h : h + 1, :], before), axis=1, keepdims=True)
            decay = jnp.exp(before - last)
            weighted = k.astype(jnp.float32) * jnp.exp(cols[:, heads + h : heads + h + 1] - last)
            memory[h] = decay * state + lax.dot_general(
                weighted.astype(jnp.bfloat16),
                v,
                (((0,), (0,)), ((), ())),
                preferred_element_type=jnp.float32,
            )
            normer[h, :1, :] = decay * normer[h, :1, :] + jnp.sum(
                weighted, axis=0, keepdims=True
            )
            running[h] = jnp.broadcast_to(last + total, running.shape[1:])

    for d in range(1, count):

        @pl.when(me + d < count)
        def _():
            push(d, me + d, me).wait_send()


def halves(x):
    high = lax.reduce_precision(x, 8, 7)
    return (high.astype(jnp.bfloat16), (x - high).astype(jnp.bfloat16))


def cell_parts(q, k, v, input_log, forget_log):
    heads = input_log.shape[1]
    tokens = q.shape[0]
    key_width = q.shape[1] // heads
    value_width = v.shape[1] // heads
    count = lax.axis_size("sp")
    blocks = tokens // BLOCK
    f = forget_log.reshape(blocks, BLOCK, heads)
    tri = jnp.tril(jnp.ones((BLOCK, BLOCK), jnp.float32))
    within = jnp.einsum("ts,bsh->bth", tri, f, precision=lax.Precision.HIGHEST)
    each = within[:, -1, :]
    later = jnp.triu(jnp.ones((blocks, blocks), jnp.float32), 1)
    after = jnp.einsum("bc,ch->bh", later, each, precision=lax.Precision.HIGHEST)
    total = jnp.sum(each, axis=0)
    shifted_log = input_log.reshape(blocks, BLOCK, heads) - within
    to_end = (shifted_log + (each + after)[:, None, :]).reshape(tokens, heads)
    level = jnp.max(to_end, axis=0)
    weighted = k.reshape(tokens, heads, key_width).astype(jnp.float32) * jnp.exp(to_end - level)[
        :, :, None
    ]
    memory = jnp.einsum(
        "shd,shv->hdv",
        weighted.astype(jnp.bfloat16),
        v.reshape(tokens, heads, value_width),
        preferred_element_type=jnp.float32,
    ).astype(jnp.bfloat16)
    normer = jnp.sum(weighted, axis=0)
    wide = (heads, 1, value_width)
    lines = [
        jnp.pad(part, ((0, 0), (0, value_width - key_width)))[:, None, :]
        for part in halves(normer)
    ]
    for scalar in (total, level):
        lines += [jnp.broadcast_to(part[:, None, None], wide) for part in halves(scalar)]
    lines.append(jnp.zeros((heads, STATE_PAD - len(lines), value_width), jnp.bfloat16))
    span = key_width + STATE_PAD
    state = jnp.concatenate([memory] + lines, axis=1).reshape(heads * span, value_width)
    lanes = jnp.concatenate(
        [
            jnp.transpose(shifted_log, (0, 2, 1)),
            jnp.broadcast_to(each[:, :, None], (blocks, heads, BLOCK)),
        ],
        axis=1,
    )
    cols = jnp.concatenate([within, shifted_log], axis=2).reshape(tokens, 2 * heads)
    return state, lanes, cols


def cell(q, k, v, gates, input_log, forget_log, gain):
    heads = input_log.shape[1]
    key_width = q.shape[1] // heads
    value_width = v.shape[1] // heads
    count = lax.axis_size("sp")
    span = key_width + STATE_PAD
    state, lanes, cols = cell_parts(q, k, v, input_log, forget_log)
    vmem = pl.BlockSpec(memory_space=pltpu.VMEM)
    return pl.pallas_call(
        functools.partial(cell_kernel, count, heads),
        out_shape=jax.ShapeDtypeStruct(v.shape, jnp.bfloat16),
        in_specs=[vmem] * 8,
        out_specs=vmem,
        scratch_shapes=[
            pltpu.VMEM((count, heads * span, value_width), jnp.bfloat16),
            pltpu.VMEM((heads, key_width, value_width), jnp.float32),
            pltpu.VMEM((heads, 8, key_width), jnp.float32),
            pltpu.VMEM((heads, 8, 128), jnp.float32),
            pltpu.SemaphoreType.DMA((count,)),
            pltpu.SemaphoreType.DMA((count,)),
        ],
        compiler_params=pltpu.CompilerParams(
            collective_id=0, has_side_effects=True, vmem_limit_bytes=40 * 1024 * 1024
        ),
        cost_estimate=pl.CostEstimate(
            flops=30_000_000_000, bytes_accessed=8 * v.size, transcendentals=0
        ),
    )(state, q, k, v, gates, gain, lanes, cols)


def rows_kernel(pieces, x_ref, out_ref, own_sem, near_send, near_recv, far_send, far_recv, on_send, on_recv):
    me = lax.axis_index("tp")
    near = me + 1 - 2 * lax.rem(me, 2)
    far = lax.rem(me + 2, 4)
    opposite = lax.rem(near + 2, 4)
    size = x_ref.shape[0]
    step = size // pieces
    barrier = pltpu.get_barrier_semaphore()
    for other in (near, far):
        pl.semaphore_signal(barrier, inc=1, device_id={"tp": other}, device_id_type=MESH)
    pl.semaphore_wait(barrier, 2)

    def at(owner, p):
        return out_ref.at[pl.ds(pl.multiple_of(owner * size + p * step, step), step)]

    def send(src, dst, sems, p, target):
        return pltpu.make_async_remote_copy(
            src_ref=src,
            dst_ref=dst,
            send_sem=sems[0].at[p],
            recv_sem=sems[1].at[p],
            device_id={"tp": target},
            device_id_type=MESH,
        )

    mine = [x_ref.at[pl.ds(p * step, step)] for p in range(pieces)]
    far_out = [send(mine[p], at(me, p), (far_send, far_recv), p, far) for p in range(pieces)]
    near_out = [send(mine[p], at(me, p), (near_send, near_recv), p, near) for p in range(pieces)]
    far_in = [send(mine[p], at(far, p), (far_send, far_recv), p, far) for p in range(pieces)]
    near_in = [send(mine[p], at(near, p), (near_send, near_recv), p, near) for p in range(pieces)]
    onward = [send(at(far, p), at(far, p), (on_send, on_recv), p, near) for p in range(pieces)]
    on_in = [
        send(at(opposite, p), at(opposite, p), (on_send, on_recv), p, near)
        for p in range(pieces)
    ]
    for p in range(pieces):
        far_out[p].start()
    for p in range(pieces):
        near_out[p].start()
    whole = pl.ds(pl.multiple_of(me * size, size), size)
    own = pltpu.make_async_copy(x_ref, out_ref.at[whole], own_sem)
    own.start()
    for p in range(pieces):
        far_in[p].wait_recv()
        onward[p].start()
    own.wait()
    for p in range(pieces):
        near_in[p].wait_recv()
        on_in[p].wait_recv()
    for p in range(pieces):
        far_out[p].wait_send()
        near_out[p].wait_send()
        onward[p].wait_send()


def gather_rows(x):
    if lax.axis_size("tp") != 4:
        return lax.all_gather(x, "tp", axis=0, tiled=True)
    pieces = 4
    vmem = pl.BlockSpec(memory_space=pltpu.VMEM)
    return pl.pallas_call(
        functools.partial(rows_kernel, pieces),
        out_shape=jax.ShapeDtypeStruct((4 * x.shape[0], x.shape[1]), x.dtype),
        in_specs=[vmem],
        out_specs=vmem,
        scratch_shapes=[pltpu.SemaphoreType.DMA] + [pltpu.SemaphoreType.DMA((pieces,))] * 6,
        compiler_params=pltpu.CompilerParams(
            collective_id=1, has_side_effects=True, vmem_limit_bytes=16 * 1024 * 1024
        ),
        cost_estimate=pl.CostEstimate(
            flops=30_000_000_000, bytes_accessed=4 * x.size, transcendentals=0
        ),
    )(x)


def product_kernel(
    pieces,
    x_ref,
    w_ref,
    out_ref,
    pair_out,
    pair_in,
    far_out,
    far_in,
    near_out,
    near_in,
    pair_send,
    pair_recv,
    far_send,
    far_recv,
    near_send,
    near_recv,
):
    me = lax.axis_index("tp")
    near = me + 1 - 2 * lax.rem(me, 2)
    far = lax.rem(me + 2, 4)
    opposite = lax.rem(near + 2, 4)
    size = out_ref.shape[0]
    step = out_ref.shape[1] // pieces
    barrier = pltpu.get_barrier_semaphore()
    for other in (near, far):
        pl.semaphore_signal(barrier, inc=1, device_id={"tp": other}, device_id_type=MESH)
    pl.semaphore_wait(barrier, 2)

    def columns(p):
        return pl.ds(pl.multiple_of(p * step, step), step)

    def term(owner, p):
        rows = pl.ds(pl.multiple_of(owner * size, size), size)
        return jnp.dot(x_ref[rows, :], w_ref[:, columns(p)], preferred_element_type=jnp.float32)

    def send(src, dst, sems, p, target):
        return pltpu.make_async_remote_copy(
            src_ref=src.at[p],
            dst_ref=dst.at[p],
            send_sem=sems[0].at[p],
            recv_sem=sems[1].at[p],
            device_id={"tp": target},
            device_id_type=MESH,
        )

    def pair(p):
        return send(pair_out, pair_in, (pair_send, pair_recv), p, near)

    def across(p):
        return send(far_out, far_in, (far_send, far_recv), p, far)

    def beside(p):
        return send(near_out, near_in, (near_send, near_recv), p, near)

    @pl.loop(0, pieces)
    def _(p):
        pair_out[p] = term(opposite, p).astype(jnp.bfloat16)
        pair(p).start()
        mine = term(far, p)
        pair(p).wait_recv()
        far_out[p] = (mine + pair_in[p].astype(jnp.float32)).astype(jnp.bfloat16)
        across(p).start()

    @pl.loop(0, pieces)
    def _(p):
        near_out[p] = term(near, p).astype(jnp.bfloat16)
        beside(p).start()

    @pl.loop(0, pieces)
    def _(p):
        own = term(me, p)
        beside(p).wait_recv()
        out_ref[:, columns(p)] = own + near_in[p].astype(jnp.float32)

    @pl.loop(0, pieces)
    def _(p):
        across(p).wait_recv()
        out_ref[:, columns(p)] += far_in[p].astype(jnp.float32)

    @pl.loop(0, pieces)
    def _(p):
        pair(p).wait_send()
        across(p).wait_send()
        beside(p).wait_send()


def product_rows(x, w, tag):
    if lax.axis_size("tp") != 4:
        partial = jnp.dot(x, w, preferred_element_type=jnp.float32).astype(jnp.bfloat16)
        return lax.psum_scatter(partial, "tp", scatter_dimension=0, tiled=True).astype(
            jnp.float32
        )
    pieces = 4
    rows, wide = x.shape[0] // 4, w.shape[1]
    vmem = pl.BlockSpec(memory_space=pltpu.VMEM)
    slots = pltpu.VMEM((pieces, rows, wide // pieces), jnp.bfloat16)
    return pl.pallas_call(
        functools.partial(product_kernel, pieces),
        out_shape=jax.ShapeDtypeStruct((rows, wide), jnp.float32),
        in_specs=[vmem] * 2,
        out_specs=vmem,
        scratch_shapes=[slots] * 6 + [pltpu.SemaphoreType.DMA((pieces,))] * 6,
        compiler_params=pltpu.CompilerParams(
            collective_id=tag, has_side_effects=True, vmem_limit_bytes=40 * 1024 * 1024
        ),
        cost_estimate=pl.CostEstimate(
            flops=30_000_000_000, bytes_accessed=2 * w.size, transcendentals=0
        ),
    )(x, w)


def walk_kernel(count, pieces, x_ref, out_ref, own_sem, send_sem, recv_sem):
    me = lax.axis_index("sp")
    odd = lax.rem(me, 2)
    place = me // 2 + odd * (count - 1 - 2 * (me // 2))
    size = x_ref.shape[0]
    step = size // (2 * pieces)

    def index(position):
        position = lax.rem(position + 2 * count, count)
        back = position // (count // 2)
        return (1 - back) * 2 * position + back * (2 * (count - 1 - position) + 1)

    ways = (1, -1)
    barrier = pltpu.get_barrier_semaphore()
    for way in ways:
        pl.semaphore_signal(
            barrier, inc=1, device_id={"sp": index(place + way)}, device_id_type=MESH
        )
    pl.semaphore_wait(barrier, 2)

    def hop(w, t, p, age, own=False):
        inner = (w * pieces + p) * step
        owner = index(place - ways[w] * age)
        dst = out_ref.at[pl.ds(pl.multiple_of(owner * size + inner, step), step)]
        return pltpu.make_async_remote_copy(
            src_ref=x_ref.at[pl.ds(inner, step)] if own else dst,
            dst_ref=dst,
            send_sem=send_sem.at[w, p, t],
            recv_sem=recv_sem.at[w, p, t],
            device_id={"sp": index(place + ways[w])},
            device_id_type=MESH,
        )

    for p in range(pieces):
        for w in range(2):
            hop(w, 0, p, 0, True).start()
    whole = pl.ds(pl.multiple_of(me * size, size), size)
    own = pltpu.make_async_copy(x_ref, out_ref.at[whole], own_sem)
    own.start()

    @pl.loop(1, count - 1)
    def _(t):
        for p in range(pieces):
            for w in range(2):
                hop(w, t - 1, p, t).wait_recv()
                hop(w, t, p, t).start()

    own.wait()
    for p in range(pieces):
        for w in range(2):
            hop(w, count - 2, p, count - 1).wait_recv()
            hop(w, 0, p, 0, True).wait_send()

    @pl.loop(1, count - 1)
    def _(t):
        for p in range(pieces):
            for w in range(2):
                hop(w, t, p, t).wait_send()


def walk_gather(x, pieces):
    count = lax.axis_size("sp")
    if count % 2 or count < 4 or x.shape[0] % (32 * pieces):
        return lax.all_gather(x, "sp", axis=0, tiled=True)
    vmem = pl.BlockSpec(memory_space=pltpu.VMEM)
    return pl.pallas_call(
        functools.partial(walk_kernel, count, pieces),
        out_shape=jax.ShapeDtypeStruct((count * x.shape[0], x.shape[1]), x.dtype),
        in_specs=[vmem],
        out_specs=vmem,
        scratch_shapes=[pltpu.SemaphoreType.DMA]
        + [pltpu.SemaphoreType.DMA((2, pieces, count - 1))] * 2,
        compiler_params=pltpu.CompilerParams(
            collective_id=4, has_side_effects=True, vmem_limit_bytes=16 * 1024 * 1024
        ),
        cost_estimate=pl.CostEstimate(
            flops=30_000_000_000, bytes_accessed=count * x.size, transcendentals=0
        ),
    )(x)


def layer_kernel(
    count,
    heads,
    up_pieces,
    down_pieces,
    logs_ref,
    q_ref,
    k_ref,
    v_ref,
    gate_ref,
    gain_ref,
    residual_ref,
    norm_gain_ref,
    gate_taps_ref,
    value_taps_ref,
    wo_ref,
    gate_w_ref,
    value_w_ref,
    down_w_ref,
    out_ref,
    rows_ref,
    cols_ref,
    state_ref,
    held,
    memory,
    normer,
    running,
    pair_memory,
    pair_normer,
    pair_level,
    handed,
    gated,
    mine,
    wo_full,
    middle,
    give_up,
    give_down,
    full_up,
    full_down,
    total_rows,
    stream,
    group,
    up_tile,
    hidden,
    pair_out,
    pair_in,
    second_out,
    second_in,
    third_out,
    third_in,
    kept,
    load_sem,
    wo_sem,
    give_sem,
    state_send,
    state_recv,
    up_send,
    up_recv,
    down_send,
    down_recv,
    block_send,
    block_recv,
    rows_send,
    rows_recv,
    sum_send,
    sum_recv,
    edge_sem,
):
    me = lax.axis_index("sp")
    tp = lax.axis_index("tp")
    core = lax.rem(tp, 2)
    chip = tp // 2
    near = tp + 1 - 2 * core
    far = lax.rem(tp + 2, 4)
    opposite = lax.rem(near + 2, 4)
    odd = lax.rem(me, 2)
    partner = me + 1 - 2 * odd
    line = count // 2
    place = me // 2
    model = full_up.shape[0]
    lane = 128
    up_rows = model // count
    up_step = 2 * up_rows // up_pieces
    half_width = full_down.shape[1]
    tiles = half_width // lane
    rest = half_width - tiles * lane
    wide = full_down.shape[2]
    down_step = 2 * half_width // down_pieces

    barrier = pltpu.get_barrier_semaphore()
    for other in (near, far, opposite):
        pl.semaphore_signal(barrier, inc=1, device_id={"tp": other}, device_id_type=MESH)
    for other in (partner, lax.rem(me + 2, count), lax.rem(me + count - 2, count)):
        pl.semaphore_signal(barrier, inc=1, device_id={"sp": other}, device_id_type=MESH)

    own_up = pl.ds(pl.multiple_of(me * up_rows, up_rows), up_rows)
    wo_rows = wo_ref.shape[0]
    wo_own = pl.ds(pl.multiple_of(tp * wo_rows, wo_rows), wo_rows)
    loads = []

    def load(src, dst):
        loads.append(pltpu.make_async_copy(src, dst, load_sem.at[len(loads)]))

    shift = tiles * lane + 2 * rest
    for i in range(tiles):
        for a, w_ref in enumerate((gate_w_ref, value_w_ref)):
            lanes = pl.ds((2 * i + a) * lane, lane)
            for to, y in ((full_up.at[own_up, lanes], odd), (give_up.at[:, lanes], 1 - odd)):
                at = pl.multiple_of(y * shift + i * lane, lane)
                load(w_ref.at[:, pl.ds(at, lane)], to)
    for a, w_ref in enumerate((gate_w_ref, value_w_ref)):
        load(w_ref.at[:, pl.ds(tiles * lane, lane)], middle.at[a])
    for to, y in ((full_down.at[me], odd), (give_down, 1 - odd)):
        at = pl.multiple_of(y * shift, rest)
        load(down_w_ref.at[pl.ds(at, tiles * lane)], to.at[pl.ds(0, tiles * lane)])
        at = pl.multiple_of(tiles * lane + y * rest, rest)
        load(down_w_ref.at[pl.ds(at, rest)], to.at[pl.ds(tiles * lane, rest)])
    load(wo_ref, wo_full.at[wo_own])
    for one in loads:
        one.start()
    pl.semaphore_wait(barrier, 6)
    for one in loads:
        one.wait()

    def remote(src, dst, send_sem, recv_sem, **to):
        return pltpu.make_async_remote_copy(
            src_ref=src,
            dst_ref=dst,
            send_sem=send_sem,
            recv_sem=recv_sem,
            device_id=to,
            device_id_type=MESH,
        )

    at_lane = lax.broadcasted_iota(jnp.int32, (up_rows, lane), 1)
    first_half = at_lane < rest

    def halves_of(g, v, low):
        a = jnp.where(low, g, pltpu.roll(v, rest, 1))
        b = jnp.where(low, pltpu.roll(g, rest, 1), v)
        return a, b

    mid_a, mid_b = halves_of(
        middle[0].astype(jnp.float32), middle[1].astype(jnp.float32), first_half
    )
    tail = slice(2 * tiles * lane, 2 * tiles * lane + lane)
    full_up[own_up, tail] = jnp.where(odd == 0, mid_a, mid_b).astype(jnp.bfloat16)
    give_up[:, tail] = jnp.where(odd == 0, mid_b, mid_a).astype(jnp.bfloat16)

    give_step = up_rows // 2

    def give_rows(p):
        at = pl.multiple_of(me * up_rows + p * give_step, give_step)
        return remote(
            give_up.at[pl.ds(p * give_step, give_step)],
            full_up.at[pl.ds(at, give_step)],
            give_sem.at[0, p],
            give_sem.at[1, p],
            sp=partner,
        )

    give_cols = remote(give_down, full_down.at[me], give_sem.at[0, 2], give_sem.at[1, 2], sp=partner)
    wo_step = wo_rows // 2

    def wo_copy(kind, owner, p, target):
        at = pl.multiple_of(owner * wo_rows + p * wo_step, wo_step)
        part = wo_full.at[pl.ds(at, wo_step)]
        return remote(part, part, wo_sem.at[0, kind, p], wo_sem.at[1, kind, p], tp=target)

    def source(w, t):
        return place - t if w == 0 else place + t

    def has(w, t):
        return place >= t if w == 0 else place + t < line

    def sends(w, t):
        onward = place + 1 < line if w == 0 else place > 0
        return has(w, t) & onward & (t < line - 1)

    def beyond(w):
        return lax.rem(me + 2, count) if w == 0 else lax.rem(me + count - 2, count)

    def up_hop(w, t, m):
        at = source(w, t) * 2 * up_rows + lax.rem(m + odd * (up_pieces // 2), up_pieces) * up_step
        part = full_up.at[pl.ds(pl.multiple_of(at, up_step), up_step)]
        return remote(part, part, up_send.at[w, t, m], up_recv.at[w, t, m], sp=beyond(w))

    def down_hop(w, t, m):
        each = down_pieces // 2
        owner = source(w, t) * 2 + lax.rem(m // each + odd, 2)
        at = lax.rem(m, each) * down_step
        part = full_down.at[owner, pl.ds(pl.multiple_of(at, down_step), down_step)]
        return remote(part, part, down_send.at[w, t, m], down_recv.at[w, t, m], sp=beyond(w))

    up_ticks = line * up_pieces
    all_ticks = up_ticks + line * down_pieces

    def move(hop, pieces, n):
        t = n // pieces
        m = lax.rem(n, pieces)
        for w in range(2):

            @pl.when(has(w, t) & (t > 0))
            def _():
                hop(w, t - 1, m).wait_recv()

            @pl.when(sends(w, t))
            def _():
                hop(w, t, m).start()

    def up_tick(n):
        for p in range(2):

            @pl.when(n == up_pieces // 2 + p * (up_pieces // 4))
            def _():
                give_rows(p).wait_recv()

        move(up_hop, up_pieces, n)

    def down_tick(n):
        @pl.when(n == down_pieces // 2)
        def _():
            give_cols.wait_recv()

        move(down_hop, down_pieces, n)

    def tick(n):
        @pl.when(n < up_ticks)
        def _():
            up_tick(n)

        @pl.when((n >= up_ticks) & (n < all_ticks))
        def _():
            down_tick(n - up_ticks)

    def up_sent(n):
        t = n // up_pieces
        for w in range(2):

            @pl.when(sends(w, t))
            def _():
                up_hop(w, t, lax.rem(n, up_pieces)).wait_send()

    give_rows(0).start()
    for p in range(2):
        wo_copy(0, tp, p, far).start()
        wo_copy(1, tp, p, near).start()
    for n in range(2):
        up_tick(n)

    key_width = memory.shape[1]
    value_width = memory.shape[2]
    span = key_width + STATE_PAD
    swap = remote(state_ref, held.at[0], state_send.at[0], state_recv.at[0], sp=partner)
    hand = remote(handed, held.at[1], state_send.at[1], state_recv.at[1], sp=beyond(0))

    def read_state(ref, h):
        low = h * span
        extra = ref[low + key_width : low + span, :].astype(jnp.float32)
        total = extra[2:3, :1] + extra[3:4, :1]
        level = extra[4:5, :1] + extra[5:6, :1]
        parts = extra[0:1, :key_width] + extra[1:2, :key_width]
        return ref[low : low + key_width, :].astype(jnp.float32), parts, level, total

    def join(first, second, total):
        mem_a, norm_a, level_a = first
        mem_b, norm_b, level_b = second
        after = jnp.maximum(total + level_a, level_b)
        one = jnp.exp(total + level_a - after)
        two = jnp.exp(level_b - after)
        return one * mem_a + two * mem_b, one * norm_a + two * norm_b, after

    def keep(refs, h, values):
        mem, norm, level = values
        refs[0][h] = mem
        refs[1][h, :1, :] = norm
        refs[2][h] = jnp.broadcast_to(level, refs[2].shape[1:])

    carried_refs = (memory, normer, running)

    def write_state(ref, h, mem, norm, level, total):
        low = h * span
        ref[low : low + key_width, :] = mem.astype(jnp.bfloat16)
        lines = jnp.zeros((STATE_PAD, value_width), jnp.float32)
        at_line = lax.broadcasted_iota(jnp.int32, lines.shape, 0)
        norm = jnp.concatenate([norm] * (value_width // key_width), axis=1)
        for i, part in enumerate((norm, total, level)):
            high = part.astype(jnp.bfloat16).astype(jnp.float32)
            lines = jnp.where(at_line == 2 * i, high, lines)
            lines = jnp.where(at_line == 2 * i + 1, part - high, lines)
        ref[low + key_width : low + span, :] = lines.astype(jnp.bfloat16)

    length = BLOCK
    blocks = q_ref.shape[0] // length
    at_row = lax.broadcasted_iota(jnp.int32, (length, length), 0)
    at_col = lax.broadcasted_iota(jnp.int32, (length, length), 1)

    def by_block(first):
        return jnp.concatenate(
            [
                logs_ref[first : first + heads, b * length : (b + 1) * length]
                for b in range(blocks)
            ],
            axis=0,
        )

    within = jnp.dot(
        by_block(heads),
        jnp.where(at_row <= at_col, 1.0, 0.0),
        precision=lax.Precision.HIGHEST,
        preferred_element_type=jnp.float32,
    )
    shifted_all = by_block(0) - within
    each_all = within[:, length - 1 : length]
    after = jnp.zeros((heads, 1), jnp.float32)
    to_end = [None] * blocks
    for b in reversed(range(blocks)):
        part = slice(b * heads, (b + 1) * heads)
        after = after + each_all[part]
        to_end[b] = shifted_all[part] + after
    own_total = after
    own_level = functools.reduce(jnp.maximum, to_end)
    own_level = jnp.max(own_level, axis=1, keepdims=True)
    for b in range(blocks):
        part = slice(b * heads, (b + 1) * heads)
        rows_ref[b, 0 : 2 * heads, :] = jnp.concatenate(
            [shifted_all[part], jnp.broadcast_to(each_all[part], (heads, length))], axis=0
        )
        lines = [within[part], shifted_all[part], jnp.exp(to_end[b] - own_level)]
        lines.append(jnp.zeros((length - 3 * heads, length), jnp.float32))
        cols_ref[b * length : (b + 1) * length, :] = jnp.transpose(
            jnp.concatenate(lines, axis=0)
        )

    memory[...] = jnp.zeros_like(memory)
    normer[...] = jnp.zeros_like(normer)

    @pl.loop(0, blocks)
    def _(j):
        rows = pl.ds(pl.multiple_of(j * length, length), length)
        cols = cols_ref[rows, :]
        for h in range(heads):
            k = k_ref[rows, h * key_width : (h + 1) * key_width]
            v = v_ref[rows, h * value_width : (h + 1) * value_width]
            weighted = k.astype(jnp.float32) * cols[:, 2 * heads + h : 2 * heads + h + 1]
            memory[h] += lax.dot_general(
                weighted.astype(jnp.bfloat16),
                v,
                (((0,), (0,)), ((), ())),
                preferred_element_type=jnp.float32,
            )
            normer[h, :1, :] += jnp.sum(weighted, axis=0, keepdims=True)

    for h in range(heads):
        write_state(
            state_ref,
            h,
            memory[h],
            normer[h, :1, :],
            own_level[h : h + 1, :],
            own_total[h : h + 1, :],
        )
    swap.start()
    give_rows(1).start()
    give_cols.start()
    swap.wait_recv()

    @pl.when(odd == 0)
    def _():
        for h in range(heads):
            mem_a, norm_a, level_a, total_a = read_state(state_ref, h)
            mem_b, norm_b, level_b, total_b = read_state(held.at[0], h)
            out = join((mem_a, norm_a, level_a), (mem_b, norm_b, level_b), total_b)
            keep((pair_memory, pair_normer, pair_level.at[0]), h, out)
            pair_level[1, h] = jnp.broadcast_to(total_a + total_b, pair_level.shape[2:])

    @pl.when(odd == 1)
    def _():
        for h in range(heads):
            mem_a, norm_a, level_a, total_a = read_state(held.at[0], h)
            mem_b, norm_b, level_b, total_b = read_state(state_ref, h)
            out = join((mem_a, norm_a, level_a), (mem_b, norm_b, level_b), total_b)
            keep((pair_memory, pair_normer, pair_level.at[0]), h, out)
            pair_level[1, h] = jnp.broadcast_to(total_a + total_b, pair_level.shape[2:])

    started = jnp.minimum(FIRST_TICKS + NEXT_TICKS * place, up_ticks)

    @pl.loop(2, started)
    def _(n):
        up_sent(n - 2)
        up_tick(n)

    memory[...] = jnp.zeros_like(memory)
    normer[...] = jnp.zeros_like(normer)
    running[...] = jnp.full(running.shape, neg_large, jnp.float32)

    @pl.when(place > 0)
    def _():
        hand.wait_recv()
        for h in range(heads):
            mem, parts, level, total = read_state(held.at[1], h)
            keep(carried_refs, h, (mem, parts, level))

    @pl.when(place + 1 < line)
    def _():
        for h in range(heads):
            mem, norm, level = join(
                (memory[h], normer[h, :1, :], running[h, :1, :1]),
                (pair_memory[h], pair_normer[h, :1, :], pair_level[0, h, :1, :1]),
                pair_level[1, h, :1, :1],
            )
            write_state(handed, h, mem, norm, level, jnp.zeros_like(level))
        hand.start()

    @pl.when(odd == 1)
    def _():
        for h in range(heads):
            mem, norm, level, total = read_state(held.at[0], h)
            out = join(
                (memory[h], normer[h, :1, :], running[h, :1, :1]), (mem, norm, level), total
            )
            keep(carried_refs, h, out)

    scale = key_width ** (-0.5)
    causal = at_col <= at_row
    size = residual_ref.shape[0]
    per = size // length

    def block_copy(j, sender):
        at = pl.multiple_of(lax.rem(j, per) * length, length)
        width = gated.shape[1]
        return remote(
            gated.at[pl.ds(pl.multiple_of(j * length, length), length)],
            mine.at[sender, pl.ds(at, length)],
            block_send.at[j],
            block_recv.at[sender, lax.rem(j, per)],
            tp=j // per,
        )

    @pl.loop(0, blocks)
    def _(j):
        tick(started + j)

        @pl.when(j == blocks - 2)
        def _():
            for p in range(2):
                wo_copy(0, far, p, far).wait_recv()
                wo_copy(2, far, p, near).start()

        rows = pl.ds(pl.multiple_of(j * length, length), length)
        lanes = rows_ref[j]
        cols = cols_ref[rows, :]
        for h in range(heads):
            keys = slice(h * key_width, (h + 1) * key_width)
            vals = slice(h * value_width, (h + 1) * value_width)
            q = q_ref[rows, keys]
            k = k_ref[rows, keys]
            v = v_ref[rows, vals]
            before = running[h, :1, :1]
            total = lanes[heads + h : heads + h + 1, :1]
            shifted_log = jnp.where(causal, lanes[h : h + 1, :], -jnp.inf)
            top = jnp.maximum(jnp.max(shifted_log, axis=1, keepdims=True), before)
            raw = (
                lax.dot_general(
                    q, k, (((1,), (1,)), ((), ())), preferred_element_type=jnp.float32
                )
                * scale
            )
            scores = raw * jnp.exp(shifted_log - top)
            carry = jnp.exp(before - top) * scale
            state = memory[h]
            high = state.astype(jnp.bfloat16)
            low = (state - high.astype(jnp.float32)).astype(jnp.bfloat16)
            carried = jnp.dot(q, high, preferred_element_type=jnp.float32) + jnp.dot(
                q, low, preferred_element_type=jnp.float32
            )
            numerator = carry * carried + jnp.dot(
                scores.astype(jnp.bfloat16), v, preferred_element_type=jnp.float32
            )
            denominator = carry * jnp.sum(
                q.astype(jnp.float32) * normer[h, :1, :], axis=1, keepdims=True
            ) + jnp.sum(scores, axis=1, keepdims=True)
            level = cols[:, h : h + 1] + top
            value = numerator / jnp.maximum(jnp.abs(denominator), jnp.exp(-level))
            mean = jnp.mean(value * value, axis=1, keepdims=True)
            normed = value * lax.rsqrt(mean + eps) * gain_ref[h : h + 1, :]
            gate = normed * jax.nn.sigmoid(gate_ref[rows, vals].astype(jnp.float32))
            gated[rows, vals] = gate.astype(gated.dtype)
            last = jnp.max(jnp.maximum(lanes[h : h + 1, :], before), axis=1, keepdims=True)
            decay = jnp.exp(before - last)
            weighted = k.astype(jnp.float32) * jnp.exp(cols[:, heads + h : heads + h + 1] - last)
            memory[h] = decay * state + lax.dot_general(
                weighted.astype(jnp.bfloat16),
                v,
                (((0,), (0,)), ((), ())),
                preferred_element_type=jnp.float32,
            )
            normer[h, :1, :] = decay * normer[h, :1, :] + jnp.sum(
                weighted, axis=0, keepdims=True
            )
            running[h] = jnp.broadcast_to(last + total, running.shape[1:])

        @pl.when(j // per == tp)
        def _():
            at = pl.multiple_of(lax.rem(j, per) * length, length)
            mine[tp, pl.ds(at, length), :] = gated[rows, :]

        @pl.when(j // per != tp)
        def _():
            block_copy(j, tp).start()

    reached = started + blocks
    for p in range(2):
        wo_copy(1, near, p, near).wait_recv()
        wo_copy(2, opposite, p, near).wait_recv()

    @pl.loop(0, 4)
    def _(s):
        tick(reached + s)

        @pl.when(s != tp)
        def _():
            for p in range(per):
                block_copy(tp * per + p, s).wait_recv()

    reached = reached + 4

    def columns(i):
        return pl.ds(pl.multiple_of(i * wide, wide), wide)

    @pl.loop(0, model // wide)
    def _(i):
        total = jnp.zeros((size, wide), jnp.float32)
        for s in range(4):
            total += jnp.dot(
                mine[s],
                wo_full[s * wo_rows : (s + 1) * wo_rows, columns(i)],
                preferred_element_type=jnp.float32,
            )
        total_rows[:, columns(i)] = total

    pad = PAD_ROWS
    tokens = 8 * size
    row_pieces = rows_send.shape[1]
    row_step = size // row_pieces

    def row_copy(kind, y, owner, p, **to):
        at = pad + (y * 4 + owner) * size + p * row_step
        part = group.at[pl.ds(pl.multiple_of(at, pad), row_step)]
        return remote(part, part, rows_send.at[kind, p], rows_recv.at[kind, p], **to)

    @pl.when(place == 0)
    def _():
        group[0:pad, :] = jnp.zeros((pad, model), group.dtype)

    @pl.loop(0, row_pieces)
    def _(p):
        rows = pl.ds(pl.multiple_of(p * row_step, row_step), row_step)
        rounded = (residual_ref[rows, :].astype(jnp.float32) + total_rows[rows, :]).astype(
            jnp.bfloat16
        )
        stream[rows, :] = rounded
        x = rounded.astype(jnp.float32)
        normed = x * lax.rsqrt(jnp.mean(x * x, axis=-1, keepdims=True) + eps) * norm_gain_ref[...]
        at = pl.multiple_of(pad + (odd * 4 + tp) * size + p * row_step, pad)
        group[pl.ds(at, row_step), :] = normed.astype(jnp.bfloat16)
        row_copy(0, odd, tp, p, tp=far).start()
        row_copy(2, odd, tp, p, sp=partner).start()
        row_copy(1, odd, tp, p, tp=near).start()

    @pl.loop(0, row_pieces)
    def _(p):
        tick(reached + 2 * p)
        row_copy(0, odd, far, p, tp=far).wait_recv()
        row_copy(3, odd, far, p, tp=near).start()

        @pl.when(lax.rem(p, 2) == 0)
        def _():
            row_copy(6, odd, far, p, sp=partner).start()

        tick(reached + 2 * p + 1)
        row_copy(2, 1 - odd, tp, p, sp=partner).wait_recv()
        row_copy(4, 1 - odd, tp, p, tp=near).start()

        @pl.when(lax.rem(p, 2) == 1)
        def _():
            row_copy(6, 1 - odd, tp, p, tp=far).start()

    reached = reached + 2 * row_pieces

    @pl.loop(0, row_pieces)
    def _(p):
        tick(reached + p)
        row_copy(6, 1 - odd, far, p, sp=partner).wait_recv()
        row_copy(5, 1 - odd, far, p, tp=near).start()
        row_copy(1, odd, near, p, tp=near).wait_recv()
        row_copy(3, odd, opposite, p, tp=near).wait_recv()
        row_copy(4, 1 - odd, near, p, tp=near).wait_recv()

    reached = reached + row_pieces

    @pl.loop(0, row_pieces)
    def _(p):
        row_copy(5, 1 - odd, opposite, p, tp=near).wait_recv()

    edge = remote(
        group.at[pl.ds(tokens, pad)],
        group.at[pl.ds(0, pad)],
        edge_sem.at[0],
        edge_sem.at[1],
        sp=beyond(0),
    )

    @pl.when(place + 1 < line)
    def _():
        edge.start()

    @pl.loop(jnp.minimum(reached, up_ticks), up_ticks)
    def _(n):
        up_tick(n)

    reached = jnp.maximum(reached, up_ticks)
    early = up_ticks + 2 * down_pieces
    parts = 4
    part_rows = tokens // parts

    def silu(a):
        return a * jax.nn.sigmoid(a)

    @pl.loop(0, parts)
    def _(b):
        part = lax.rem(b + 1, parts)
        at = pl.multiple_of(part * part_rows, part_rows)
        window = pl.ds(at, part_rows + pad)
        outs = pl.ds(at, part_rows)

        @pl.when((b == parts - 1) & (place > 0))
        def _():
            edge.wait_recv()

        def conv(taps, width):
            return (
                taps[0:1, :] * up_tile[pad - 2 : pad - 2 + part_rows, width]
                + taps[1:2, :] * up_tile[pad - 1 : pad - 1 + part_rows, width]
                + taps[2:3, :] * up_tile[pad : pad + part_rows, width]
            )

        @pl.loop(0, tiles)
        def _(i):
            n = reached + b * (tiles + 1) + i

            @pl.when(n < early)
            def _():
                tick(n)

            lanes = pl.ds(pl.multiple_of(i * 2 * lane, 2 * lane), 2 * lane)
            up_tile[...] = jnp.dot(
                group[window, :], full_up[:, lanes], preferred_element_type=jnp.float32
            )
            taps_at = pl.ds(pl.multiple_of(odd * shift + i * lane, lane), lane)
            act = silu(conv(gate_taps_ref[:, taps_at], slice(0, lane))) * conv(
                value_taps_ref[:, taps_at], slice(lane, 2 * lane)
            )
            hidden[outs, pl.ds(pl.multiple_of(i * lane, lane), lane)] = act.astype(jnp.bfloat16)

        n = reached + b * (tiles + 1) + tiles

        @pl.when(n < early)
        def _():
            tick(n)

        up_tile[:, 0:lane] = jnp.dot(
            group[window, :], full_up[:, tail], preferred_element_type=jnp.float32
        )
        mid = slice(tiles * lane, (tiles + 1) * lane)
        low = lax.broadcasted_iota(jnp.int32, (3, lane), 1) < rest
        taps_a, taps_b = halves_of(gate_taps_ref[:, mid], value_taps_ref[:, mid], low)
        both = conv(jnp.where(odd == 0, taps_a, taps_b), slice(0, lane))
        act = silu(both) * pltpu.roll(both, rest, 1)
        hidden[outs, tiles * lane : tiles * lane + rest] = act[:, :rest].astype(jnp.bfloat16)

    @pl.loop(jnp.minimum(reached + parts * (tiles + 1), early), early)
    def _(n):
        tick(n)

    both_sides = jnp.minimum(place, line - 1 - place)

    def away(k):
        return jnp.where(k <= 2 * both_sides, (k + 1) // 2, k - both_sides)

    def unit(k):
        rising = jnp.where(place < line - 1 - place, 1, -1)
        way = jnp.where(k <= 2 * both_sides, 1 - 2 * lax.rem(k, 2), rising)
        return place + way * away(k)

    def sum_copy(stage, i, parity):
        src, dst = ((pair_out, pair_in), (second_out, second_in), (third_out, third_in))[stage]
        if stage == 0:
            to = {"tp": near}
        elif (stage == 1) == (parity == 0):
            to = {"tp": far}
        else:
            to = {"sp": partner}
        return remote(src.at[i], dst.at[i], sum_send.at[stage, i], sum_recv.at[stage, i], **to)

    def term(i, y, owner):
        rows = pl.ds(pl.multiple_of((y * 4 + owner) * size, size), size)
        return jnp.dot(hidden[rows, :], full_down[i], preferred_element_type=jnp.float32)

    def first_stage(i, parity):
        for y in range(2):
            for x in range(2):
                pair_out[i, 2 * y + x] = term(i, y, 2 * x + 1 - core).astype(jnp.bfloat16)
        sum_copy(0, i, parity).start()

    def second_stage(i, parity):
        for a in range(2):
            y, x = (a, 1 - chip) if parity == 0 else (1 - odd, a)
            pair_in_at = 2 * y + x
            second_out[i, a] = term(i, y, 2 * x + core).astype(jnp.bfloat16)
        for a in range(2):
            y, x = (a, chip) if parity == 0 else (odd, a)
            kept[i, a] = term(i, y, 2 * x + core)
        sum_copy(0, i, parity).wait_recv()
        for a in range(2):
            y, x = (a, 1 - chip) if parity == 0 else (1 - odd, a)
            second_out[i, a] = (
                second_out[i, a].astype(jnp.float32) + pair_in[i, 2 * y + x].astype(jnp.float32)
            ).astype(jnp.bfloat16)
        sum_copy(1, i, parity).start()
        for a in range(2):
            y, x = (a, chip) if parity == 0 else (odd, a)
            kept[i, a] += pair_in[i, 2 * y + x].astype(jnp.float32)

    def third_stage(i, parity):
        sum_copy(1, i, parity).wait_recv()
        own = odd if parity == 0 else chip
        third_out[i] = (kept[i, 1 - own] + second_in[i, 1 - own].astype(jnp.float32)).astype(
            jnp.bfloat16
        )
        sum_copy(2, i, parity).start()
        total_rows[:, columns(i)] = kept[i, own] + second_in[i, own].astype(jnp.float32)

    def last_stage(i, parity):
        sum_copy(2, i, parity).wait_recv()
        cols = columns(i)
        out_ref[:, cols] = (
            stream[:, cols].astype(jnp.float32)
            + (total_rows[:, cols] + third_in[i].astype(jnp.float32))
        ).astype(out_ref.dtype)

    def until(k):
        return up_ticks + down_pieces * (jnp.maximum(away(k), 1) + 1)

    @pl.loop(0, line)
    def _(k):
        @pl.when(k > 0)
        def _():
            @pl.loop(until(k - 1), until(k))
            def _(n):
                tick(n)

        for parity in range(2):
            first_stage(2 * unit(k) + parity, parity)
        for parity in range(2):
            second_stage(2 * unit(k) + parity, parity)

        @pl.when(k > 0)
        def _():
            for parity in range(2):
                third_stage(2 * unit(k - 1) + parity, parity)

    for parity in range(2):
        third_stage(2 * unit(line - 1) + parity, parity)

    @pl.loop(0, line)
    def _(k):
        for parity in range(2):
            last_stage(2 * unit(k) + parity, parity)

    swap.wait_send()

    @pl.when(place + 1 < line)
    def _():
        hand.wait_send()
        edge.wait_send()

    for p in range(2):
        give_rows(p).wait_send()
        for kind in range(3):
            wo_copy(kind, tp, p, near).wait_send()
    give_cols.wait_send()

    @pl.loop(0, blocks)
    def _(j):
        @pl.when(j // per != tp)
        def _():
            block_copy(j, tp).wait_send()

    @pl.loop(0, row_pieces)
    def _(p):
        for kind in range(7):
            row_copy(kind, odd, tp, p, tp=near).wait_send()

    @pl.loop(0, count)
    def _(i):
        for stage in range(3):
            sum_copy(stage, i, 0).wait_send()

    @pl.loop(started - 2, up_ticks)
    def _(n):
        up_sent(n)

    @pl.loop(0, line - 1)
    def _(t):
        for w in range(2):

            @pl.when(sends(w, t))
            def _():
                for m in range(down_pieces):
                    down_hop(w, t, m).wait_send()


FIRST_TICKS = 4
NEXT_TICKS = 2
UP_PIECES = 8
DOWN_PIECES = 4
PAD_ROWS = 16


def one_kernel_fits(rows, gate_w, down_w):
    count = lax.axis_size("sp")
    return (
        lax.axis_size("tp") == 4
        and count >= 4
        and count % 2 == 0
        and 2 * gate_w.shape[0] % (16 * UP_PIECES) == 0
        and gate_w.shape[1] % 256 == 128
        and down_w.shape[0] % (16 * DOWN_PIECES) == 0
        and down_w.shape[1] % 128 == 0
        and rows % (2 * BLOCK) == 0
    )


def layer(q, k, v, gates, input_log, forget_log, gain, wo, residual, norm_gain, gate_w, value_w, down_w, gate_taps, value_taps):
    count = lax.axis_size("sp")
    line = count // 2
    heads = input_log.shape[1]
    tokens = q.shape[0]
    key_width = q.shape[1] // heads
    value_width = v.shape[1] // heads
    span = key_width + STATE_PAD
    model = wo.shape[1]
    rows = residual.shape[0]
    lane = 128
    half_width = gate_w.shape[1] // 2
    tiles = half_width // lane
    wide = down_w.shape[1]
    row_pieces = 4
    blocks = tokens // BLOCK
    logs = jnp.concatenate([input_log.T, forget_log.T], axis=0)
    vmem = pl.BlockSpec(memory_space=pltpu.VMEM)
    hbm = pl.BlockSpec(memory_space=pl.ANY)
    low, full = jnp.bfloat16, jnp.float32
    dma = pltpu.SemaphoreType.DMA
    return pl.pallas_call(
        functools.partial(layer_kernel, count, heads, UP_PIECES, DOWN_PIECES),
        out_shape=jax.ShapeDtypeStruct(residual.shape, low),
        in_specs=[vmem] * 10 + [hbm] * 4,
        out_specs=vmem,
        scratch_shapes=[
            pltpu.VMEM((blocks, 8, BLOCK), full),
            pltpu.VMEM((tokens, BLOCK), full),
            pltpu.VMEM((heads * span, value_width), low),
            pltpu.VMEM((2, heads * span, value_width), low),
            pltpu.VMEM((heads, key_width, value_width), full),
            pltpu.VMEM((heads, 8, key_width), full),
            pltpu.VMEM((heads, 8, 128), full),
            pltpu.VMEM((heads, key_width, value_width), full),
            pltpu.VMEM((heads, 8, key_width), full),
            pltpu.VMEM((2, heads, 8, 128), full),
            pltpu.VMEM((heads * span, value_width), low),
            pltpu.VMEM((tokens, v.shape[1]), low),
            pltpu.VMEM((4, rows, v.shape[1]), low),
            pltpu.VMEM((model, model), low),
            pltpu.VMEM((2, gate_w.shape[0], lane), low),
            pltpu.VMEM((gate_w.shape[0], 2 * half_width), low),
            pltpu.VMEM((half_width, wide), low),
            pltpu.VMEM((model, 2 * half_width), low),
            pltpu.VMEM((count, half_width, wide), low),
            pltpu.VMEM((rows, model), full),
            pltpu.VMEM((rows, model), low),
            pltpu.VMEM((PAD_ROWS + 2 * tokens, model), low),
            pltpu.VMEM((PAD_ROWS + tokens // 2, 2 * lane), full),
            pltpu.VMEM((2 * tokens, half_width), low),
            pltpu.VMEM((count, 4, rows, wide), low),
            pltpu.VMEM((count, 4, rows, wide), low),
            pltpu.VMEM((count, 2, rows, wide), low),
            pltpu.VMEM((count, 2, rows, wide), low),
            pltpu.VMEM((count, rows, wide), low),
            pltpu.VMEM((count, rows, wide), low),
            pltpu.VMEM((count, 2, rows, wide), full),
            dma((4 * tiles + 7,)),
            dma((2, 3, 2)),
            dma((2, 3)),
            dma((2,)),
            dma((2,)),
            dma((2, line - 1, UP_PIECES)),
            dma((2, line - 1, UP_PIECES)),
            dma((2, line - 1, DOWN_PIECES)),
            dma((2, line - 1, DOWN_PIECES)),
            dma((blocks,)),
            dma((4, rows // BLOCK)),
            dma((7, row_pieces)),
            dma((7, row_pieces)),
            dma((3, count)),
            dma((3, count)),
            dma((2,)),
        ],
        compiler_params=pltpu.CompilerParams(
            collective_id=0, has_side_effects=True, vmem_limit_bytes=63 * 1024 * 1024
        ),
        cost_estimate=pl.CostEstimate(
            flops=30_000_000_000, bytes_accessed=8 * v.size, transcendentals=0
        ),
    )(
        logs,
        q,
        k,
        v,
        gates,
        gain,
        residual,
        norm_gain[None, :],
        gate_taps,
        value_taps,
        wo,
        gate_w,
        value_w,
        down_w,
    )


def local(
    residual_entry_input,
    query_matrix_rows,
    key_matrix_rows,
    value_matrix_rows,
    output_gate_logits,
    input_gate_logits,
    forget_gate_logits,
    forget_decay_offset,
    head_norm_gain,
    cell_output_weight,
    feedforward_norm_gain,
    gate_up_weight,
    value_up_weight,
    gate_filter_taps,
    value_filter_taps,
    down_projection_weight,
):
    input_log, forget_log = gate_log_values(
        input_gate_logits, forget_gate_logits, forget_decay_offset
    )
    if one_kernel_fits(residual_entry_input.shape[0], gate_up_weight, down_projection_weight):
        return layer(
            query_matrix_rows,
            key_matrix_rows,
            value_matrix_rows,
            output_gate_logits,
            input_log,
            forget_log,
            head_norm_gain,
            cell_output_weight,
            residual_entry_input,
            feedforward_norm_gain,
            gate_up_weight,
            value_up_weight,
            down_projection_weight,
            gate_filter_taps,
            value_filter_taps,
        )
    whole_gate = lax.all_gather(gate_up_weight, "sp", axis=0, tiled=True)
    whole_down = lax.all_gather(down_projection_weight, "sp", axis=1, tiled=True)
    gated_rows = cell(
        query_matrix_rows,
        key_matrix_rows,
        value_matrix_rows,
        output_gate_logits,
        input_log,
        forget_log,
        head_norm_gain,
    )
    mixed_rows = product_rows(gated_rows, cell_output_weight, 2)
    stream_wide = residual_entry_input.astype(jnp.float32) + mixed_rows
    stream = stream_wide.astype(jnp.bfloat16)
    stream_wide = lax.optimization_barrier(stream).astype(jnp.float32)
    normed_rows = (
        stream_wide
        * lax.rsqrt(jnp.mean(stream_wide * stream_wide, axis=-1, keepdims=True) + eps)
        * feedforward_norm_gain[None, :]
    ).astype(jnp.bfloat16)
    group_rows = gather_rows(normed_rows)
    group_rows, value_shard = lax.optimization_barrier((group_rows, value_up_weight))
    whole_value = walk_gather(value_shard, 2)
    earlier_rows = shifted(group_rows[-2:], "sp", 1)
    window = jnp.concatenate([earlier_rows, group_rows], axis=0)
    up_gate = jnp.dot(
        window,
        whole_gate,
        preferred_element_type=jnp.float32,
    )
    up_value = jnp.dot(
        window,
        whole_value,
        preferred_element_type=jnp.float32,
    )
    conv_g = (
        gate_filter_taps[0][None, :] * up_gate[:-2]
        + gate_filter_taps[1][None, :] * up_gate[1:-1]
        + gate_filter_taps[2][None, :] * up_gate[2:]
    )
    conv_v = (
        value_filter_taps[0][None, :] * up_value[:-2]
        + value_filter_taps[1][None, :] * up_value[1:-1]
        + value_filter_taps[2][None, :] * up_value[2:]
    )
    hidden = (jax.nn.silu(conv_g) * conv_v).astype(jnp.bfloat16)
    ffn_rows = product_rows(hidden, whole_down, 3)
    return (stream_wide + ffn_rows).astype(jnp.bfloat16)


def solution(mesh):
    in_specs = (
        P(("sp", "tp"), None),
        P("sp", "tp"),
        P("sp", "tp"),
        P("sp", "tp"),
        P("sp", "tp"),
        P("sp", "tp"),
        P("sp", "tp"),
        P("sp", "tp"),
        P("tp", None),
        P("tp", None),
        P(),
        P("sp", "tp"),
        P("sp", "tp"),
        P(None, "tp"),
        P(None, "tp"),
        P("tp", "sp"),
    )
    out_specs = P(("sp", "tp"), None)
    return jax.shard_map(local, mesh=mesh, in_specs=in_specs, out_specs=out_specs, check_vma=False)
```

```python
import functools

import jax
import jax.numpy as jnp
from jax import lax
from jax.experimental import pallas as pl
from jax.experimental.pallas import tpu as pltpu
from jax.sharding import PartitionSpec as P

BLOCK = 128


eps = 1e-06
neg_large = -1e30


def shifted(x, axis, by):
    count = lax.axis_size(axis)
    pairs = [(i, i + by) for i in range(count) if 0 <= i + by < count]
    return lax.ppermute(x, axis, pairs)


def gate_log_values(input_gate_logits, forget_gate_logits, forget_decay_offset):
    input_log_value = 15.0 * jnp.tanh(input_gate_logits / 15.0)
    forget_log_sigmoid = (
        jax.nn.log_sigmoid(15.0 * jnp.tanh(forget_gate_logits / 15.0)) + forget_decay_offset
    )
    return (input_log_value, forget_log_sigmoid)


STATE_PAD = 16
MESH = pl.DeviceIdType.MESH


def cell_kernel(
    count,
    heads,
    state_ref,
    q_ref,
    k_ref,
    v_ref,
    gate_ref,
    gain_ref,
    rows_ref,
    cols_ref,
    out_ref,
    held,
    memory,
    normer,
    running,
    send_sem,
    recv_sem,
):
    me = lax.axis_index("sp")
    barrier = pltpu.get_barrier_semaphore()
    for d in range(1, count):
        pl.semaphore_signal(
            barrier, inc=1, device_id={"sp": lax.rem(me + d, count)}, device_id_type=MESH
        )
    pl.semaphore_wait(barrier, count - 1)

    def push(d, target, slot):
        return pltpu.make_async_remote_copy(
            src_ref=state_ref,
            dst_ref=held.at[slot],
            send_sem=send_sem.at[d],
            recv_sem=recv_sem.at[d],
            device_id={"sp": target},
            device_id_type=MESH,
        )

    for d in range(1, count):

        @pl.when(me + d < count)
        def _():
            push(d, me + d, me).start()

    memory[...] = jnp.zeros_like(memory)
    normer[...] = jnp.zeros_like(normer)
    running[...] = jnp.full(running.shape, neg_large, jnp.float32)
    for d in range(1, count):

        @pl.when(me - d >= 0)
        def _():
            push(d, lax.rem(me + d, count), me - d).wait_recv()

    key_width = memory.shape[1]
    value_width = memory.shape[2]
    span = key_width + STATE_PAD

    @pl.loop(0, me)
    def _(j):
        for h in range(heads):
            low = h * span
            extra = held[j, low + key_width : low + span, :].astype(jnp.float32)
            total = extra[2:3, :1] + extra[3:4, :1]
            level = extra[4:5, :1] + extra[5:6, :1]
            before = running[h, :1, :1]
            after = jnp.maximum(total + before, level)
            one = jnp.exp(total + before - after)
            two = jnp.exp(level - after)
            memory[h] = one * memory[h] + two * held[j, low : low + key_width, :].astype(
                jnp.float32
            )
            parts = extra[0:1, :key_width] + extra[1:2, :key_width]
            normer[h, :1, :] = one * normer[h, :1, :] + two * parts
            running[h] = jnp.broadcast_to(after, running.shape[1:])

    length = BLOCK
    scale = key_width ** (-0.5)
    at_row = lax.broadcasted_iota(jnp.int32, (length, length), 0)
    at_col = lax.broadcasted_iota(jnp.int32, (length, length), 1)
    causal = at_col <= at_row

    @pl.loop(0, q_ref.shape[0] // length)
    def _(j):
        rows = pl.ds(pl.multiple_of(j * length, length), length)
        lanes = rows_ref[j]
        cols = cols_ref[rows, :]
        for h in range(heads):
            keys = slice(h * key_width, (h + 1) * key_width)
            vals = slice(h * value_width, (h + 1) * value_width)
            q = q_ref[rows, keys]
            k = k_ref[rows, keys]
            v = v_ref[rows, vals]
            before = running[h, :1, :1]
            total = lanes[heads + h : heads + h + 1, :1]
            shifted_log = jnp.where(causal, lanes[h : h + 1, :], -jnp.inf)
            top = jnp.maximum(jnp.max(shifted_log, axis=1, keepdims=True), before)
            raw = (
                lax.dot_general(
                    q, k, (((1,), (1,)), ((), ())), preferred_element_type=jnp.float32
                )
                * scale
            )
            scores = raw * jnp.exp(shifted_log - top)
            carry = jnp.exp(before - top) * scale
            state = memory[h]
            high = state.astype(jnp.bfloat16)
            low = (state - high.astype(jnp.float32)).astype(jnp.bfloat16)
            carried = jnp.dot(q, high, preferred_element_type=jnp.float32) + jnp.dot(
                q, low, preferred_element_type=jnp.float32
            )
            numerator = carry * carried + jnp.dot(
                scores.astype(jnp.bfloat16), v, preferred_element_type=jnp.float32
            )
            denominator = carry * jnp.sum(
                q.astype(jnp.float32) * normer[h, :1, :], axis=1, keepdims=True
            ) + jnp.sum(scores, axis=1, keepdims=True)
            level = cols[:, h : h + 1] + top
            value = numerator / jnp.maximum(jnp.abs(denominator), jnp.exp(-level))
            mean = jnp.mean(value * value, axis=1, keepdims=True)
            normed = value * lax.rsqrt(mean + eps) * gain_ref[h : h + 1, :]
            gated = normed * jax.nn.sigmoid(gate_ref[rows, vals].astype(jnp.float32))
            out_ref[rows, vals] = gated.astype(out_ref.dtype)
            last = jnp.max(jnp.maximum(lanes[h : h + 1, :], before), axis=1, keepdims=True)
            decay = jnp.exp(before - last)
            weighted = k.astype(jnp.float32) * jnp.exp(cols[:, heads + h : heads + h + 1] - last)
            memory[h] = decay * state + lax.dot_general(
                weighted.astype(jnp.bfloat16),
                v,
                (((0,), (0,)), ((), ())),
                preferred_element_type=jnp.float32,
            )
            normer[h, :1, :] = decay * normer[h, :1, :] + jnp.sum(
                weighted, axis=0, keepdims=True
            )
            running[h] = jnp.broadcast_to(last + total, running.shape[1:])

    for d in range(1, count):

        @pl.when(me + d < count)
        def _():
            push(d, me + d, me).wait_send()


def halves(x):
    high = lax.reduce_precision(x, 8, 7)
    return (high.astype(jnp.bfloat16), (x - high).astype(jnp.bfloat16))


def cell_parts(q, k, v, input_log, forget_log):
    heads = input_log.shape[1]
    tokens = q.shape[0]
    key_width = q.shape[1] // heads
    value_width = v.shape[1] // heads
    count = lax.axis_size("sp")
    blocks = tokens // BLOCK
    f = forget_log.reshape(blocks, BLOCK, heads)
    tri = jnp.tril(jnp.ones((BLOCK, BLOCK), jnp.float32))
    within = jnp.einsum("ts,bsh->bth", tri, f, precision=lax.Precision.HIGHEST)
    each = within[:, -1, :]
    later = jnp.triu(jnp.ones((blocks, blocks), jnp.float32), 1)
    after = jnp.einsum("bc,ch->bh", later, each, precision=lax.Precision.HIGHEST)
    total = jnp.sum(each, axis=0)
    shifted_log = input_log.reshape(blocks, BLOCK, heads) - within
    to_end = (shifted_log + (each + after)[:, None, :]).reshape(tokens, heads)
    level = jnp.max(to_end, axis=0)
    weighted = k.reshape(tokens, heads, key_width).astype(jnp.float32) * jnp.exp(to_end - level)[
        :, :, None
    ]
    memory = jnp.einsum(
        "shd,shv->hdv",
        weighted.astype(jnp.bfloat16),
        v.reshape(tokens, heads, value_width),
        preferred_element_type=jnp.float32,
    ).astype(jnp.bfloat16)
    normer = jnp.sum(weighted, axis=0)
    wide = (heads, 1, value_width)
    lines = [
        jnp.pad(part, ((0, 0), (0, value_width - key_width)))[:, None, :]
        for part in halves(normer)
    ]
    for scalar in (total, level):
        lines += [jnp.broadcast_to(part[:, None, None], wide) for part in halves(scalar)]
    lines.append(jnp.zeros((heads, STATE_PAD - len(lines), value_width), jnp.bfloat16))
    span = key_width + STATE_PAD
    state = jnp.concatenate([memory] + lines, axis=1).reshape(heads * span, value_width)
    lanes = jnp.concatenate(
        [
            jnp.transpose(shifted_log, (0, 2, 1)),
            jnp.broadcast_to(each[:, :, None], (blocks, heads, BLOCK)),
        ],
        axis=1,
    )
    cols = jnp.concatenate([within, shifted_log], axis=2).reshape(tokens, 2 * heads)
    return state, lanes, cols


def cell(q, k, v, gates, input_log, forget_log, gain):
    heads = input_log.shape[1]
    key_width = q.shape[1] // heads
    value_width = v.shape[1] // heads
    count = lax.axis_size("sp")
    span = key_width + STATE_PAD
    state, lanes, cols = cell_parts(q, k, v, input_log, forget_log)
    vmem = pl.BlockSpec(memory_space=pltpu.VMEM)
    return pl.pallas_call(
        functools.partial(cell_kernel, count, heads),
        out_shape=jax.ShapeDtypeStruct(v.shape, jnp.bfloat16),
        in_specs=[vmem] * 8,
        out_specs=vmem,
        scratch_shapes=[
            pltpu.VMEM((count, heads * span, value_width), jnp.bfloat16),
            pltpu.VMEM((heads, key_width, value_width), jnp.float32),
            pltpu.VMEM((heads, 8, key_width), jnp.float32),
            pltpu.VMEM((heads, 8, 128), jnp.float32),
            pltpu.SemaphoreType.DMA((count,)),
            pltpu.SemaphoreType.DMA((count,)),
        ],
        compiler_params=pltpu.CompilerParams(
            collective_id=0, has_side_effects=True, vmem_limit_bytes=40 * 1024 * 1024
        ),
        cost_estimate=pl.CostEstimate(
            flops=30_000_000_000, bytes_accessed=8 * v.size, transcendentals=0
        ),
    )(state, q, k, v, gates, gain, lanes, cols)


def rows_kernel(pieces, x_ref, out_ref, own_sem, near_send, near_recv, far_send, far_recv, on_send, on_recv):
    me = lax.axis_index("tp")
    near = me + 1 - 2 * lax.rem(me, 2)
    far = lax.rem(me + 2, 4)
    opposite = lax.rem(near + 2, 4)
    size = x_ref.shape[0]
    step = size // pieces
    barrier = pltpu.get_barrier_semaphore()
    for other in (near, far):
        pl.semaphore_signal(barrier, inc=1, device_id={"tp": other}, device_id_type=MESH)
    pl.semaphore_wait(barrier, 2)

    def at(owner, p):
        return out_ref.at[pl.ds(pl.multiple_of(owner * size + p * step, step), step)]

    def send(src, dst, sems, p, target):
        return pltpu.make_async_remote_copy(
            src_ref=src,
            dst_ref=dst,
            send_sem=sems[0].at[p],
            recv_sem=sems[1].at[p],
            device_id={"tp": target},
            device_id_type=MESH,
        )

    mine = [x_ref.at[pl.ds(p * step, step)] for p in range(pieces)]
    far_out = [send(mine[p], at(me, p), (far_send, far_recv), p, far) for p in range(pieces)]
    near_out = [send(mine[p], at(me, p), (near_send, near_recv), p, near) for p in range(pieces)]
    far_in = [send(mine[p], at(far, p), (far_send, far_recv), p, far) for p in range(pieces)]
    near_in = [send(mine[p], at(near, p), (near_send, near_recv), p, near) for p in range(pieces)]
    onward = [send(at(far, p), at(far, p), (on_send, on_recv), p, near) for p in range(pieces)]
    on_in = [
        send(at(opposite, p), at(opposite, p), (on_send, on_recv), p, near)
        for p in range(pieces)
    ]
    for p in range(pieces):
        far_out[p].start()
    for p in range(pieces):
        near_out[p].start()
    whole = pl.ds(pl.multiple_of(me * size, size), size)
    own = pltpu.make_async_copy(x_ref, out_ref.at[whole], own_sem)
    own.start()
    for p in range(pieces):
        far_in[p].wait_recv()
        onward[p].start()
    own.wait()
    for p in range(pieces):
        near_in[p].wait_recv()
        on_in[p].wait_recv()
    for p in range(pieces):
        far_out[p].wait_send()
        near_out[p].wait_send()
        onward[p].wait_send()


def gather_rows(x):
    if lax.axis_size("tp") != 4:
        return lax.all_gather(x, "tp", axis=0, tiled=True)
    pieces = 4
    vmem = pl.BlockSpec(memory_space=pltpu.VMEM)
    return pl.pallas_call(
        functools.partial(rows_kernel, pieces),
        out_shape=jax.ShapeDtypeStruct((4 * x.shape[0], x.shape[1]), x.dtype),
        in_specs=[vmem],
        out_specs=vmem,
        scratch_shapes=[pltpu.SemaphoreType.DMA] + [pltpu.SemaphoreType.DMA((pieces,))] * 6,
        compiler_params=pltpu.CompilerParams(
            collective_id=1, has_side_effects=True, vmem_limit_bytes=16 * 1024 * 1024
        ),
        cost_estimate=pl.CostEstimate(
            flops=30_000_000_000, bytes_accessed=4 * x.size, transcendentals=0
        ),
    )(x)


def product_kernel(
    pieces,
    x_ref,
    w_ref,
    out_ref,
    pair_out,
    pair_in,
    far_out,
    far_in,
    near_out,
    near_in,
    pair_send,
    pair_recv,
    far_send,
    far_recv,
    near_send,
    near_recv,
):
    me = lax.axis_index("tp")
    near = me + 1 - 2 * lax.rem(me, 2)
    far = lax.rem(me + 2, 4)
    opposite = lax.rem(near + 2, 4)
    size = out_ref.shape[0]
    step = out_ref.shape[1] // pieces
    barrier = pltpu.get_barrier_semaphore()
    for other in (near, far):
        pl.semaphore_signal(barrier, inc=1, device_id={"tp": other}, device_id_type=MESH)
    pl.semaphore_wait(barrier, 2)

    def columns(p):
        return pl.ds(pl.multiple_of(p * step, step), step)

    def term(owner, p):
        rows = pl.ds(pl.multiple_of(owner * size, size), size)
        return jnp.dot(x_ref[rows, :], w_ref[:, columns(p)], preferred_element_type=jnp.float32)

    def send(src, dst, sems, p, target):
        return pltpu.make_async_remote_copy(
            src_ref=src.at[p],
            dst_ref=dst.at[p],
            send_sem=sems[0].at[p],
            recv_sem=sems[1].at[p],
            device_id={"tp": target},
            device_id_type=MESH,
        )

    def pair(p):
        return send(pair_out, pair_in, (pair_send, pair_recv), p, near)

    def across(p):
        return send(far_out, far_in, (far_send, far_recv), p, far)

    def beside(p):
        return send(near_out, near_in, (near_send, near_recv), p, near)

    @pl.loop(0, pieces)
    def _(p):
        pair_out[p] = term(opposite, p).astype(jnp.bfloat16)
        pair(p).start()
        mine = term(far, p)
        pair(p).wait_recv()
        far_out[p] = (mine + pair_in[p].astype(jnp.float32)).astype(jnp.bfloat16)
        across(p).start()

    @pl.loop(0, pieces)
    def _(p):
        near_out[p] = term(near, p).astype(jnp.bfloat16)
        beside(p).start()

    @pl.loop(0, pieces)
    def _(p):
        own = term(me, p)
        beside(p).wait_recv()
        out_ref[:, columns(p)] = own + near_in[p].astype(jnp.float32)

    @pl.loop(0, pieces)
    def _(p):
        across(p).wait_recv()
        out_ref[:, columns(p)] += far_in[p].astype(jnp.float32)

    @pl.loop(0, pieces)
    def _(p):
        pair(p).wait_send()
        across(p).wait_send()
        beside(p).wait_send()


def product_rows(x, w, tag):
    if lax.axis_size("tp") != 4:
        partial = jnp.dot(x, w, preferred_element_type=jnp.float32).astype(jnp.bfloat16)
        return lax.psum_scatter(partial, "tp", scatter_dimension=0, tiled=True).astype(
            jnp.float32
        )
    pieces = 4
    rows, wide = x.shape[0] // 4, w.shape[1]
    vmem = pl.BlockSpec(memory_space=pltpu.VMEM)
    slots = pltpu.VMEM((pieces, rows, wide // pieces), jnp.bfloat16)
    return pl.pallas_call(
        functools.partial(product_kernel, pieces),
        out_shape=jax.ShapeDtypeStruct((rows, wide), jnp.float32),
        in_specs=[vmem] * 2,
        out_specs=vmem,
        scratch_shapes=[slots] * 6 + [pltpu.SemaphoreType.DMA((pieces,))] * 6,
        compiler_params=pltpu.CompilerParams(
            collective_id=tag, has_side_effects=True, vmem_limit_bytes=40 * 1024 * 1024
        ),
        cost_estimate=pl.CostEstimate(
            flops=30_000_000_000, bytes_accessed=2 * w.size, transcendentals=0
        ),
    )(x, w)


def walk_kernel(count, pieces, x_ref, out_ref, own_sem, send_sem, recv_sem):
    me = lax.axis_index("sp")
    odd = lax.rem(me, 2)
    place = me // 2 + odd * (count - 1 - 2 * (me // 2))
    size = x_ref.shape[0]
    step = size // (2 * pieces)

    def index(position):
        position = lax.rem(position + 2 * count, count)
        back = position // (count // 2)
        return (1 - back) * 2 * position + back * (2 * (count - 1 - position) + 1)

    ways = (1, -1)
    barrier = pltpu.get_barrier_semaphore()
    for way in ways:
        pl.semaphore_signal(
            barrier, inc=1, device_id={"sp": index(place + way)}, device_id_type=MESH
        )
    pl.semaphore_wait(barrier, 2)

    def hop(w, t, p, age, own=False):
        inner = (w * pieces + p) * step
        owner = index(place - ways[w] * age)
        dst = out_ref.at[pl.ds(pl.multiple_of(owner * size + inner, step), step)]
        return pltpu.make_async_remote_copy(
            src_ref=x_ref.at[pl.ds(inner, step)] if own else dst,
            dst_ref=dst,
            send_sem=send_sem.at[w, p, t],
            recv_sem=recv_sem.at[w, p, t],
            device_id={"sp": index(place + ways[w])},
            device_id_type=MESH,
        )

    for p in range(pieces):
        for w in range(2):
            hop(w, 0, p, 0, True).start()
    whole = pl.ds(pl.multiple_of(me * size, size), size)
    own = pltpu.make_async_copy(x_ref, out_ref.at[whole], own_sem)
    own.start()

    @pl.loop(1, count - 1)
    def _(t):
        for p in range(pieces):
            for w in range(2):
                hop(w, t - 1, p, t).wait_recv()
                hop(w, t, p, t).start()

    own.wait()
    for p in range(pieces):
        for w in range(2):
            hop(w, count - 2, p, count - 1).wait_recv()
            hop(w, 0, p, 0, True).wait_send()

    @pl.loop(1, count - 1)
    def _(t):
        for p in range(pieces):
            for w in range(2):
                hop(w, t, p, t).wait_send()


def walk_gather(x, pieces):
    count = lax.axis_size("sp")
    if count % 2 or count < 4 or x.shape[0] % (32 * pieces):
        return lax.all_gather(x, "sp", axis=0, tiled=True)
    vmem = pl.BlockSpec(memory_space=pltpu.VMEM)
    return pl.pallas_call(
        functools.partial(walk_kernel, count, pieces),
        out_shape=jax.ShapeDtypeStruct((count * x.shape[0], x.shape[1]), x.dtype),
        in_specs=[vmem],
        out_specs=vmem,
        scratch_shapes=[pltpu.SemaphoreType.DMA]
        + [pltpu.SemaphoreType.DMA((2, pieces, count - 1))] * 2,
        compiler_params=pltpu.CompilerParams(
            collective_id=4, has_side_effects=True, vmem_limit_bytes=16 * 1024 * 1024
        ),
        cost_estimate=pl.CostEstimate(
            flops=30_000_000_000, bytes_accessed=count * x.size, transcendentals=0
        ),
    )(x)


def layer_kernel(
    count,
    heads,
    up_pieces,
    down_pieces,
    logs_ref,
    q_ref,
    k_ref,
    v_ref,
    gate_ref,
    gain_ref,
    residual_ref,
    norm_gain_ref,
    gate_taps_ref,
    value_taps_ref,
    wo_ref,
    gate_w_ref,
    value_w_ref,
    down_w_ref,
    out_ref,
    rows_ref,
    cols_ref,
    state_ref,
    held,
    memory,
    normer,
    running,
    pair_memory,
    pair_normer,
    pair_level,
    handed,
    gated,
    mine,
    wo_full,
    middle,
    give_up,
    give_down,
    full_up,
    full_down,
    total_rows,
    stream,
    group,
    up_tile,
    hidden,
    pair_out,
    pair_in,
    second_out,
    second_in,
    third_out,
    third_in,
    kept,
    blocks_of,
    load_sem,
    wo_sem,
    give_sem,
    state_send,
    state_recv,
    up_send,
    up_recv,
    down_send,
    down_recv,
    block_send,
    block_recv,
    rows_send,
    rows_recv,
    sum_send,
    sum_recv,
    edge_sem,
):
    me = lax.axis_index("sp")
    tp = lax.axis_index("tp")
    core = lax.rem(tp, 2)
    chip = tp // 2
    near = tp + 1 - 2 * core
    far = lax.rem(tp + 2, 4)
    opposite = lax.rem(near + 2, 4)
    odd = lax.rem(me, 2)
    partner = me + 1 - 2 * odd
    line = count // 2
    place = me // 2
    model = full_up.shape[0]
    lane = 128
    up_rows = model // count
    up_step = 2 * up_rows // up_pieces
    half_width = full_down.shape[1]
    tiles = half_width // lane
    rest = half_width - tiles * lane
    wide = full_down.shape[2]
    down_step = 2 * half_width // down_pieces

    barrier = pltpu.get_barrier_semaphore()
    for other in (near, far, opposite):
        pl.semaphore_signal(barrier, inc=1, device_id={"tp": other}, device_id_type=MESH)
    for other in (partner, lax.rem(me + 2, count), lax.rem(me + count - 2, count)):
        pl.semaphore_signal(barrier, inc=1, device_id={"sp": other}, device_id_type=MESH)

    own_up = pl.ds(pl.multiple_of(me * up_rows, up_rows), up_rows)
    wo_rows = wo_ref.shape[0]
    wo_own = pl.ds(pl.multiple_of(tp * wo_rows, wo_rows), wo_rows)
    loads = []

    def load(src, dst):
        loads.append(pltpu.make_async_copy(src, dst, load_sem.at[len(loads)]))

    shift = tiles * lane + 2 * rest
    for i in range(tiles):
        for a, w_ref in enumerate((gate_w_ref, value_w_ref)):
            lanes = pl.ds((2 * i + a) * lane, lane)
            for to, y in ((full_up.at[own_up, lanes], odd), (give_up.at[:, lanes], 1 - odd)):
                at = pl.multiple_of(y * shift + i * lane, lane)
                load(w_ref.at[:, pl.ds(at, lane)], to)
    for a, w_ref in enumerate((gate_w_ref, value_w_ref)):
        load(w_ref.at[:, pl.ds(tiles * lane, lane)], middle.at[a])
    for to, y in ((full_down.at[me], odd), (give_down, 1 - odd)):
        at = pl.multiple_of(y * shift, rest)
        load(down_w_ref.at[pl.ds(at, tiles * lane)], to.at[pl.ds(0, tiles * lane)])
        at = pl.multiple_of(tiles * lane + y * rest, rest)
        load(down_w_ref.at[pl.ds(at, rest)], to.at[pl.ds(tiles * lane, rest)])
    load(wo_ref, wo_full.at[wo_own])
    for one in loads:
        one.start()
    pl.semaphore_wait(barrier, 6)
    for one in loads:
        one.wait()

    def remote(src, dst, send_sem, recv_sem, **to):
        return pltpu.make_async_remote_copy(
            src_ref=src,
            dst_ref=dst,
            send_sem=send_sem,
            recv_sem=recv_sem,
            device_id=to,
            device_id_type=MESH,
        )

    at_lane = lax.broadcasted_iota(jnp.int32, (up_rows, lane), 1)
    first_half = at_lane < rest

    def halves_of(g, v, low):
        a = jnp.where(low, g, pltpu.roll(v, rest, 1))
        b = jnp.where(low, pltpu.roll(g, rest, 1), v)
        return a, b

    mid_a, mid_b = halves_of(
        middle[0].astype(jnp.float32), middle[1].astype(jnp.float32), first_half
    )
    tail = slice(2 * tiles * lane, 2 * tiles * lane + lane)
    full_up[own_up, tail] = jnp.where(odd == 0, mid_a, mid_b).astype(jnp.bfloat16)
    give_up[:, tail] = jnp.where(odd == 0, mid_b, mid_a).astype(jnp.bfloat16)

    give_step = up_rows // 2

    def give_rows(p):
        at = pl.multiple_of(me * up_rows + p * give_step, give_step)
        return remote(
            give_up.at[pl.ds(p * give_step, give_step)],
            full_up.at[pl.ds(at, give_step)],
            give_sem.at[0, p],
            give_sem.at[1, p],
            sp=partner,
        )

    give_cols = remote(give_down, full_down.at[me], give_sem.at[0, 2], give_sem.at[1, 2], sp=partner)
    wo_pieces = wo_sem.shape[2]
    wo_step = wo_rows // 2 // wo_pieces

    def wo_copy(kind, owner, y, s, **to):
        at = pl.multiple_of(owner * wo_rows + (y * wo_pieces + s) * wo_step, wo_step)
        part = wo_full.at[pl.ds(at, wo_step)]
        return remote(part, part, wo_sem.at[0, kind, s], wo_sem.at[1, kind, s], **to)

    def wo_shard(owner):
        part = wo_full.at[pl.ds(pl.multiple_of(owner * wo_rows, wo_rows), wo_rows)]
        return remote(part, part, wo_sem.at[0, 0, 0], wo_sem.at[1, 0, 0], tp=near)

    def wo_onward(s):
        wo_copy(1, far, odd, s, tp=far).wait_recv()
        wo_copy(2, far, odd, s, sp=partner).start()
        wo_copy(3, far, odd, s, tp=near).start()

    def source(w, t):
        return place - t if w == 0 else place + t

    def has(w, t):
        return place >= t if w == 0 else place + t < line

    def sends(w, t):
        onward = place + 1 < line if w == 0 else place > 0
        return has(w, t) & onward & (t < line - 1)

    def beyond(w):
        return lax.rem(me + 2, count) if w == 0 else lax.rem(me + count - 2, count)

    def up_hop(w, t, m):
        at = source(w, t) * 2 * up_rows + lax.rem(m + odd * (up_pieces // 2), up_pieces) * up_step
        part = full_up.at[pl.ds(pl.multiple_of(at, up_step), up_step)]
        return remote(part, part, up_send.at[w, t, m], up_recv.at[w, t, m], sp=beyond(w))

    def down_hop(w, t, m):
        each = down_pieces // 2
        owner = source(w, t) * 2 + m // each
        at = lax.rem(m, each) * down_step
        part = full_down.at[owner, pl.ds(pl.multiple_of(at, down_step), down_step)]
        return remote(part, part, down_send.at[w, t, m], down_recv.at[w, t, m], sp=beyond(w))

    up_ticks = line * up_pieces
    all_ticks = up_ticks + line * down_pieces

    def move(hop, pieces, n):
        t = n // pieces
        m = lax.rem(n, pieces)
        for w in range(2):

            @pl.when(has(w, t) & (t > 0))
            def _():
                hop(w, t - 1, m).wait_recv()

            @pl.when(sends(w, t))
            def _():
                hop(w, t, m).start()

    def up_tick(n):
        for p in range(2):

            @pl.when(n == up_pieces // 2 + p * (up_pieces // 4))
            def _():
                give_rows(p).wait_recv()

        move(up_hop, up_pieces, n)

    def down_tick(n):
        @pl.when(n == 0)
        def _():
            give_cols.wait_recv()

        move(down_hop, down_pieces, n)

    def tick(n):
        @pl.when(n < up_ticks)
        def _():
            up_tick(n)

        @pl.when((n >= up_ticks) & (n < all_ticks))
        def _():
            down_tick(n - up_ticks)

    def up_sent(n):
        t = n // up_pieces
        for w in range(2):

            @pl.when(sends(w, t))
            def _():
                up_hop(w, t, lax.rem(n, up_pieces)).wait_send()

    give_rows(0).start()
    for s in range(wo_pieces):
        wo_copy(1, tp, odd, s, tp=far).start()
    wo_shard(tp).start()
    for n in range(2):
        up_tick(n)

    key_width = memory.shape[1]
    value_width = memory.shape[2]
    span = key_width + STATE_PAD
    swap = remote(state_ref, held.at[0], state_send.at[0], state_recv.at[0], sp=partner)
    hand = remote(handed, held.at[1], state_send.at[1], state_recv.at[1], sp=beyond(0))

    def read_state(ref, h):
        low = h * span
        extra = ref[low + key_width : low + span, :].astype(jnp.float32)
        total = extra[2:3, :1] + extra[3:4, :1]
        level = extra[4:5, :1] + extra[5:6, :1]
        parts = extra[0:1, :key_width] + extra[1:2, :key_width]
        return ref[low : low + key_width, :].astype(jnp.float32), parts, level, total

    def join(first, second, total):
        mem_a, norm_a, level_a = first
        mem_b, norm_b, level_b = second
        after = jnp.maximum(total + level_a, level_b)
        one = jnp.exp(total + level_a - after)
        two = jnp.exp(level_b - after)
        return one * mem_a + two * mem_b, one * norm_a + two * norm_b, after

    def keep(refs, h, values):
        mem, norm, level = values
        refs[0][h] = mem
        refs[1][h, :1, :] = norm
        refs[2][h] = jnp.broadcast_to(level, refs[2].shape[1:])

    carried_refs = (memory, normer, running)

    def write_state(ref, h, mem, norm, level, total):
        low = h * span
        ref[low : low + key_width, :] = mem.astype(jnp.bfloat16)
        lines = jnp.zeros((STATE_PAD, value_width), jnp.float32)
        at_line = lax.broadcasted_iota(jnp.int32, lines.shape, 0)
        norm = jnp.concatenate([norm] * (value_width // key_width), axis=1)
        for i, part in enumerate((norm, total, level)):
            high = part.astype(jnp.bfloat16).astype(jnp.float32)
            lines = jnp.where(at_line == 2 * i, high, lines)
            lines = jnp.where(at_line == 2 * i + 1, part - high, lines)
        ref[low + key_width : low + span, :] = lines.astype(jnp.bfloat16)

    length = BLOCK
    blocks = q_ref.shape[0] // length
    at_row = lax.broadcasted_iota(jnp.int32, (length, length), 0)
    at_col = lax.broadcasted_iota(jnp.int32, (length, length), 1)

    def by_block(first):
        return jnp.concatenate(
            [
                logs_ref[first : first + heads, b * length : (b + 1) * length]
                for b in range(blocks)
            ],
            axis=0,
        )

    within = jnp.dot(
        by_block(heads),
        jnp.where(at_row <= at_col, 1.0, 0.0),
        precision=lax.Precision.HIGHEST,
        preferred_element_type=jnp.float32,
    )
    shifted_all = by_block(0) - within
    each_all = within[:, length - 1 : length]
    after = jnp.zeros((heads, 1), jnp.float32)
    to_end = [None] * blocks
    for b in reversed(range(blocks)):
        part = slice(b * heads, (b + 1) * heads)
        after = after + each_all[part]
        to_end[b] = shifted_all[part] + after
    own_total = after
    own_level = functools.reduce(jnp.maximum, to_end)
    own_level = jnp.max(own_level, axis=1, keepdims=True)
    for b in range(blocks):
        part = slice(b * heads, (b + 1) * heads)
        rows_ref[b, 0 : 2 * heads, :] = jnp.concatenate(
            [shifted_all[part], jnp.broadcast_to(each_all[part], (heads, length))], axis=0
        )
        lines = [within[part], shifted_all[part], jnp.exp(to_end[b] - own_level)]
        lines.append(jnp.zeros((length - 3 * heads, length), jnp.float32))
        cols_ref[b * length : (b + 1) * length, :] = jnp.transpose(
            jnp.concatenate(lines, axis=0)
        )

    memory[...] = jnp.zeros_like(memory)
    normer[...] = jnp.zeros_like(normer)

    @pl.loop(0, blocks)
    def _(j):
        rows = pl.ds(pl.multiple_of(j * length, length), length)
        cols = cols_ref[rows, :]
        for h in range(heads):
            k = k_ref[rows, h * key_width : (h + 1) * key_width]
            v = v_ref[rows, h * value_width : (h + 1) * value_width]
            weighted = k.astype(jnp.float32) * cols[:, 2 * heads + h : 2 * heads + h + 1]
            memory[h] += lax.dot_general(
                weighted.astype(jnp.bfloat16),
                v,
                (((0,), (0,)), ((), ())),
                preferred_element_type=jnp.float32,
            )
            normer[h, :1, :] += jnp.sum(weighted, axis=0, keepdims=True)

    for h in range(heads):
        write_state(
            state_ref,
            h,
            memory[h],
            normer[h, :1, :],
            own_level[h : h + 1, :],
            own_total[h : h + 1, :],
        )
    swap.start()
    give_rows(1).start()
    swap.wait_recv()
    for s in range(wo_pieces // 2):
        wo_onward(s)

    @pl.when(odd == 0)
    def _():
        for h in range(heads):
            mem_a, norm_a, level_a, total_a = read_state(state_ref, h)
            mem_b, norm_b, level_b, total_b = read_state(held.at[0], h)
            out = join((mem_a, norm_a, level_a), (mem_b, norm_b, level_b), total_b)
            keep((pair_memory, pair_normer, pair_level.at[0]), h, out)
            pair_level[1, h] = jnp.broadcast_to(total_a + total_b, pair_level.shape[2:])

    @pl.when(odd == 1)
    def _():
        for h in range(heads):
            mem_a, norm_a, level_a, total_a = read_state(held.at[0], h)
            mem_b, norm_b, level_b, total_b = read_state(state_ref, h)
            out = join((mem_a, norm_a, level_a), (mem_b, norm_b, level_b), total_b)
            keep((pair_memory, pair_normer, pair_level.at[0]), h, out)
            pair_level[1, h] = jnp.broadcast_to(total_a + total_b, pair_level.shape[2:])

    started = jnp.minimum(FIRST_TICKS + NEXT_TICKS * place, up_ticks)

    @pl.loop(2, started)
    def _(n):
        up_sent(n - 2)
        up_tick(n)

    memory[...] = jnp.zeros_like(memory)
    normer[...] = jnp.zeros_like(normer)
    running[...] = jnp.full(running.shape, neg_large, jnp.float32)

    @pl.when(place > 0)
    def _():
        hand.wait_recv()
        for h in range(heads):
            mem, parts, level, total = read_state(held.at[1], h)
            keep(carried_refs, h, (mem, parts, level))

    @pl.when(place + 1 < line)
    def _():
        for h in range(heads):
            mem, norm, level = join(
                (memory[h], normer[h, :1, :], running[h, :1, :1]),
                (pair_memory[h], pair_normer[h, :1, :], pair_level[0, h, :1, :1]),
                pair_level[1, h, :1, :1],
            )
            write_state(handed, h, mem, norm, level, jnp.zeros_like(level))
        hand.start()

    @pl.when(odd == 1)
    def _():
        for h in range(heads):
            mem, norm, level, total = read_state(held.at[0], h)
            out = join(
                (memory[h], normer[h, :1, :], running[h, :1, :1]), (mem, norm, level), total
            )
            keep(carried_refs, h, out)

    scale = key_width ** (-0.5)
    causal = at_col <= at_row
    size = residual_ref.shape[0]
    per = size // length

    def block_copy(j, sender):
        at = pl.multiple_of(lax.rem(j, per) * length, length)
        width = gated.shape[1]
        return remote(
            gated.at[pl.ds(pl.multiple_of(j * length, length), length)],
            mine.at[sender, pl.ds(at, length)],
            block_send.at[j],
            block_recv.at[sender, lax.rem(j, per)],
            tp=j // per,
        )

    @pl.loop(0, blocks)
    def _(j):
        tick(started + j)

        @pl.when(j < wo_pieces // 2)
        def _():
            wo_onward(wo_pieces // 2 + j)

        @pl.when(j == wo_pieces // 2)
        def _():
            give_cols.start()

        @pl.when(j >= blocks - wo_pieces)
        def _():
            s = j - (blocks - wo_pieces)
            wo_copy(2, far, 1 - odd, s, sp=partner).wait_recv()
            wo_copy(4, far, 1 - odd, s, tp=near).start()

        rows = pl.ds(pl.multiple_of(j * length, length), length)
        lanes = rows_ref[j]
        cols = cols_ref[rows, :]
        for h in range(heads):
            keys = slice(h * key_width, (h + 1) * key_width)
            vals = slice(h * value_width, (h + 1) * value_width)
            q = q_ref[rows, keys]
            k = k_ref[rows, keys]
            v = v_ref[rows, vals]
            before = running[h, :1, :1]
            total = lanes[heads + h : heads + h + 1, :1]
            shifted_log = jnp.where(causal, lanes[h : h + 1, :], -jnp.inf)
            top = jnp.maximum(jnp.max(shifted_log, axis=1, keepdims=True), before)
            raw = (
                lax.dot_general(
                    q, k, (((1,), (1,)), ((), ())), preferred_element_type=jnp.float32
                )
                * scale
            )
            scores = raw * jnp.exp(shifted_log - top)
            carry = jnp.exp(before - top) * scale
            state = memory[h]
            high = state.astype(jnp.bfloat16)
            low = (state - high.astype(jnp.float32)).astype(jnp.bfloat16)
            carried = jnp.dot(q, high, preferred_element_type=jnp.float32) + jnp.dot(
                q, low, preferred_element_type=jnp.float32
            )
            numerator = carry * carried + jnp.dot(
                scores.astype(jnp.bfloat16), v, preferred_element_type=jnp.float32
            )
            denominator = carry * jnp.sum(
                q.astype(jnp.float32) * normer[h, :1, :], axis=1, keepdims=True
            ) + jnp.sum(scores, axis=1, keepdims=True)
            level = cols[:, h : h + 1] + top
            value = numerator / jnp.maximum(jnp.abs(denominator), jnp.exp(-level))
            mean = jnp.mean(value * value, axis=1, keepdims=True)
            normed = value * lax.rsqrt(mean + eps) * gain_ref[h : h + 1, :]
            gate = normed * jax.nn.sigmoid(gate_ref[rows, vals].astype(jnp.float32))
            gated[rows, vals] = gate.astype(gated.dtype)
            last = jnp.max(jnp.maximum(lanes[h : h + 1, :], before), axis=1, keepdims=True)
            decay = jnp.exp(before - last)
            weighted = k.astype(jnp.float32) * jnp.exp(cols[:, heads + h : heads + h + 1] - last)
            memory[h] = decay * state + lax.dot_general(
                weighted.astype(jnp.bfloat16),
                v,
                (((0,), (0,)), ((), ())),
                preferred_element_type=jnp.float32,
            )
            normer[h, :1, :] = decay * normer[h, :1, :] + jnp.sum(
                weighted, axis=0, keepdims=True
            )
            running[h] = jnp.broadcast_to(last + total, running.shape[1:])

        @pl.when(j // per == tp)
        def _():
            at = pl.multiple_of(lax.rem(j, per) * length, length)
            mine[tp, pl.ds(at, length), :] = gated[rows, :]

        @pl.when(j // per != tp)
        def _():
            block_copy(j, tp).start()

    reached = started + blocks
    wo_shard(near).wait_recv()
    for s in range(wo_pieces):
        wo_copy(3, opposite, odd, s, tp=near).wait_recv()
        wo_copy(4, opposite, 1 - odd, s, tp=near).wait_recv()

    @pl.loop(0, 4)
    def _(s):
        tick(reached + s)

        @pl.when(s != tp)
        def _():
            for p in range(per):
                block_copy(tp * per + p, s).wait_recv()

    reached = reached + 4

    def columns(i):
        return pl.ds(pl.multiple_of(i * wide, wide), wide)

    @pl.loop(0, model // wide)
    def _(i):
        total = jnp.zeros((size, wide), jnp.float32)
        for s in range(4):
            total += jnp.dot(
                mine[s],
                wo_full[s * wo_rows : (s + 1) * wo_rows, columns(i)],
                preferred_element_type=jnp.float32,
            )
        total_rows[:, columns(i)] = total

    pad = PAD_ROWS
    tokens = 8 * size
    row_pieces = rows_send.shape[1]
    row_step = size // row_pieces

    def row_copy(kind, y, owner, p, **to):
        at = pad + (y * 4 + owner) * size + p * row_step
        part = group.at[pl.ds(pl.multiple_of(at, pad), row_step)]
        return remote(part, part, rows_send.at[kind, p], rows_recv.at[kind, p], **to)

    @pl.when(place == 0)
    def _():
        group[0:pad, :] = jnp.zeros((pad, model), group.dtype)

    @pl.loop(0, row_pieces)
    def _(p):
        rows = pl.ds(pl.multiple_of(p * row_step, row_step), row_step)
        rounded = (residual_ref[rows, :].astype(jnp.float32) + total_rows[rows, :]).astype(
            jnp.bfloat16
        )
        stream[rows, :] = rounded
        x = rounded.astype(jnp.float32)
        normed = x * lax.rsqrt(jnp.mean(x * x, axis=-1, keepdims=True) + eps) * norm_gain_ref[...]
        at = pl.multiple_of(pad + (odd * 4 + tp) * size + p * row_step, pad)
        group[pl.ds(at, row_step), :] = normed.astype(jnp.bfloat16)
        row_copy(0, odd, tp, p, tp=far).start()
        row_copy(2, odd, tp, p, sp=partner).start()
        row_copy(1, odd, tp, p, tp=near).start()

    @pl.loop(0, row_pieces)
    def _(p):
        tick(reached + 2 * p)
        row_copy(0, odd, far, p, tp=far).wait_recv()
        row_copy(3, odd, far, p, tp=near).start()

        @pl.when(lax.rem(p, 2) == 0)
        def _():
            row_copy(6, odd, far, p, sp=partner).start()

        tick(reached + 2 * p + 1)
        row_copy(2, 1 - odd, tp, p, sp=partner).wait_recv()
        row_copy(4, 1 - odd, tp, p, tp=near).start()

        @pl.when(lax.rem(p, 2) == 1)
        def _():
            row_copy(6, 1 - odd, tp, p, tp=far).start()

    reached = reached + 2 * row_pieces

    @pl.loop(0, row_pieces)
    def _(p):
        tick(reached + p)
        row_copy(6, 1 - odd, far, p, sp=partner).wait_recv()
        row_copy(5, 1 - odd, far, p, tp=near).start()
        row_copy(1, odd, near, p, tp=near).wait_recv()
        row_copy(3, odd, opposite, p, tp=near).wait_recv()
        row_copy(4, 1 - odd, near, p, tp=near).wait_recv()

    reached = reached + row_pieces

    @pl.loop(0, row_pieces)
    def _(p):
        row_copy(5, 1 - odd, opposite, p, tp=near).wait_recv()

    edge = remote(
        group.at[pl.ds(tokens, pad)],
        group.at[pl.ds(0, pad)],
        edge_sem.at[0],
        edge_sem.at[1],
        sp=beyond(0),
    )

    @pl.when(place + 1 < line)
    def _():
        edge.start()

    @pl.loop(jnp.minimum(reached, up_ticks), up_ticks)
    def _(n):
        up_tick(n)

    reached = jnp.maximum(reached, up_ticks)
    early = up_ticks + 2 * down_pieces
    parts = 4
    part_rows = tokens // parts

    def ups_tick(step):
        n = reached + step // UPS_PER_TICK

        @pl.when((n < early) & (lax.rem(step, UPS_PER_TICK) == 0))
        def _():
            tick(n)

    def silu(a):
        return a * jax.nn.sigmoid(a)

    @pl.loop(0, parts)
    def _(b):
        part = lax.rem(b + 1, parts)
        at = pl.multiple_of(part * part_rows, part_rows)
        window = pl.ds(at, part_rows + pad)
        outs = pl.ds(at, part_rows)

        @pl.when((b == parts - 1) & (place > 0))
        def _():
            edge.wait_recv()

        def conv(taps, width):
            return (
                taps[0:1, :] * up_tile[pad - 2 : pad - 2 + part_rows, width]
                + taps[1:2, :] * up_tile[pad - 1 : pad - 1 + part_rows, width]
                + taps[2:3, :] * up_tile[pad : pad + part_rows, width]
            )

        @pl.loop(0, tiles)
        def _(i):
            ups_tick(b * (tiles + 1) + i)
            lanes = pl.ds(pl.multiple_of(i * 2 * lane, 2 * lane), 2 * lane)
            up_tile[...] = jnp.dot(
                group[window, :], full_up[:, lanes], preferred_element_type=jnp.float32
            )
            taps_at = pl.ds(pl.multiple_of(odd * shift + i * lane, lane), lane)
            act = silu(conv(gate_taps_ref[:, taps_at], slice(0, lane))) * conv(
                value_taps_ref[:, taps_at], slice(lane, 2 * lane)
            )
            hidden[outs, pl.ds(pl.multiple_of(i * lane, lane), lane)] = act.astype(jnp.bfloat16)

        ups_tick(b * (tiles + 1) + tiles)
        up_tile[:, 0:lane] = jnp.dot(
            group[window, :], full_up[:, tail], preferred_element_type=jnp.float32
        )
        mid = slice(tiles * lane, (tiles + 1) * lane)
        low = lax.broadcasted_iota(jnp.int32, (3, lane), 1) < rest
        taps_a, taps_b = halves_of(gate_taps_ref[:, mid], value_taps_ref[:, mid], low)
        both = conv(jnp.where(odd == 0, taps_a, taps_b), slice(0, lane))
        act = silu(both) * pltpu.roll(both, rest, 1)
        hidden[outs, tiles * lane : tiles * lane + rest] = act[:, :rest].astype(jnp.bfloat16)

    ups_ticks = (parts * (tiles + 1) + UPS_PER_TICK - 1) // UPS_PER_TICK

    @pl.loop(jnp.minimum(reached + ups_ticks, early), early)
    def _(n):
        tick(n)

    both_sides = jnp.minimum(place, line - 1 - place)

    def away(k):
        return jnp.where(k <= 2 * both_sides, (k + 1) // 2, k - both_sides)

    def unit(k):
        rising = jnp.where(place < line - 1 - place, 1, -1)
        way = jnp.where(k <= 2 * both_sides, 1 - 2 * lax.rem(k, 2), rising)
        return place + way * away(k)

    def sum_copy(kind, i):
        src, dst, to = (
            (pair_out.at[i], pair_in.at[i], {"tp": near}),
            (second_out.at[i, 0], second_in.at[i, 0], {"tp": far}),
            (second_out.at[i, 1], second_in.at[i, 1], {"sp": partner}),
            (third_out.at[i, 0], third_in.at[i, 0], {"sp": partner}),
            (third_out.at[i, 1], third_in.at[i, 1], {"tp": far}),
        )[kind]
        return remote(src, dst, sum_send.at[kind, i], sum_recv.at[kind, i], **to)

    part_wide = wide // 2
    cut = (slice(0, part_wide), slice(part_wide, wide))

    def term(i, a, b, side):
        y = lax.rem(odd + a, 2)
        x = lax.rem(chip + b, 2)
        owner = 2 * x + lax.rem(core + side, 2)
        rows = pl.ds(pl.multiple_of((y * 4 + owner) * size, size), size)
        return jnp.dot(hidden[rows, :], full_down[i], preferred_element_type=jnp.float32)

    def first_stage(i):
        for a in range(2):
            for b in range(2):
                pair_out[i, 2 * a + b] = term(i, a, b, 1).astype(jnp.bfloat16)
        sum_copy(0, i).start()
        for a in range(2):
            for b in range(2):
                blocks_of[2 * a + b] = term(i, a, b, 0)

    def second_stage(i):
        sum_copy(0, i).wait_recv()

        def block(a, b, side):
            at = 2 * a + b
            return blocks_of[at, :, cut[side]] + pair_in[i, at, :, cut[side]].astype(jnp.float32)

        for a in range(2):
            second_out[i, 0, a] = block(a, 1, 0).astype(jnp.bfloat16)
        sum_copy(1, i).start()
        for b in range(2):
            second_out[i, 1, b] = block(1, b, 1).astype(jnp.bfloat16)
        sum_copy(2, i).start()
        for a in range(2):
            kept[i, 0, a] = block(a, 0, 0)
        for b in range(2):
            kept[i, 1, b] = block(0, b, 1)

    def third_stage(i):
        for side in range(2):
            sum_copy(1 + side, i).wait_recv()
            third_out[i, side] = (
                kept[i, side, 1] + second_in[i, side, 1].astype(jnp.float32)
            ).astype(jnp.bfloat16)
            sum_copy(3 + side, i).start()
            kept[i, side, 0] += second_in[i, side, 0].astype(jnp.float32)

    def last_stage(i):
        for side in range(2):
            sum_copy(3 + side, i).wait_recv()
            at = pl.multiple_of(i * wide + side * part_wide, part_wide)
            cols = pl.ds(at, part_wide)
            out_ref[:, cols] = (
                stream[:, cols].astype(jnp.float32)
                + (kept[i, side, 0] + third_in[i, side].astype(jnp.float32))
            ).astype(out_ref.dtype)

    def slice_at(n):
        return 2 * unit(n // 2) + lax.rem(n, 2)

    def due(k, j):
        return up_ticks + down_pieces * away(k) + (j + 1) * (down_pieces // 2)

    def until(n):
        k = n // 2
        last = jnp.where(k > 0, due(jnp.maximum(k - 1, 0), 1), early)
        return jnp.maximum(jnp.maximum(due(k, lax.rem(n, 2)), last), early)

    @pl.loop(0, count)
    def _(n):
        @pl.when(n > 0)
        def _():
            @pl.loop(until(n - 1), until(n))
            def _(at):
                tick(at)

        first_stage(slice_at(n))

        @pl.when(n > 1)
        def _():
            third_stage(slice_at(n - 2))

        second_stage(slice_at(n))

    for n in (count - 2, count - 1):
        third_stage(slice_at(n))

    @pl.loop(0, count)
    def _(n):
        last_stage(slice_at(n))

    swap.wait_send()

    @pl.when(place + 1 < line)
    def _():
        hand.wait_send()
        edge.wait_send()

    for p in range(2):
        give_rows(p).wait_send()
    wo_shard(tp).wait_send()
    for s in range(wo_pieces):
        for kind in range(1, 5):
            wo_copy(kind, tp, 0, s, tp=near).wait_send()
    give_cols.wait_send()

    @pl.loop(0, blocks)
    def _(j):
        @pl.when(j // per != tp)
        def _():
            block_copy(j, tp).wait_send()

    @pl.loop(0, row_pieces)
    def _(p):
        for kind in range(7):
            row_copy(kind, odd, tp, p, tp=near).wait_send()

    @pl.loop(0, count)
    def _(i):
        for kind in range(5):
            sum_copy(kind, i).wait_send()

    @pl.loop(started - 2, up_ticks)
    def _(n):
        up_sent(n)

    @pl.loop(0, line - 1)
    def _(t):
        for w in range(2):

            @pl.when(sends(w, t))
            def _():
                for m in range(down_pieces):
                    down_hop(w, t, m).wait_send()


FIRST_TICKS = 4
NEXT_TICKS = 2
UPS_PER_TICK = 4
UP_PIECES = 8
DOWN_PIECES = 4
PAD_ROWS = 16


def one_kernel_fits(rows, gate_w, down_w):
    count = lax.axis_size("sp")
    return (
        lax.axis_size("tp") == 4
        and count >= 4
        and count % 2 == 0
        and 2 * gate_w.shape[0] % (16 * UP_PIECES) == 0
        and gate_w.shape[1] % 256 == 128
        and down_w.shape[0] % (16 * DOWN_PIECES) == 0
        and down_w.shape[1] % 256 == 0
        and rows % (2 * BLOCK) == 0
        and 4 * rows >= 6 * BLOCK
    )


def layer(q, k, v, gates, input_log, forget_log, gain, wo, residual, norm_gain, gate_w, value_w, down_w, gate_taps, value_taps):
    count = lax.axis_size("sp")
    line = count // 2
    heads = input_log.shape[1]
    tokens = q.shape[0]
    key_width = q.shape[1] // heads
    value_width = v.shape[1] // heads
    span = key_width + STATE_PAD
    model = wo.shape[1]
    rows = residual.shape[0]
    lane = 128
    half_width = gate_w.shape[1] // 2
    tiles = half_width // lane
    wide = down_w.shape[1]
    row_pieces = 4
    blocks = tokens // BLOCK
    logs = jnp.concatenate([input_log.T, forget_log.T], axis=0)
    vmem = pl.BlockSpec(memory_space=pltpu.VMEM)
    hbm = pl.BlockSpec(memory_space=pl.ANY)
    low, full = jnp.bfloat16, jnp.float32
    dma = pltpu.SemaphoreType.DMA
    return pl.pallas_call(
        functools.partial(layer_kernel, count, heads, UP_PIECES, DOWN_PIECES),
        out_shape=jax.ShapeDtypeStruct(residual.shape, low),
        in_specs=[vmem] * 10 + [hbm] * 4,
        out_specs=vmem,
        scratch_shapes=[
            pltpu.VMEM((blocks, 8, BLOCK), full),
            pltpu.VMEM((tokens, BLOCK), full),
            pltpu.VMEM((heads * span, value_width), low),
            pltpu.VMEM((2, heads * span, value_width), low),
            pltpu.VMEM((heads, key_width, value_width), full),
            pltpu.VMEM((heads, 8, key_width), full),
            pltpu.VMEM((heads, 8, 128), full),
            pltpu.VMEM((heads, key_width, value_width), full),
            pltpu.VMEM((heads, 8, key_width), full),
            pltpu.VMEM((2, heads, 8, 128), full),
            pltpu.VMEM((heads * span, value_width), low),
            pltpu.VMEM((tokens, v.shape[1]), low),
            pltpu.VMEM((4, rows, v.shape[1]), low),
            pltpu.VMEM((model, model), low),
            pltpu.VMEM((2, gate_w.shape[0], lane), low),
            pltpu.VMEM((gate_w.shape[0], 2 * half_width), low),
            pltpu.VMEM((half_width, wide), low),
            pltpu.VMEM((model, 2 * half_width), low),
            pltpu.VMEM((count, half_width, wide), low),
            pltpu.VMEM((rows, model), full),
            pltpu.VMEM((rows, model), low),
            pltpu.VMEM((PAD_ROWS + 2 * tokens, model), low),
            pltpu.VMEM((PAD_ROWS + tokens // 2, 2 * lane), full),
            pltpu.VMEM((2 * tokens, half_width), low),
            pltpu.VMEM((count, 4, rows, wide), low),
            pltpu.VMEM((count, 4, rows, wide), low),
            pltpu.VMEM((count, 2, 2, rows, wide // 2), low),
            pltpu.VMEM((count, 2, 2, rows, wide // 2), low),
            pltpu.VMEM((count, 2, rows, wide // 2), low),
            pltpu.VMEM((count, 2, rows, wide // 2), low),
            pltpu.VMEM((count, 2, 2, rows, wide // 2), full),
            pltpu.VMEM((4, rows, wide), full),
            dma((4 * tiles + 7,)),
            dma((2, 5, 4)),
            dma((2, 3)),
            dma((2,)),
            dma((2,)),
            dma((2, line - 1, UP_PIECES)),
            dma((2, line - 1, UP_PIECES)),
            dma((2, line - 1, DOWN_PIECES)),
            dma((2, line - 1, DOWN_PIECES)),
            dma((blocks,)),
            dma((4, rows // BLOCK)),
            dma((7, row_pieces)),
            dma((7, row_pieces)),
            dma((5, count)),
            dma((5, count)),
            dma((2,)),
        ],
        compiler_params=pltpu.CompilerParams(
            collective_id=0, has_side_effects=True, vmem_limit_bytes=63 * 1024 * 1024
        ),
        cost_estimate=pl.CostEstimate(
            flops=30_000_000_000, bytes_accessed=8 * v.size, transcendentals=0
        ),
    )(
        logs,
        q,
        k,
        v,
        gates,
        gain,
        residual,
        norm_gain[None, :],
        gate_taps,
        value_taps,
        wo,
        gate_w,
        value_w,
        down_w,
    )


def local(
    residual_entry_input,
    query_matrix_rows,
    key_matrix_rows,
    value_matrix_rows,
    output_gate_logits,
    input_gate_logits,
    forget_gate_logits,
    forget_decay_offset,
    head_norm_gain,
    cell_output_weight,
    feedforward_norm_gain,
    gate_up_weight,
    value_up_weight,
    gate_filter_taps,
    value_filter_taps,
    down_projection_weight,
):
    input_log, forget_log = gate_log_values(
        input_gate_logits, forget_gate_logits, forget_decay_offset
    )
    if one_kernel_fits(residual_entry_input.shape[0], gate_up_weight, down_projection_weight):
        return layer(
            query_matrix_rows,
            key_matrix_rows,
            value_matrix_rows,
            output_gate_logits,
            input_log,
            forget_log,
            head_norm_gain,
            cell_output_weight,
            residual_entry_input,
            feedforward_norm_gain,
            gate_up_weight,
            value_up_weight,
            down_projection_weight,
            gate_filter_taps,
            value_filter_taps,
        )
    whole_gate = lax.all_gather(gate_up_weight, "sp", axis=0, tiled=True)
    whole_down = lax.all_gather(down_projection_weight, "sp", axis=1, tiled=True)
    gated_rows = cell(
        query_matrix_rows,
        key_matrix_rows,
        value_matrix_rows,
        output_gate_logits,
        input_log,
        forget_log,
        head_norm_gain,
    )
    mixed_rows = product_rows(gated_rows, cell_output_weight, 2)
    stream_wide = residual_entry_input.astype(jnp.float32) + mixed_rows
    stream = stream_wide.astype(jnp.bfloat16)
    stream_wide = lax.optimization_barrier(stream).astype(jnp.float32)
    normed_rows = (
        stream_wide
        * lax.rsqrt(jnp.mean(stream_wide * stream_wide, axis=-1, keepdims=True) + eps)
        * feedforward_norm_gain[None, :]
    ).astype(jnp.bfloat16)
    group_rows = gather_rows(normed_rows)
    group_rows, value_shard = lax.optimization_barrier((group_rows, value_up_weight))
    whole_value = walk_gather(value_shard, 2)
    earlier_rows = shifted(group_rows[-2:], "sp", 1)
    window = jnp.concatenate([earlier_rows, group_rows], axis=0)
    up_gate = jnp.dot(
        window,
        whole_gate,
        preferred_element_type=jnp.float32,
    )
    up_value = jnp.dot(
        window,
        whole_value,
        preferred_element_type=jnp.float32,
    )
    conv_g = (
        gate_filter_taps[0][None, :] * up_gate[:-2]
        + gate_filter_taps[1][None, :] * up_gate[1:-1]
        + gate_filter_taps[2][None, :] * up_gate[2:]
    )
    conv_v = (
        value_filter_taps[0][None, :] * up_value[:-2]
        + value_filter_taps[1][None, :] * up_value[1:-1]
        + value_filter_taps[2][None, :] * up_value[2:]
    )
    hidden = (jax.nn.silu(conv_g) * conv_v).astype(jnp.bfloat16)
    ffn_rows = product_rows(hidden, whole_down, 3)
    return (stream_wide + ffn_rows).astype(jnp.bfloat16)


def solution(mesh):
    in_specs = (
        P(("sp", "tp"), None),
        P("sp", "tp"),
        P("sp", "tp"),
        P("sp", "tp"),
        P("sp", "tp"),
        P("sp", "tp"),
        P("sp", "tp"),
        P("sp", "tp"),
        P("tp", None),
        P("tp", None),
        P(),
        P("sp", "tp"),
        P("sp", "tp"),
        P(None, "tp"),
        P(None, "tp"),
        P("tp", "sp"),
    )
    out_specs = P(("sp", "tp"), None)
    return jax.shard_map(local, mesh=mesh, in_specs=in_specs, out_specs=out_specs, check_vma=False)
```

```python
import functools

import jax
import jax.numpy as jnp
from jax import lax
from jax.experimental import pallas as pl
from jax.experimental.pallas import tpu as pltpu
from jax.sharding import PartitionSpec as P

BLOCK = 128


eps = 1e-06
neg_large = -1e30


def shifted(x, axis, by):
    count = lax.axis_size(axis)
    pairs = [(i, i + by) for i in range(count) if 0 <= i + by < count]
    return lax.ppermute(x, axis, pairs)


def gate_log_values(input_gate_logits, forget_gate_logits, forget_decay_offset):
    input_log_value = 15.0 * jnp.tanh(input_gate_logits / 15.0)
    forget_log_sigmoid = (
        jax.nn.log_sigmoid(15.0 * jnp.tanh(forget_gate_logits / 15.0)) + forget_decay_offset
    )
    return (input_log_value, forget_log_sigmoid)


STATE_PAD = 16
MESH = pl.DeviceIdType.MESH


def cell_kernel(
    count,
    heads,
    state_ref,
    q_ref,
    k_ref,
    v_ref,
    gate_ref,
    gain_ref,
    rows_ref,
    cols_ref,
    out_ref,
    held,
    memory,
    normer,
    running,
    send_sem,
    recv_sem,
):
    me = lax.axis_index("sp")
    barrier = pltpu.get_barrier_semaphore()
    for d in range(1, count):
        pl.semaphore_signal(
            barrier, inc=1, device_id={"sp": lax.rem(me + d, count)}, device_id_type=MESH
        )
    pl.semaphore_wait(barrier, count - 1)

    def push(d, target, slot):
        return pltpu.make_async_remote_copy(
            src_ref=state_ref,
            dst_ref=held.at[slot],
            send_sem=send_sem.at[d],
            recv_sem=recv_sem.at[d],
            device_id={"sp": target},
            device_id_type=MESH,
        )

    for d in range(1, count):

        @pl.when(me + d < count)
        def _():
            push(d, me + d, me).start()

    memory[...] = jnp.zeros_like(memory)
    normer[...] = jnp.zeros_like(normer)
    running[...] = jnp.full(running.shape, neg_large, jnp.float32)
    for d in range(1, count):

        @pl.when(me - d >= 0)
        def _():
            push(d, lax.rem(me + d, count), me - d).wait_recv()

    key_width = memory.shape[1]
    value_width = memory.shape[2]
    span = key_width + STATE_PAD

    @pl.loop(0, me)
    def _(j):
        for h in range(heads):
            low = h * span
            extra = held[j, low + key_width : low + span, :].astype(jnp.float32)
            total = extra[2:3, :1] + extra[3:4, :1]
            level = extra[4:5, :1] + extra[5:6, :1]
            before = running[h, :1, :1]
            after = jnp.maximum(total + before, level)
            one = jnp.exp(total + before - after)
            two = jnp.exp(level - after)
            memory[h] = one * memory[h] + two * held[j, low : low + key_width, :].astype(
                jnp.float32
            )
            parts = extra[0:1, :key_width] + extra[1:2, :key_width]
            normer[h, :1, :] = one * normer[h, :1, :] + two * parts
            running[h] = jnp.broadcast_to(after, running.shape[1:])

    length = BLOCK
    scale = key_width ** (-0.5)
    at_row = lax.broadcasted_iota(jnp.int32, (length, length), 0)
    at_col = lax.broadcasted_iota(jnp.int32, (length, length), 1)
    causal = at_col <= at_row

    @pl.loop(0, q_ref.shape[0] // length)
    def _(j):
        rows = pl.ds(pl.multiple_of(j * length, length), length)
        lanes = rows_ref[j]
        cols = cols_ref[rows, :]
        for h in range(heads):
            keys = slice(h * key_width, (h + 1) * key_width)
            vals = slice(h * value_width, (h + 1) * value_width)
            q = q_ref[rows, keys]
            k = k_ref[rows, keys]
            v = v_ref[rows, vals]
            before = running[h, :1, :1]
            total = lanes[heads + h : heads + h + 1, :1]
            shifted_log = jnp.where(causal, lanes[h : h + 1, :], -jnp.inf)
            top = jnp.maximum(jnp.max(shifted_log, axis=1, keepdims=True), before)
            raw = (
                lax.dot_general(
                    q, k, (((1,), (1,)), ((), ())), preferred_element_type=jnp.float32
                )
                * scale
            )
            scores = raw * jnp.exp(shifted_log - top)
            carry = jnp.exp(before - top) * scale
            state = memory[h]
            high = state.astype(jnp.bfloat16)
            low = (state - high.astype(jnp.float32)).astype(jnp.bfloat16)
            carried = jnp.dot(q, high, preferred_element_type=jnp.float32) + jnp.dot(
                q, low, preferred_element_type=jnp.float32
            )
            numerator = carry * carried + jnp.dot(
                scores.astype(jnp.bfloat16), v, preferred_element_type=jnp.float32
            )
            denominator = carry * jnp.sum(
                q.astype(jnp.float32) * normer[h, :1, :], axis=1, keepdims=True
            ) + jnp.sum(scores, axis=1, keepdims=True)
            level = cols[:, h : h + 1] + top
            value = numerator / jnp.maximum(jnp.abs(denominator), jnp.exp(-level))
            mean = jnp.mean(value * value, axis=1, keepdims=True)
            normed = value * lax.rsqrt(mean + eps) * gain_ref[h : h + 1, :]
            gated = normed * jax.nn.sigmoid(gate_ref[rows, vals].astype(jnp.float32))
            out_ref[rows, vals] = gated.astype(out_ref.dtype)
            last = jnp.max(jnp.maximum(lanes[h : h + 1, :], before), axis=1, keepdims=True)
            decay = jnp.exp(before - last)
            weighted = k.astype(jnp.float32) * jnp.exp(cols[:, heads + h : heads + h + 1] - last)
            memory[h] = decay * state + lax.dot_general(
                weighted.astype(jnp.bfloat16),
                v,
                (((0,), (0,)), ((), ())),
                preferred_element_type=jnp.float32,
            )
            normer[h, :1, :] = decay * normer[h, :1, :] + jnp.sum(
                weighted, axis=0, keepdims=True
            )
            running[h] = jnp.broadcast_to(last + total, running.shape[1:])

    for d in range(1, count):

        @pl.when(me + d < count)
        def _():
            push(d, me + d, me).wait_send()


def halves(x):
    high = lax.reduce_precision(x, 8, 7)
    return (high.astype(jnp.bfloat16), (x - high).astype(jnp.bfloat16))


def cell_parts(q, k, v, input_log, forget_log):
    heads = input_log.shape[1]
    tokens = q.shape[0]
    key_width = q.shape[1] // heads
    value_width = v.shape[1] // heads
    count = lax.axis_size("sp")
    blocks = tokens // BLOCK
    f = forget_log.reshape(blocks, BLOCK, heads)
    tri = jnp.tril(jnp.ones((BLOCK, BLOCK), jnp.float32))
    within = jnp.einsum("ts,bsh->bth", tri, f, precision=lax.Precision.HIGHEST)
    each = within[:, -1, :]
    later = jnp.triu(jnp.ones((blocks, blocks), jnp.float32), 1)
    after = jnp.einsum("bc,ch->bh", later, each, precision=lax.Precision.HIGHEST)
    total = jnp.sum(each, axis=0)
    shifted_log = input_log.reshape(blocks, BLOCK, heads) - within
    to_end = (shifted_log + (each + after)[:, None, :]).reshape(tokens, heads)
    level = jnp.max(to_end, axis=0)
    weighted = k.reshape(tokens, heads, key_width).astype(jnp.float32) * jnp.exp(to_end - level)[
        :, :, None
    ]
    memory = jnp.einsum(
        "shd,shv->hdv",
        weighted.astype(jnp.bfloat16),
        v.reshape(tokens, heads, value_width),
        preferred_element_type=jnp.float32,
    ).astype(jnp.bfloat16)
    normer = jnp.sum(weighted, axis=0)
    wide = (heads, 1, value_width)
    lines = [
        jnp.pad(part, ((0, 0), (0, value_width - key_width)))[:, None, :]
        for part in halves(normer)
    ]
    for scalar in (total, level):
        lines += [jnp.broadcast_to(part[:, None, None], wide) for part in halves(scalar)]
    lines.append(jnp.zeros((heads, STATE_PAD - len(lines), value_width), jnp.bfloat16))
    span = key_width + STATE_PAD
    state = jnp.concatenate([memory] + lines, axis=1).reshape(heads * span, value_width)
    lanes = jnp.concatenate(
        [
            jnp.transpose(shifted_log, (0, 2, 1)),
            jnp.broadcast_to(each[:, :, None], (blocks, heads, BLOCK)),
        ],
        axis=1,
    )
    cols = jnp.concatenate([within, shifted_log], axis=2).reshape(tokens, 2 * heads)
    return state, lanes, cols


def cell(q, k, v, gates, input_log, forget_log, gain):
    heads = input_log.shape[1]
    key_width = q.shape[1] // heads
    value_width = v.shape[1] // heads
    count = lax.axis_size("sp")
    span = key_width + STATE_PAD
    state, lanes, cols = cell_parts(q, k, v, input_log, forget_log)
    vmem = pl.BlockSpec(memory_space=pltpu.VMEM)
    return pl.pallas_call(
        functools.partial(cell_kernel, count, heads),
        out_shape=jax.ShapeDtypeStruct(v.shape, jnp.bfloat16),
        in_specs=[vmem] * 8,
        out_specs=vmem,
        scratch_shapes=[
            pltpu.VMEM((count, heads * span, value_width), jnp.bfloat16),
            pltpu.VMEM((heads, key_width, value_width), jnp.float32),
            pltpu.VMEM((heads, 8, key_width), jnp.float32),
            pltpu.VMEM((heads, 8, 128), jnp.float32),
            pltpu.SemaphoreType.DMA((count,)),
            pltpu.SemaphoreType.DMA((count,)),
        ],
        compiler_params=pltpu.CompilerParams(
            collective_id=0, has_side_effects=True, vmem_limit_bytes=40 * 1024 * 1024
        ),
        cost_estimate=pl.CostEstimate(
            flops=30_000_000_000, bytes_accessed=8 * v.size, transcendentals=0
        ),
    )(state, q, k, v, gates, gain, lanes, cols)


def rows_kernel(pieces, x_ref, out_ref, own_sem, near_send, near_recv, far_send, far_recv, on_send, on_recv):
    me = lax.axis_index("tp")
    near = me + 1 - 2 * lax.rem(me, 2)
    far = lax.rem(me + 2, 4)
    opposite = lax.rem(near + 2, 4)
    size = x_ref.shape[0]
    step = size // pieces
    barrier = pltpu.get_barrier_semaphore()
    for other in (near, far):
        pl.semaphore_signal(barrier, inc=1, device_id={"tp": other}, device_id_type=MESH)
    pl.semaphore_wait(barrier, 2)

    def at(owner, p):
        return out_ref.at[pl.ds(pl.multiple_of(owner * size + p * step, step), step)]

    def send(src, dst, sems, p, target):
        return pltpu.make_async_remote_copy(
            src_ref=src,
            dst_ref=dst,
            send_sem=sems[0].at[p],
            recv_sem=sems[1].at[p],
            device_id={"tp": target},
            device_id_type=MESH,
        )

    mine = [x_ref.at[pl.ds(p * step, step)] for p in range(pieces)]
    far_out = [send(mine[p], at(me, p), (far_send, far_recv), p, far) for p in range(pieces)]
    near_out = [send(mine[p], at(me, p), (near_send, near_recv), p, near) for p in range(pieces)]
    far_in = [send(mine[p], at(far, p), (far_send, far_recv), p, far) for p in range(pieces)]
    near_in = [send(mine[p], at(near, p), (near_send, near_recv), p, near) for p in range(pieces)]
    onward = [send(at(far, p), at(far, p), (on_send, on_recv), p, near) for p in range(pieces)]
    on_in = [
        send(at(opposite, p), at(opposite, p), (on_send, on_recv), p, near)
        for p in range(pieces)
    ]
    for p in range(pieces):
        far_out[p].start()
    for p in range(pieces):
        near_out[p].start()
    whole = pl.ds(pl.multiple_of(me * size, size), size)
    own = pltpu.make_async_copy(x_ref, out_ref.at[whole], own_sem)
    own.start()
    for p in range(pieces):
        far_in[p].wait_recv()
        onward[p].start()
    own.wait()
    for p in range(pieces):
        near_in[p].wait_recv()
        on_in[p].wait_recv()
    for p in range(pieces):
        far_out[p].wait_send()
        near_out[p].wait_send()
        onward[p].wait_send()


def gather_rows(x):
    if lax.axis_size("tp") != 4:
        return lax.all_gather(x, "tp", axis=0, tiled=True)
    pieces = 4
    vmem = pl.BlockSpec(memory_space=pltpu.VMEM)
    return pl.pallas_call(
        functools.partial(rows_kernel, pieces),
        out_shape=jax.ShapeDtypeStruct((4 * x.shape[0], x.shape[1]), x.dtype),
        in_specs=[vmem],
        out_specs=vmem,
        scratch_shapes=[pltpu.SemaphoreType.DMA] + [pltpu.SemaphoreType.DMA((pieces,))] * 6,
        compiler_params=pltpu.CompilerParams(
            collective_id=1, has_side_effects=True, vmem_limit_bytes=16 * 1024 * 1024
        ),
        cost_estimate=pl.CostEstimate(
            flops=30_000_000_000, bytes_accessed=4 * x.size, transcendentals=0
        ),
    )(x)


def product_kernel(
    pieces,
    x_ref,
    w_ref,
    out_ref,
    pair_out,
    pair_in,
    far_out,
    far_in,
    near_out,
    near_in,
    pair_send,
    pair_recv,
    far_send,
    far_recv,
    near_send,
    near_recv,
):
    me = lax.axis_index("tp")
    near = me + 1 - 2 * lax.rem(me, 2)
    far = lax.rem(me + 2, 4)
    opposite = lax.rem(near + 2, 4)
    size = out_ref.shape[0]
    step = out_ref.shape[1] // pieces
    barrier = pltpu.get_barrier_semaphore()
    for other in (near, far):
        pl.semaphore_signal(barrier, inc=1, device_id={"tp": other}, device_id_type=MESH)
    pl.semaphore_wait(barrier, 2)

    def columns(p):
        return pl.ds(pl.multiple_of(p * step, step), step)

    def term(owner, p):
        rows = pl.ds(pl.multiple_of(owner * size, size), size)
        return jnp.dot(x_ref[rows, :], w_ref[:, columns(p)], preferred_element_type=jnp.float32)

    def send(src, dst, sems, p, target):
        return pltpu.make_async_remote_copy(
            src_ref=src.at[p],
            dst_ref=dst.at[p],
            send_sem=sems[0].at[p],
            recv_sem=sems[1].at[p],
            device_id={"tp": target},
            device_id_type=MESH,
        )

    def pair(p):
        return send(pair_out, pair_in, (pair_send, pair_recv), p, near)

    def across(p):
        return send(far_out, far_in, (far_send, far_recv), p, far)

    def beside(p):
        return send(near_out, near_in, (near_send, near_recv), p, near)

    @pl.loop(0, pieces)
    def _(p):
        pair_out[p] = term(opposite, p).astype(jnp.bfloat16)
        pair(p).start()
        mine = term(far, p)
        pair(p).wait_recv()
        far_out[p] = (mine + pair_in[p].astype(jnp.float32)).astype(jnp.bfloat16)
        across(p).start()

    @pl.loop(0, pieces)
    def _(p):
        near_out[p] = term(near, p).astype(jnp.bfloat16)
        beside(p).start()

    @pl.loop(0, pieces)
    def _(p):
        own = term(me, p)
        beside(p).wait_recv()
        out_ref[:, columns(p)] = own + near_in[p].astype(jnp.float32)

    @pl.loop(0, pieces)
    def _(p):
        across(p).wait_recv()
        out_ref[:, columns(p)] += far_in[p].astype(jnp.float32)

    @pl.loop(0, pieces)
    def _(p):
        pair(p).wait_send()
        across(p).wait_send()
        beside(p).wait_send()


def product_rows(x, w, tag):
    if lax.axis_size("tp") != 4:
        partial = jnp.dot(x, w, preferred_element_type=jnp.float32).astype(jnp.bfloat16)
        return lax.psum_scatter(partial, "tp", scatter_dimension=0, tiled=True).astype(
            jnp.float32
        )
    pieces = 4
    rows, wide = x.shape[0] // 4, w.shape[1]
    vmem = pl.BlockSpec(memory_space=pltpu.VMEM)
    slots = pltpu.VMEM((pieces, rows, wide // pieces), jnp.bfloat16)
    return pl.pallas_call(
        functools.partial(product_kernel, pieces),
        out_shape=jax.ShapeDtypeStruct((rows, wide), jnp.float32),
        in_specs=[vmem] * 2,
        out_specs=vmem,
        scratch_shapes=[slots] * 6 + [pltpu.SemaphoreType.DMA((pieces,))] * 6,
        compiler_params=pltpu.CompilerParams(
            collective_id=tag, has_side_effects=True, vmem_limit_bytes=40 * 1024 * 1024
        ),
        cost_estimate=pl.CostEstimate(
            flops=30_000_000_000, bytes_accessed=2 * w.size, transcendentals=0
        ),
    )(x, w)


def walk_kernel(count, pieces, x_ref, out_ref, own_sem, send_sem, recv_sem):
    me = lax.axis_index("sp")
    odd = lax.rem(me, 2)
    place = me // 2 + odd * (count - 1 - 2 * (me // 2))
    size = x_ref.shape[0]
    step = size // (2 * pieces)

    def index(position):
        position = lax.rem(position + 2 * count, count)
        back = position // (count // 2)
        return (1 - back) * 2 * position + back * (2 * (count - 1 - position) + 1)

    ways = (1, -1)
    barrier = pltpu.get_barrier_semaphore()
    for way in ways:
        pl.semaphore_signal(
            barrier, inc=1, device_id={"sp": index(place + way)}, device_id_type=MESH
        )
    pl.semaphore_wait(barrier, 2)

    def hop(w, t, p, age, own=False):
        inner = (w * pieces + p) * step
        owner = index(place - ways[w] * age)
        dst = out_ref.at[pl.ds(pl.multiple_of(owner * size + inner, step), step)]
        return pltpu.make_async_remote_copy(
            src_ref=x_ref.at[pl.ds(inner, step)] if own else dst,
            dst_ref=dst,
            send_sem=send_sem.at[w, p, t],
            recv_sem=recv_sem.at[w, p, t],
            device_id={"sp": index(place + ways[w])},
            device_id_type=MESH,
        )

    for p in range(pieces):
        for w in range(2):
            hop(w, 0, p, 0, True).start()
    whole = pl.ds(pl.multiple_of(me * size, size), size)
    own = pltpu.make_async_copy(x_ref, out_ref.at[whole], own_sem)
    own.start()

    @pl.loop(1, count - 1)
    def _(t):
        for p in range(pieces):
            for w in range(2):
                hop(w, t - 1, p, t).wait_recv()
                hop(w, t, p, t).start()

    own.wait()
    for p in range(pieces):
        for w in range(2):
            hop(w, count - 2, p, count - 1).wait_recv()
            hop(w, 0, p, 0, True).wait_send()

    @pl.loop(1, count - 1)
    def _(t):
        for p in range(pieces):
            for w in range(2):
                hop(w, t, p, t).wait_send()


def walk_gather(x, pieces):
    count = lax.axis_size("sp")
    if count % 2 or count < 4 or x.shape[0] % (32 * pieces):
        return lax.all_gather(x, "sp", axis=0, tiled=True)
    vmem = pl.BlockSpec(memory_space=pltpu.VMEM)
    return pl.pallas_call(
        functools.partial(walk_kernel, count, pieces),
        out_shape=jax.ShapeDtypeStruct((count * x.shape[0], x.shape[1]), x.dtype),
        in_specs=[vmem],
        out_specs=vmem,
        scratch_shapes=[pltpu.SemaphoreType.DMA]
        + [pltpu.SemaphoreType.DMA((2, pieces, count - 1))] * 2,
        compiler_params=pltpu.CompilerParams(
            collective_id=4, has_side_effects=True, vmem_limit_bytes=16 * 1024 * 1024
        ),
        cost_estimate=pl.CostEstimate(
            flops=30_000_000_000, bytes_accessed=count * x.size, transcendentals=0
        ),
    )(x)


def layer_kernel(
    count,
    heads,
    up_pieces,
    down_pieces,
    logs_ref,
    gain_ref,
    norm_gain_ref,
    gate_taps_ref,
    value_taps_ref,
    q_hbm,
    k_hbm,
    v_hbm,
    gate_hbm,
    residual_hbm,
    wo_ref,
    gate_w_ref,
    value_w_ref,
    down_w_ref,
    out_ref,
    q_ref,
    k_ref,
    v_ref,
    gate_ref,
    residual_ref,
    rows_ref,
    cols_ref,
    state_ref,
    held,
    memory,
    normer,
    running,
    pair_memory,
    pair_normer,
    pair_level,
    handed,
    gated,
    mine,
    wo_full,
    middle,
    give_up,
    give_down,
    full_up,
    full_down,
    total_rows,
    stream,
    group,
    up_tile,
    up_other,
    hidden,
    pair_out,
    pair_in,
    second_out,
    second_in,
    third_out,
    third_in,
    kept,
    blocks_of,
    load_sem,
    wo_sem,
    give_sem,
    state_send,
    state_recv,
    up_send,
    up_recv,
    down_send,
    down_recv,
    block_send,
    block_recv,
    rows_send,
    rows_recv,
    sum_send,
    sum_recv,
    edge_sem,
):
    me = lax.axis_index("sp")
    tp = lax.axis_index("tp")
    core = lax.rem(tp, 2)
    chip = tp // 2
    near = tp + 1 - 2 * core
    far = lax.rem(tp + 2, 4)
    opposite = lax.rem(near + 2, 4)
    odd = lax.rem(me, 2)
    partner = me + 1 - 2 * odd
    line = count // 2
    place = me // 2
    model = full_up.shape[0]
    lane = 128
    up_rows = model // count
    up_step = 2 * up_rows // up_pieces
    half_width = full_down.shape[1]
    tiles = half_width // lane
    rest = half_width - tiles * lane
    wide = full_down.shape[2]
    down_step = 2 * half_width // down_pieces

    barrier = pltpu.get_barrier_semaphore()
    for other in (near, far, opposite):
        pl.semaphore_signal(barrier, inc=1, device_id={"tp": other}, device_id_type=MESH)
    for other in (partner, lax.rem(me + 2, count), lax.rem(me + count - 2, count)):
        pl.semaphore_signal(barrier, inc=1, device_id={"sp": other}, device_id_type=MESH)

    own_up = pl.ds(pl.multiple_of(me * up_rows, up_rows), up_rows)
    wo_rows = wo_ref.shape[0]
    wo_own = pl.ds(pl.multiple_of(tp * wo_rows, wo_rows), wo_rows)
    loads = []

    def load(src, dst):
        loads.append(pltpu.make_async_copy(src, dst, load_sem.at[len(loads)]))

    shift = tiles * lane + 2 * rest
    for i in range(tiles):
        for a, w_ref in enumerate((gate_w_ref, value_w_ref)):
            lanes = pl.ds((2 * i + a) * lane, lane)
            for to, y in ((full_up.at[own_up, lanes], odd), (give_up.at[:, lanes], 1 - odd)):
                at = pl.multiple_of(y * shift + i * lane, lane)
                load(w_ref.at[:, pl.ds(at, lane)], to)
    for a, w_ref in enumerate((gate_w_ref, value_w_ref)):
        load(w_ref.at[:, pl.ds(tiles * lane, lane)], middle.at[a])
    first_loads = len(loads)
    load(k_hbm, k_ref)
    load(v_hbm, v_ref)
    load(wo_ref, wo_full.at[wo_own])
    soon_loads = len(loads)
    for to, y in ((full_down.at[me], odd), (give_down, 1 - odd)):
        at = pl.multiple_of(y * shift, rest)
        load(down_w_ref.at[pl.ds(at, tiles * lane)], to.at[pl.ds(0, tiles * lane)])
        at = pl.multiple_of(tiles * lane + y * rest, rest)
        load(down_w_ref.at[pl.ds(at, rest)], to.at[pl.ds(tiles * lane, rest)])
    load(q_hbm, q_ref)
    load(gate_hbm, gate_ref)
    load(residual_hbm, residual_ref)
    for one in loads[:first_loads]:
        one.start()
    for one in loads[first_loads:]:
        one.start()
    for one in loads[:first_loads]:
        one.wait()

    def remote(src, dst, send_sem, recv_sem, **to):
        return pltpu.make_async_remote_copy(
            src_ref=src,
            dst_ref=dst,
            send_sem=send_sem,
            recv_sem=recv_sem,
            device_id=to,
            device_id_type=MESH,
        )

    at_lane = lax.broadcasted_iota(jnp.int32, (up_rows, lane), 1)
    first_half = at_lane < rest

    def halves_of(g, v, low):
        a = jnp.where(low, g, pltpu.roll(v, rest, 1))
        b = jnp.where(low, pltpu.roll(g, rest, 1), v)
        return a, b

    mid_a, mid_b = halves_of(
        middle[0].astype(jnp.float32), middle[1].astype(jnp.float32), first_half
    )
    tail = slice(2 * tiles * lane, 2 * tiles * lane + lane)
    full_up[own_up, tail] = jnp.where(odd == 0, mid_a, mid_b).astype(jnp.bfloat16)
    give_up[:, tail] = jnp.where(odd == 0, mid_b, mid_a).astype(jnp.bfloat16)

    give_step = up_rows // 2

    def give_rows(p):
        at = pl.multiple_of(me * up_rows + p * give_step, give_step)
        return remote(
            give_up.at[pl.ds(p * give_step, give_step)],
            full_up.at[pl.ds(at, give_step)],
            give_sem.at[0, p],
            give_sem.at[1, p],
            sp=partner,
        )

    give_cols = remote(give_down, full_down.at[me], give_sem.at[0, 2], give_sem.at[1, 2], sp=partner)
    wo_pieces = wo_sem.shape[2]
    wo_step = wo_rows // 2 // wo_pieces

    def wo_copy(kind, owner, y, s, **to):
        at = pl.multiple_of(owner * wo_rows + (y * wo_pieces + s) * wo_step, wo_step)
        part = wo_full.at[pl.ds(at, wo_step)]
        return remote(part, part, wo_sem.at[0, kind, s], wo_sem.at[1, kind, s], **to)

    def wo_shard(owner):
        part = wo_full.at[pl.ds(pl.multiple_of(owner * wo_rows, wo_rows), wo_rows)]
        return remote(part, part, wo_sem.at[0, 0, 0], wo_sem.at[1, 0, 0], tp=near)

    def wo_onward(s):
        wo_copy(1, far, odd, s, tp=far).wait_recv()
        wo_copy(2, far, odd, s, sp=partner).start()
        wo_copy(3, far, odd, s, tp=near).start()

    def source(w, t):
        return place - t if w == 0 else place + t

    def has(w, t):
        return place >= t if w == 0 else place + t < line

    def sends(w, t):
        onward = place + 1 < line if w == 0 else place > 0
        return has(w, t) & onward & (t < line - 1)

    def beyond(w):
        return lax.rem(me + 2, count) if w == 0 else lax.rem(me + count - 2, count)

    def up_hop(w, t, m):
        at = source(w, t) * 2 * up_rows + lax.rem(m + odd * (up_pieces // 2), up_pieces) * up_step
        part = full_up.at[pl.ds(pl.multiple_of(at, up_step), up_step)]
        return remote(part, part, up_send.at[w, t, m], up_recv.at[w, t, m], sp=beyond(w))

    def down_hop(w, t, m):
        each = down_pieces // 2
        owner = source(w, t) * 2 + m // each
        at = lax.rem(m, each) * down_step
        part = full_down.at[owner, pl.ds(pl.multiple_of(at, down_step), down_step)]
        return remote(part, part, down_send.at[w, t, m], down_recv.at[w, t, m], sp=beyond(w))

    up_ticks = line * up_pieces
    all_ticks = up_ticks + line * down_pieces

    at_end = (place == 0) | (place == line - 1)

    def move(hop, pieces, n):
        t = n // pieces
        m = lax.rem(n, pieces)
        for w in range(2):
            due = sends(w, t)
            if hop is down_hop:
                due = due & ((t > 0) | jnp.logical_not(at_end))

            @pl.when(has(w, t) & (t > 0))
            def _():
                hop(w, t - 1, m).wait_recv()

            @pl.when(due)
            def _():
                hop(w, t, m).start()

    def up_tick(n):
        for p in range(2):

            @pl.when(n == up_pieces // 2 + p * (up_pieces // 4))
            def _():
                give_rows(p).wait_recv()

        move(up_hop, up_pieces, n)

    def down_tick(n):
        @pl.when((n == 0) & jnp.logical_not(at_end))
        def _():
            give_cols.wait_recv()

        move(down_hop, down_pieces, n)

    def late_tick(n):
        @pl.when((n >= up_ticks) & (n < all_ticks))
        def _():
            down_tick(n - up_ticks)

    def tick(n):
        @pl.when((n < up_pieces) | jnp.logical_not(at_end))
        def _():
            @pl.when(n < up_ticks)
            def _():
                up_tick(n)

            late_tick(n)

    def up_sent(n):
        t = n // up_pieces
        for w in range(2):

            @pl.when(sends(w, t))
            def _():
                up_hop(w, t, lax.rem(n, up_pieces)).wait_send()

    pl.semaphore_wait(barrier, 6)
    for n in range(2):
        up_tick(n)
    give_rows(0).start()
    for one in loads[first_loads:soon_loads]:
        one.wait()
    for s in range(wo_pieces):
        wo_copy(1, tp, odd, s, tp=far).start()
    wo_shard(tp).start()

    key_width = memory.shape[1]
    value_width = memory.shape[2]
    span = key_width + STATE_PAD
    swap = remote(state_ref, held.at[0], state_send.at[0], state_recv.at[0], sp=partner)
    hand = remote(handed, held.at[1], state_send.at[1], state_recv.at[1], sp=beyond(0))

    def read_state(ref, h):
        low = h * span
        extra = ref[low + key_width : low + span, :].astype(jnp.float32)
        total = extra[2:3, :1] + extra[3:4, :1]
        level = extra[4:5, :1] + extra[5:6, :1]
        parts = extra[0:1, :key_width] + extra[1:2, :key_width]
        return ref[low : low + key_width, :].astype(jnp.float32), parts, level, total

    def join(first, second, total):
        mem_a, norm_a, level_a = first
        mem_b, norm_b, level_b = second
        after = jnp.maximum(total + level_a, level_b)
        one = jnp.exp(total + level_a - after)
        two = jnp.exp(level_b - after)
        return one * mem_a + two * mem_b, one * norm_a + two * norm_b, after

    def keep(refs, h, values):
        mem, norm, level = values
        refs[0][h] = mem
        refs[1][h, :1, :] = norm
        refs[2][h] = jnp.broadcast_to(level, refs[2].shape[1:])

    carried_refs = (memory, normer, running)

    def write_state(ref, h, mem, norm, level, total):
        low = h * span
        ref[low : low + key_width, :] = mem.astype(jnp.bfloat16)
        lines = jnp.zeros((STATE_PAD, value_width), jnp.float32)
        at_line = lax.broadcasted_iota(jnp.int32, lines.shape, 0)
        norm = jnp.concatenate([norm] * (value_width // key_width), axis=1)
        for i, part in enumerate((norm, total, level)):
            high = part.astype(jnp.bfloat16).astype(jnp.float32)
            lines = jnp.where(at_line == 2 * i, high, lines)
            lines = jnp.where(at_line == 2 * i + 1, part - high, lines)
        ref[low + key_width : low + span, :] = lines.astype(jnp.bfloat16)

    length = BLOCK
    blocks = q_ref.shape[0] // length
    at_row = lax.broadcasted_iota(jnp.int32, (length, length), 0)
    at_col = lax.broadcasted_iota(jnp.int32, (length, length), 1)

    def by_block(first):
        return jnp.concatenate(
            [
                logs_ref[first : first + heads, b * length : (b + 1) * length]
                for b in range(blocks)
            ],
            axis=0,
        )

    within = jnp.dot(
        by_block(heads),
        jnp.where(at_row <= at_col, 1.0, 0.0),
        precision=lax.Precision.HIGHEST,
        preferred_element_type=jnp.float32,
    )
    shifted_all = by_block(0) - within
    each_all = within[:, length - 1 : length]
    after = jnp.zeros((heads, 1), jnp.float32)
    to_end = [None] * blocks
    for b in reversed(range(blocks)):
        part = slice(b * heads, (b + 1) * heads)
        after = after + each_all[part]
        to_end[b] = shifted_all[part] + after
    own_total = after
    own_level = functools.reduce(jnp.maximum, to_end)
    own_level = jnp.max(own_level, axis=1, keepdims=True)
    for b in range(blocks):
        part = slice(b * heads, (b + 1) * heads)
        rows_ref[b, 0 : 2 * heads, :] = jnp.concatenate(
            [shifted_all[part], jnp.broadcast_to(each_all[part], (heads, length))], axis=0
        )
        lines = [within[part], shifted_all[part], jnp.exp(to_end[b] - own_level)]
        lines.append(jnp.zeros((length - 3 * heads, length), jnp.float32))
        cols_ref[b * length : (b + 1) * length, :] = jnp.transpose(
            jnp.concatenate(lines, axis=0)
        )

    memory[...] = jnp.zeros_like(memory)
    normer[...] = jnp.zeros_like(normer)

    @pl.loop(0, blocks)
    def _(j):
        rows = pl.ds(pl.multiple_of(j * length, length), length)
        cols = cols_ref[rows, :]
        for h in range(heads):
            k = k_ref[rows, h * key_width : (h + 1) * key_width]
            v = v_ref[rows, h * value_width : (h + 1) * value_width]
            weighted = k.astype(jnp.float32) * cols[:, 2 * heads + h : 2 * heads + h + 1]
            memory[h] += lax.dot_general(
                weighted.astype(jnp.bfloat16),
                v,
                (((0,), (0,)), ((), ())),
                preferred_element_type=jnp.float32,
            )
            normer[h, :1, :] += jnp.sum(weighted, axis=0, keepdims=True)

    for h in range(heads):
        write_state(
            state_ref,
            h,
            memory[h],
            normer[h, :1, :],
            own_level[h : h + 1, :],
            own_total[h : h + 1, :],
        )
    swap.start()
    give_rows(1).start()
    for one in loads[soon_loads:]:
        one.wait()
    swap.wait_recv()
    for s in range(wo_pieces // 2):
        wo_onward(s)

    @pl.when(odd == 0)
    def _():
        for h in range(heads):
            mem_a, norm_a, level_a, total_a = read_state(state_ref, h)
            mem_b, norm_b, level_b, total_b = read_state(held.at[0], h)
            out = join((mem_a, norm_a, level_a), (mem_b, norm_b, level_b), total_b)
            keep((pair_memory, pair_normer, pair_level.at[0]), h, out)
            pair_level[1, h] = jnp.broadcast_to(total_a + total_b, pair_level.shape[2:])

    @pl.when(odd == 1)
    def _():
        for h in range(heads):
            mem_a, norm_a, level_a, total_a = read_state(held.at[0], h)
            mem_b, norm_b, level_b, total_b = read_state(state_ref, h)
            out = join((mem_a, norm_a, level_a), (mem_b, norm_b, level_b), total_b)
            keep((pair_memory, pair_normer, pair_level.at[0]), h, out)
            pair_level[1, h] = jnp.broadcast_to(total_a + total_b, pair_level.shape[2:])

    started = jnp.minimum(FIRST_TICKS + NEXT_TICKS * place, jnp.where(at_end, up_pieces, up_ticks))

    @pl.loop(2, started)
    def _(n):
        up_sent(n - 2)
        up_tick(n)

    memory[...] = jnp.zeros_like(memory)
    normer[...] = jnp.zeros_like(normer)
    running[...] = jnp.full(running.shape, neg_large, jnp.float32)

    @pl.when(place > 0)
    def _():
        hand.wait_recv()
        for h in range(heads):
            mem, parts, level, total = read_state(held.at[1], h)
            keep(carried_refs, h, (mem, parts, level))

    @pl.when(place + 1 < line)
    def _():
        for h in range(heads):
            mem, norm, level = join(
                (memory[h], normer[h, :1, :], running[h, :1, :1]),
                (pair_memory[h], pair_normer[h, :1, :], pair_level[0, h, :1, :1]),
                pair_level[1, h, :1, :1],
            )
            write_state(handed, h, mem, norm, level, jnp.zeros_like(level))
        hand.start()

    @pl.when(odd == 1)
    def _():
        for h in range(heads):
            mem, norm, level, total = read_state(held.at[0], h)
            out = join(
                (memory[h], normer[h, :1, :], running[h, :1, :1]), (mem, norm, level), total
            )
            keep(carried_refs, h, out)

    scale = key_width ** (-0.5)
    causal = at_col <= at_row
    size = residual_ref.shape[0]
    per = size // length

    def block_copy(j, sender):
        at = pl.multiple_of(lax.rem(j, per) * length, length)
        width = gated.shape[1]
        return remote(
            gated.at[pl.ds(pl.multiple_of(j * length, length), length)],
            mine.at[sender, pl.ds(at, length)],
            block_send.at[j],
            block_recv.at[sender, lax.rem(j, per)],
            tp=j // per,
        )

    @pl.loop(0, blocks)
    def _(j):
        tick(started + j)

        @pl.when(j < wo_pieces // 2)
        def _():
            wo_onward(wo_pieces // 2 + j)

        @pl.when(j == wo_pieces // 2)
        def _():
            give_cols.start()

        @pl.when(j >= blocks - wo_pieces)
        def _():
            s = j - (blocks - wo_pieces)
            wo_copy(2, far, 1 - odd, s, sp=partner).wait_recv()
            wo_copy(4, far, 1 - odd, s, tp=near).start()

        rows = pl.ds(pl.multiple_of(j * length, length), length)
        lanes = rows_ref[j]
        cols = cols_ref[rows, :]
        for h in range(heads):
            keys = slice(h * key_width, (h + 1) * key_width)
            vals = slice(h * value_width, (h + 1) * value_width)
            q = q_ref[rows, keys]
            k = k_ref[rows, keys]
            v = v_ref[rows, vals]
            before = running[h, :1, :1]
            total = lanes[heads + h : heads + h + 1, :1]
            shifted_log = jnp.where(causal, lanes[h : h + 1, :], -jnp.inf)
            top = jnp.maximum(jnp.max(shifted_log, axis=1, keepdims=True), before)
            raw = (
                lax.dot_general(
                    q, k, (((1,), (1,)), ((), ())), preferred_element_type=jnp.float32
                )
                * scale
            )
            scores = raw * jnp.exp(shifted_log - top)
            carry = jnp.exp(before - top) * scale
            state = memory[h]
            high = state.astype(jnp.bfloat16)
            low = (state - high.astype(jnp.float32)).astype(jnp.bfloat16)
            carried = jnp.dot(q, high, preferred_element_type=jnp.float32) + jnp.dot(
                q, low, preferred_element_type=jnp.float32
            )
            numerator = carry * carried + jnp.dot(
                scores.astype(jnp.bfloat16), v, preferred_element_type=jnp.float32
            )
            denominator = carry * jnp.sum(
                q.astype(jnp.float32) * normer[h, :1, :], axis=1, keepdims=True
            ) + jnp.sum(scores, axis=1, keepdims=True)
            level = cols[:, h : h + 1] + top
            value = numerator / jnp.maximum(jnp.abs(denominator), jnp.exp(-level))
            mean = jnp.mean(value * value, axis=1, keepdims=True)
            normed = value * lax.rsqrt(mean + eps) * gain_ref[h : h + 1, :]
            gate = normed * jax.nn.sigmoid(gate_ref[rows, vals].astype(jnp.float32))
            gated[rows, vals] = gate.astype(gated.dtype)
            last = jnp.max(jnp.maximum(lanes[h : h + 1, :], before), axis=1, keepdims=True)
            decay = jnp.exp(before - last)
            weighted = k.astype(jnp.float32) * jnp.exp(cols[:, heads + h : heads + h + 1] - last)
            memory[h] = decay * state + lax.dot_general(
                weighted.astype(jnp.bfloat16),
                v,
                (((0,), (0,)), ((), ())),
                preferred_element_type=jnp.float32,
            )
            normer[h, :1, :] = decay * normer[h, :1, :] + jnp.sum(
                weighted, axis=0, keepdims=True
            )
            running[h] = jnp.broadcast_to(last + total, running.shape[1:])

        @pl.when(j // per == tp)
        def _():
            at = pl.multiple_of(lax.rem(j, per) * length, length)
            mine[tp, pl.ds(at, length), :] = gated[rows, :]

        @pl.when(j // per != tp)
        def _():
            block_copy(j, tp).start()

    reached = started + blocks
    wo_shard(near).wait_recv()
    for s in range(wo_pieces):
        wo_copy(3, opposite, odd, s, tp=near).wait_recv()
        wo_copy(4, opposite, 1 - odd, s, tp=near).wait_recv()

    @pl.loop(0, 4)
    def _(s):
        tick(reached + s)

        @pl.when(s != tp)
        def _():
            for p in range(per):
                block_copy(tp * per + p, s).wait_recv()

    reached = reached + 4

    @pl.when(at_end)
    def _():
        give_cols.wait_recv()
        for w in range(2):

            @pl.when(sends(w, 0))
            def _():
                for m in range(down_pieces):
                    down_hop(w, 0, m).start()

    def columns(i):
        return pl.ds(pl.multiple_of(i * wide, wide), wide)

    @pl.loop(0, model // wide)
    def _(i):
        total = jnp.zeros((size, wide), jnp.float32)
        for s in range(4):
            total += jnp.dot(
                mine[s],
                wo_full[s * wo_rows : (s + 1) * wo_rows, columns(i)],
                preferred_element_type=jnp.float32,
            )
        total_rows[:, columns(i)] = total

    pad = PAD_ROWS
    tokens = 8 * size
    row_pieces = rows_send.shape[1]
    row_step = size // row_pieces

    def row_copy(kind, y, owner, p, **to):
        at = pad + (y * 4 + owner) * size + p * row_step
        part = group.at[pl.ds(pl.multiple_of(at, pad), row_step)]
        return remote(part, part, rows_send.at[kind, p], rows_recv.at[kind, p], **to)

    @pl.when(place == 0)
    def _():
        group[0:pad, :] = jnp.zeros((pad, model), group.dtype)

    @pl.loop(0, row_pieces)
    def _(p):
        rows = pl.ds(pl.multiple_of(p * row_step, row_step), row_step)
        rounded = (residual_ref[rows, :].astype(jnp.float32) + total_rows[rows, :]).astype(
            jnp.bfloat16
        )
        stream[rows, :] = rounded
        x = rounded.astype(jnp.float32)
        normed = x * lax.rsqrt(jnp.mean(x * x, axis=-1, keepdims=True) + eps) * norm_gain_ref[...]
        at = pl.multiple_of(pad + (odd * 4 + tp) * size + p * row_step, pad)
        group[pl.ds(at, row_step), :] = normed.astype(jnp.bfloat16)
        row_copy(0, odd, tp, p, tp=far).start()
        row_copy(2, odd, tp, p, sp=partner).start()
        row_copy(1, odd, tp, p, tp=near).start()

    @pl.loop(0, row_pieces)
    def _(p):
        tick(reached + 2 * p)
        row_copy(0, odd, far, p, tp=far).wait_recv()
        row_copy(3, odd, far, p, tp=near).start()

        @pl.when(lax.rem(p, 2) == 0)
        def _():
            row_copy(6, odd, far, p, sp=partner).start()

        tick(reached + 2 * p + 1)
        row_copy(2, 1 - odd, tp, p, sp=partner).wait_recv()
        row_copy(4, 1 - odd, tp, p, tp=near).start()

        @pl.when(lax.rem(p, 2) == 1)
        def _():
            row_copy(6, 1 - odd, tp, p, tp=far).start()

    reached = reached + 2 * row_pieces

    @pl.loop(0, row_pieces)
    def _(p):
        tick(reached + p)
        row_copy(6, 1 - odd, far, p, sp=partner).wait_recv()
        row_copy(5, 1 - odd, far, p, tp=near).start()
        row_copy(1, odd, near, p, tp=near).wait_recv()
        row_copy(3, odd, opposite, p, tp=near).wait_recv()
        row_copy(4, 1 - odd, near, p, tp=near).wait_recv()

    reached = reached + row_pieces

    @pl.loop(0, row_pieces)
    def _(p):
        row_copy(5, 1 - odd, opposite, p, tp=near).wait_recv()

    edge = remote(
        group.at[pl.ds(tokens, pad)],
        group.at[pl.ds(0, pad)],
        edge_sem.at[0],
        edge_sem.at[1],
        sp=beyond(0),
    )

    @pl.when(place + 1 < line)
    def _():
        edge.start()

    @pl.loop(jnp.where(at_end, up_pieces, jnp.minimum(reached, up_ticks)), up_ticks)
    def _(n):
        up_tick(n)

    reached = jnp.maximum(reached, up_ticks)
    early = up_ticks + jnp.where(at_end, 1, 2) * down_pieces
    parts = 4
    up_tiles = (up_tile, up_other)
    part_rows = tokens // parts

    def silu(a):
        return a * jax.nn.sigmoid(a)

    @pl.loop(0, parts)
    def _(b):
        part = lax.rem(b + 1, parts)
        at = pl.multiple_of(part * part_rows, part_rows)
        window = pl.ds(at, part_rows + pad)
        outs = pl.ds(at, part_rows)

        @pl.when((b == parts - 1) & (place > 0))
        def _():
            edge.wait_recv()

        for m in range(UPS_TICKS):
            n = reached + b * UPS_TICKS + m

            @pl.when(n < early)
            def _():
                tick(n)

        def conv(ref, taps, width):
            return (
                taps[0:1, :] * ref[pad - 2 : pad - 2 + part_rows, width]
                + taps[1:2, :] * ref[pad - 1 : pad - 1 + part_rows, width]
                + taps[2:3, :] * ref[pad : pad + part_rows, width]
            )

        def product(i):
            ref = up_tiles[i % 2]
            if i < tiles:
                ref[...] = jnp.dot(
                    group[window, :],
                    full_up[:, 2 * i * lane : 2 * (i + 1) * lane],
                    preferred_element_type=jnp.float32,
                )
            else:
                ref[:, 0:lane] = jnp.dot(
                    group[window, :], full_up[:, tail], preferred_element_type=jnp.float32
                )

        def finish(i):
            ref = up_tiles[i % 2]
            if i < tiles:
                taps_at = pl.ds(pl.multiple_of(odd * shift + i * lane, lane), lane)
                act = silu(conv(ref, gate_taps_ref[:, taps_at], slice(0, lane))) * conv(
                    ref, value_taps_ref[:, taps_at], slice(lane, 2 * lane)
                )
                hidden[outs, i * lane : (i + 1) * lane] = act.astype(jnp.bfloat16)
            else:
                mid = slice(tiles * lane, (tiles + 1) * lane)
                low = lax.broadcasted_iota(jnp.int32, (3, lane), 1) < rest
                taps_a, taps_b = halves_of(gate_taps_ref[:, mid], value_taps_ref[:, mid], low)
                both = conv(ref, jnp.where(odd == 0, taps_a, taps_b), slice(0, lane))
                act = silu(both) * pltpu.roll(both, rest, 1)
                hidden[outs, tiles * lane : tiles * lane + rest] = act[:, :rest].astype(
                    jnp.bfloat16
                )

        product(0)
        for i in range(tiles):
            product(i + 1)
            finish(i)
        finish(tiles)

    @pl.loop(jnp.minimum(reached + parts * UPS_TICKS, early), early)
    def _(n):
        tick(n)

    both_sides = jnp.minimum(place, line - 1 - place)

    def away(k):
        return jnp.where(k <= 2 * both_sides, (k + 1) // 2, k - both_sides)

    def unit(k):
        rising = jnp.where(place < line - 1 - place, 1, -1)
        way = jnp.where(k <= 2 * both_sides, 1 - 2 * lax.rem(k, 2), rising)
        return place + way * away(k)

    def sum_copy(kind, i):
        src, dst, to = (
            (pair_out.at[i], pair_in.at[i], {"tp": near}),
            (second_out.at[i, 0], second_in.at[i, 0], {"tp": far}),
            (second_out.at[i, 1], second_in.at[i, 1], {"sp": partner}),
            (third_out.at[i, 0], third_in.at[i, 0], {"sp": partner}),
            (third_out.at[i, 1], third_in.at[i, 1], {"tp": far}),
        )[kind]
        return remote(src, dst, sum_send.at[kind, i], sum_recv.at[kind, i], **to)

    part_wide = wide // 2
    cut = (slice(0, part_wide), slice(part_wide, wide))

    def term(i, a, b, side):
        y = lax.rem(odd + a, 2)
        x = lax.rem(chip + b, 2)
        owner = 2 * x + lax.rem(core + side, 2)
        rows = pl.ds(pl.multiple_of((y * 4 + owner) * size, size), size)
        return jnp.dot(hidden[rows, :], full_down[i], preferred_element_type=jnp.float32)

    def first_stage(i):
        for a in range(2):
            for b in range(2):
                pair_out[i, 2 * a + b] = term(i, a, b, 1).astype(jnp.bfloat16)
        sum_copy(0, i).start()
        for a in range(2):
            for b in range(2):
                blocks_of[2 * a + b] = term(i, a, b, 0)

    def second_stage(i):
        sum_copy(0, i).wait_recv()

        def block(a, b, side):
            at = 2 * a + b
            return blocks_of[at, :, cut[side]] + pair_in[i, at, :, cut[side]].astype(jnp.float32)

        for a in range(2):
            second_out[i, 0, a] = block(a, 1, 0).astype(jnp.bfloat16)
        sum_copy(1, i).start()
        for b in range(2):
            second_out[i, 1, b] = block(1, b, 1).astype(jnp.bfloat16)
        sum_copy(2, i).start()
        for a in range(2):
            kept[i, 0, a] = block(a, 0, 0)
        for b in range(2):
            kept[i, 1, b] = block(0, b, 1)

    def third_stage(i):
        for side in range(2):
            sum_copy(1 + side, i).wait_recv()
            third_out[i, side] = (
                kept[i, side, 1] + second_in[i, side, 1].astype(jnp.float32)
            ).astype(jnp.bfloat16)
            sum_copy(3 + side, i).start()
            kept[i, side, 0] += second_in[i, side, 0].astype(jnp.float32)

    def last_stage(i):
        for side in range(2):
            sum_copy(3 + side, i).wait_recv()
            at = pl.multiple_of(i * wide + side * part_wide, part_wide)
            cols = pl.ds(at, part_wide)
            out_ref[:, cols] = (
                stream[:, cols].astype(jnp.float32)
                + (kept[i, side, 0] + third_in[i, side].astype(jnp.float32))
            ).astype(out_ref.dtype)

    def slice_at(n):
        return 2 * unit(n // 2) + lax.rem(n, 2)

    def due(k, j):
        return up_ticks + down_pieces * away(k) + (j + 1) * (down_pieces // 2)

    def until(n):
        k = n // 2
        last = jnp.where(k > 0, due(jnp.maximum(k - 1, 0), 1), early)
        return jnp.maximum(jnp.maximum(due(k, lax.rem(n, 2)), last), early)

    @pl.loop(0, count)
    def _(n):
        @pl.when(n > 0)
        def _():
            @pl.loop(until(n - 1), until(n))
            def _(at):
                late_tick(at)

        first_stage(slice_at(n))

        @pl.when(n > 1)
        def _():
            third_stage(slice_at(n - 2))

        second_stage(slice_at(n))

    for n in (count - 2, count - 1):
        third_stage(slice_at(n))

    @pl.loop(0, count)
    def _(n):
        last_stage(slice_at(n))

    swap.wait_send()

    @pl.when(place + 1 < line)
    def _():
        hand.wait_send()
        edge.wait_send()

    for p in range(2):
        give_rows(p).wait_send()
    wo_shard(tp).wait_send()
    for s in range(wo_pieces):
        for kind in range(1, 5):
            wo_copy(kind, tp, 0, s, tp=near).wait_send()
    give_cols.wait_send()

    @pl.loop(0, blocks)
    def _(j):
        @pl.when(j // per != tp)
        def _():
            block_copy(j, tp).wait_send()

    @pl.loop(0, row_pieces)
    def _(p):
        for kind in range(7):
            row_copy(kind, odd, tp, p, tp=near).wait_send()

    @pl.loop(0, count)
    def _(i):
        for kind in range(5):
            sum_copy(kind, i).wait_send()

    @pl.loop(started - 2, up_ticks)
    def _(n):
        up_sent(n)

    @pl.loop(0, line - 1)
    def _(t):
        for w in range(2):

            @pl.when(sends(w, t))
            def _():
                for m in range(down_pieces):
                    down_hop(w, t, m).wait_send()


FIRST_TICKS = 4
NEXT_TICKS = 2
UPS_TICKS = 1
UP_PIECES = 8
DOWN_PIECES = 4
PAD_ROWS = 16


def one_kernel_fits(rows, gate_w, down_w):
    count = lax.axis_size("sp")
    return (
        lax.axis_size("tp") == 4
        and count >= 4
        and count % 2 == 0
        and 2 * gate_w.shape[0] % (16 * UP_PIECES) == 0
        and gate_w.shape[1] % 256 == 128
        and down_w.shape[0] % (16 * DOWN_PIECES) == 0
        and down_w.shape[1] % 256 == 0
        and rows % (2 * BLOCK) == 0
        and 4 * rows >= 6 * BLOCK
    )


def layer(q, k, v, gates, input_log, forget_log, gain, wo, residual, norm_gain, gate_w, value_w, down_w, gate_taps, value_taps):
    count = lax.axis_size("sp")
    line = count // 2
    heads = input_log.shape[1]
    tokens = q.shape[0]
    key_width = q.shape[1] // heads
    value_width = v.shape[1] // heads
    span = key_width + STATE_PAD
    model = wo.shape[1]
    rows = residual.shape[0]
    lane = 128
    half_width = gate_w.shape[1] // 2
    tiles = half_width // lane
    wide = down_w.shape[1]
    row_pieces = 4
    blocks = tokens // BLOCK
    logs = jnp.concatenate([input_log.T, forget_log.T], axis=0)
    vmem = pl.BlockSpec(memory_space=pltpu.VMEM)
    hbm = pl.BlockSpec(memory_space=pl.ANY)
    low, full = jnp.bfloat16, jnp.float32
    dma = pltpu.SemaphoreType.DMA
    return pl.pallas_call(
        functools.partial(layer_kernel, count, heads, UP_PIECES, DOWN_PIECES),
        out_shape=jax.ShapeDtypeStruct(residual.shape, low),
        in_specs=[vmem] * 5 + [hbm] * 9,
        out_specs=vmem,
        scratch_shapes=[
            pltpu.VMEM(q.shape, low),
            pltpu.VMEM(k.shape, low),
            pltpu.VMEM(v.shape, low),
            pltpu.VMEM(gates.shape, low),
            pltpu.VMEM(residual.shape, low),
            pltpu.VMEM((blocks, 8, BLOCK), full),
            pltpu.VMEM((tokens, BLOCK), full),
            pltpu.VMEM((heads * span, value_width), low),
            pltpu.VMEM((2, heads * span, value_width), low),
            pltpu.VMEM((heads, key_width, value_width), full),
            pltpu.VMEM((heads, 8, key_width), full),
            pltpu.VMEM((heads, 8, 128), full),
            pltpu.VMEM((heads, key_width, value_width), full),
            pltpu.VMEM((heads, 8, key_width), full),
            pltpu.VMEM((2, heads, 8, 128), full),
            pltpu.VMEM((heads * span, value_width), low),
            pltpu.VMEM((tokens, v.shape[1]), low),
            pltpu.VMEM((4, rows, v.shape[1]), low),
            pltpu.VMEM((model, model), low),
            pltpu.VMEM((2, gate_w.shape[0], lane), low),
            pltpu.VMEM((gate_w.shape[0], 2 * half_width), low),
            pltpu.VMEM((half_width, wide), low),
            pltpu.VMEM((model, 2 * half_width), low),
            pltpu.VMEM((count, half_width, wide), low),
            pltpu.VMEM((rows, model), full),
            pltpu.VMEM((rows, model), low),
            pltpu.VMEM((PAD_ROWS + 2 * tokens, model), low),
            pltpu.VMEM((PAD_ROWS + tokens // 2, 2 * lane), full),
            pltpu.VMEM((PAD_ROWS + tokens // 2, 2 * lane), full),
            pltpu.VMEM((2 * tokens, half_width), low),
            pltpu.VMEM((count, 4, rows, wide), low),
            pltpu.VMEM((count, 4, rows, wide), low),
            pltpu.VMEM((count, 2, 2, rows, wide // 2), low),
            pltpu.VMEM((count, 2, 2, rows, wide // 2), low),
            pltpu.VMEM((count, 2, rows, wide // 2), low),
            pltpu.VMEM((count, 2, rows, wide // 2), low),
            pltpu.VMEM((count, 2, 2, rows, wide // 2), full),
            pltpu.VMEM((4, rows, wide), full),
            dma((4 * tiles + 12,)),
            dma((2, 5, 4)),
            dma((2, 3)),
            dma((2,)),
            dma((2,)),
            dma((2, line - 1, UP_PIECES)),
            dma((2, line - 1, UP_PIECES)),
            dma((2, line - 1, DOWN_PIECES)),
            dma((2, line - 1, DOWN_PIECES)),
            dma((blocks,)),
            dma((4, rows // BLOCK)),
            dma((7, row_pieces)),
            dma((7, row_pieces)),
            dma((5, count)),
            dma((5, count)),
            dma((2,)),
        ],
        compiler_params=pltpu.CompilerParams(
            collective_id=0, has_side_effects=True, vmem_limit_bytes=63 * 1024 * 1024
        ),
        cost_estimate=pl.CostEstimate(
            flops=30_000_000_000, bytes_accessed=8 * v.size, transcendentals=0
        ),
    )(
        logs,
        gain,
        norm_gain[None, :],
        gate_taps,
        value_taps,
        q,
        k,
        v,
        gates,
        residual,
        wo,
        gate_w,
        value_w,
        down_w,
    )


def local(
    residual_entry_input,
    query_matrix_rows,
    key_matrix_rows,
    value_matrix_rows,
    output_gate_logits,
    input_gate_logits,
    forget_gate_logits,
    forget_decay_offset,
    head_norm_gain,
    cell_output_weight,
    feedforward_norm_gain,
    gate_up_weight,
    value_up_weight,
    gate_filter_taps,
    value_filter_taps,
    down_projection_weight,
):
    input_log, forget_log = gate_log_values(
        input_gate_logits, forget_gate_logits, forget_decay_offset
    )
    if one_kernel_fits(residual_entry_input.shape[0], gate_up_weight, down_projection_weight):
        return layer(
            query_matrix_rows,
            key_matrix_rows,
            value_matrix_rows,
            output_gate_logits,
            input_log,
            forget_log,
            head_norm_gain,
            cell_output_weight,
            residual_entry_input,
            feedforward_norm_gain,
            gate_up_weight,
            value_up_weight,
            down_projection_weight,
            gate_filter_taps,
            value_filter_taps,
        )
    whole_gate = lax.all_gather(gate_up_weight, "sp", axis=0, tiled=True)
    whole_down = lax.all_gather(down_projection_weight, "sp", axis=1, tiled=True)
    gated_rows = cell(
        query_matrix_rows,
        key_matrix_rows,
        value_matrix_rows,
        output_gate_logits,
        input_log,
        forget_log,
        head_norm_gain,
    )
    mixed_rows = product_rows(gated_rows, cell_output_weight, 2)
    stream_wide = residual_entry_input.astype(jnp.float32) + mixed_rows
    stream = stream_wide.astype(jnp.bfloat16)
    stream_wide = lax.optimization_barrier(stream).astype(jnp.float32)
    normed_rows = (
        stream_wide
        * lax.rsqrt(jnp.mean(stream_wide * stream_wide, axis=-1, keepdims=True) + eps)
        * feedforward_norm_gain[None, :]
    ).astype(jnp.bfloat16)
    group_rows = gather_rows(normed_rows)
    group_rows, value_shard = lax.optimization_barrier((group_rows, value_up_weight))
    whole_value = walk_gather(value_shard, 2)
    earlier_rows = shifted(group_rows[-2:], "sp", 1)
    window = jnp.concatenate([earlier_rows, group_rows], axis=0)
    up_gate = jnp.dot(
        window,
        whole_gate,
        preferred_element_type=jnp.float32,
    )
    up_value = jnp.dot(
        window,
        whole_value,
        preferred_element_type=jnp.float32,
    )
    conv_g = (
        gate_filter_taps[0][None, :] * up_gate[:-2]
        + gate_filter_taps[1][None, :] * up_gate[1:-1]
        + gate_filter_taps[2][None, :] * up_gate[2:]
    )
    conv_v = (
        value_filter_taps[0][None, :] * up_value[:-2]
        + value_filter_taps[1][None, :] * up_value[1:-1]
        + value_filter_taps[2][None, :] * up_value[2:]
    )
    hidden = (jax.nn.silu(conv_g) * conv_v).astype(jnp.bfloat16)
    ffn_rows = product_rows(hidden, whole_down, 3)
    return (stream_wide + ffn_rows).astype(jnp.bfloat16)


def solution(mesh):
    in_specs = (
        P(("sp", "tp"), None),
        P("sp", "tp"),
        P("sp", "tp"),
        P("sp", "tp"),
        P("sp", "tp"),
        P("sp", "tp"),
        P("sp", "tp"),
        P("sp", "tp"),
        P("tp", None),
        P("tp", None),
        P(),
        P("sp", "tp"),
        P("sp", "tp"),
        P(None, "tp"),
        P(None, "tp"),
        P("tp", "sp"),
    )
    out_specs = P(("sp", "tp"), None)
    return jax.shard_map(local, mesh=mesh, in_specs=in_specs, out_specs=out_specs, check_vma=False)
```

```python
import functools

import jax
import jax.numpy as jnp
from jax import lax
from jax.experimental import pallas as pl
from jax.experimental.pallas import tpu as pltpu
from jax.sharding import PartitionSpec as P

BLOCK = 128


eps = 1e-06
neg_large = -1e30


def shifted(x, axis, by):
    count = lax.axis_size(axis)
    pairs = [(i, i + by) for i in range(count) if 0 <= i + by < count]
    return lax.ppermute(x, axis, pairs)


def gate_log_values(input_gate_logits, forget_gate_logits, forget_decay_offset):
    input_log_value = 15.0 * jnp.tanh(input_gate_logits / 15.0)
    forget_log_sigmoid = (
        jax.nn.log_sigmoid(15.0 * jnp.tanh(forget_gate_logits / 15.0)) + forget_decay_offset
    )
    return (input_log_value, forget_log_sigmoid)


STATE_PAD = 16
MESH = pl.DeviceIdType.MESH


def cell_kernel(
    count,
    heads,
    state_ref,
    q_ref,
    k_ref,
    v_ref,
    gate_ref,
    gain_ref,
    rows_ref,
    cols_ref,
    out_ref,
    held,
    memory,
    normer,
    running,
    send_sem,
    recv_sem,
):
    me = lax.axis_index("sp")
    barrier = pltpu.get_barrier_semaphore()
    for d in range(1, count):
        pl.semaphore_signal(
            barrier, inc=1, device_id={"sp": lax.rem(me + d, count)}, device_id_type=MESH
        )
    pl.semaphore_wait(barrier, count - 1)

    def push(d, target, slot):
        return pltpu.make_async_remote_copy(
            src_ref=state_ref,
            dst_ref=held.at[slot],
            send_sem=send_sem.at[d],
            recv_sem=recv_sem.at[d],
            device_id={"sp": target},
            device_id_type=MESH,
        )

    for d in range(1, count):

        @pl.when(me + d < count)
        def _():
            push(d, me + d, me).start()

    memory[...] = jnp.zeros_like(memory)
    normer[...] = jnp.zeros_like(normer)
    running[...] = jnp.full(running.shape, neg_large, jnp.float32)
    for d in range(1, count):

        @pl.when(me - d >= 0)
        def _():
            push(d, lax.rem(me + d, count), me - d).wait_recv()

    key_width = memory.shape[1]
    value_width = memory.shape[2]
    span = key_width + STATE_PAD

    @pl.loop(0, me)
    def _(j):
        for h in range(heads):
            low = h * span
            extra = held[j, low + key_width : low + span, :].astype(jnp.float32)
            total = extra[2:3, :1] + extra[3:4, :1]
            level = extra[4:5, :1] + extra[5:6, :1]
            before = running[h, :1, :1]
            after = jnp.maximum(total + before, level)
            one = jnp.exp(total + before - after)
            two = jnp.exp(level - after)
            memory[h] = one * memory[h] + two * held[j, low : low + key_width, :].astype(
                jnp.float32
            )
            parts = extra[0:1, :key_width] + extra[1:2, :key_width]
            normer[h, :1, :] = one * normer[h, :1, :] + two * parts
            running[h] = jnp.broadcast_to(after, running.shape[1:])

    length = BLOCK
    scale = key_width ** (-0.5)
    at_row = lax.broadcasted_iota(jnp.int32, (length, length), 0)
    at_col = lax.broadcasted_iota(jnp.int32, (length, length), 1)
    causal = at_col <= at_row

    @pl.loop(0, q_ref.shape[0] // length)
    def _(j):
        rows = pl.ds(pl.multiple_of(j * length, length), length)
        lanes = rows_ref[j]
        cols = cols_ref[rows, :]
        for h in range(heads):
            keys = slice(h * key_width, (h + 1) * key_width)
            vals = slice(h * value_width, (h + 1) * value_width)
            q = q_ref[rows, keys]
            k = k_ref[rows, keys]
            v = v_ref[rows, vals]
            before = running[h, :1, :1]
            total = lanes[heads + h : heads + h + 1, :1]
            shifted_log = jnp.where(causal, lanes[h : h + 1, :], -jnp.inf)
            top = jnp.maximum(jnp.max(shifted_log, axis=1, keepdims=True), before)
            raw = (
                lax.dot_general(
                    q, k, (((1,), (1,)), ((), ())), preferred_element_type=jnp.float32
                )
                * scale
            )
            scores = raw * jnp.exp(shifted_log - top)
            carry = jnp.exp(before - top) * scale
            state = memory[h]
            high = state.astype(jnp.bfloat16)
            low = (state - high.astype(jnp.float32)).astype(jnp.bfloat16)
            carried = jnp.dot(q, high, preferred_element_type=jnp.float32) + jnp.dot(
                q, low, preferred_element_type=jnp.float32
            )
            numerator = carry * carried + jnp.dot(
                scores.astype(jnp.bfloat16), v, preferred_element_type=jnp.float32
            )
            denominator = carry * jnp.sum(
                q.astype(jnp.float32) * normer[h, :1, :], axis=1, keepdims=True
            ) + jnp.sum(scores, axis=1, keepdims=True)
            level = cols[:, h : h + 1] + top
            value = numerator / jnp.maximum(jnp.abs(denominator), jnp.exp(-level))
            mean = jnp.mean(value * value, axis=1, keepdims=True)
            normed = value * lax.rsqrt(mean + eps) * gain_ref[h : h + 1, :]
            gated = normed * jax.nn.sigmoid(gate_ref[rows, vals].astype(jnp.float32))
            out_ref[rows, vals] = gated.astype(out_ref.dtype)
            last = jnp.max(jnp.maximum(lanes[h : h + 1, :], before), axis=1, keepdims=True)
            decay = jnp.exp(before - last)
            weighted = k.astype(jnp.float32) * jnp.exp(cols[:, heads + h : heads + h + 1] - last)
            memory[h] = decay * state + lax.dot_general(
                weighted.astype(jnp.bfloat16),
                v,
                (((0,), (0,)), ((), ())),
                preferred_element_type=jnp.float32,
            )
            normer[h, :1, :] = decay * normer[h, :1, :] + jnp.sum(
                weighted, axis=0, keepdims=True
            )
            running[h] = jnp.broadcast_to(last + total, running.shape[1:])

    for d in range(1, count):

        @pl.when(me + d < count)
        def _():
            push(d, me + d, me).wait_send()


def halves(x):
    high = lax.reduce_precision(x, 8, 7)
    return (high.astype(jnp.bfloat16), (x - high).astype(jnp.bfloat16))


def cell_parts(q, k, v, input_log, forget_log):
    heads = input_log.shape[1]
    tokens = q.shape[0]
    key_width = q.shape[1] // heads
    value_width = v.shape[1] // heads
    count = lax.axis_size("sp")
    blocks = tokens // BLOCK
    f = forget_log.reshape(blocks, BLOCK, heads)
    tri = jnp.tril(jnp.ones((BLOCK, BLOCK), jnp.float32))
    within = jnp.einsum("ts,bsh->bth", tri, f, precision=lax.Precision.HIGHEST)
    each = within[:, -1, :]
    later = jnp.triu(jnp.ones((blocks, blocks), jnp.float32), 1)
    after = jnp.einsum("bc,ch->bh", later, each, precision=lax.Precision.HIGHEST)
    total = jnp.sum(each, axis=0)
    shifted_log = input_log.reshape(blocks, BLOCK, heads) - within
    to_end = (shifted_log + (each + after)[:, None, :]).reshape(tokens, heads)
    level = jnp.max(to_end, axis=0)
    weighted = k.reshape(tokens, heads, key_width).astype(jnp.float32) * jnp.exp(to_end - level)[
        :, :, None
    ]
    memory = jnp.einsum(
        "shd,shv->hdv",
        weighted.astype(jnp.bfloat16),
        v.reshape(tokens, heads, value_width),
        preferred_element_type=jnp.float32,
    ).astype(jnp.bfloat16)
    normer = jnp.sum(weighted, axis=0)
    wide = (heads, 1, value_width)
    lines = [
        jnp.pad(part, ((0, 0), (0, value_width - key_width)))[:, None, :]
        for part in halves(normer)
    ]
    for scalar in (total, level):
        lines += [jnp.broadcast_to(part[:, None, None], wide) for part in halves(scalar)]
    lines.append(jnp.zeros((heads, STATE_PAD - len(lines), value_width), jnp.bfloat16))
    span = key_width + STATE_PAD
    state = jnp.concatenate([memory] + lines, axis=1).reshape(heads * span, value_width)
    lanes = jnp.concatenate(
        [
            jnp.transpose(shifted_log, (0, 2, 1)),
            jnp.broadcast_to(each[:, :, None], (blocks, heads, BLOCK)),
        ],
        axis=1,
    )
    cols = jnp.concatenate([within, shifted_log], axis=2).reshape(tokens, 2 * heads)
    return state, lanes, cols


def cell(q, k, v, gates, input_log, forget_log, gain):
    heads = input_log.shape[1]
    key_width = q.shape[1] // heads
    value_width = v.shape[1] // heads
    count = lax.axis_size("sp")
    span = key_width + STATE_PAD
    state, lanes, cols = cell_parts(q, k, v, input_log, forget_log)
    vmem = pl.BlockSpec(memory_space=pltpu.VMEM)
    return pl.pallas_call(
        functools.partial(cell_kernel, count, heads),
        out_shape=jax.ShapeDtypeStruct(v.shape, jnp.bfloat16),
        in_specs=[vmem] * 8,
        out_specs=vmem,
        scratch_shapes=[
            pltpu.VMEM((count, heads * span, value_width), jnp.bfloat16),
            pltpu.VMEM((heads, key_width, value_width), jnp.float32),
            pltpu.VMEM((heads, 8, key_width), jnp.float32),
            pltpu.VMEM((heads, 8, 128), jnp.float32),
            pltpu.SemaphoreType.DMA((count,)),
            pltpu.SemaphoreType.DMA((count,)),
        ],
        compiler_params=pltpu.CompilerParams(
            collective_id=0, has_side_effects=True, vmem_limit_bytes=40 * 1024 * 1024
        ),
        cost_estimate=pl.CostEstimate(
            flops=30_000_000_000, bytes_accessed=8 * v.size, transcendentals=0
        ),
    )(state, q, k, v, gates, gain, lanes, cols)


def rows_kernel(pieces, x_ref, out_ref, own_sem, near_send, near_recv, far_send, far_recv, on_send, on_recv):
    me = lax.axis_index("tp")
    near = me + 1 - 2 * lax.rem(me, 2)
    far = lax.rem(me + 2, 4)
    opposite = lax.rem(near + 2, 4)
    size = x_ref.shape[0]
    step = size // pieces
    barrier = pltpu.get_barrier_semaphore()
    for other in (near, far):
        pl.semaphore_signal(barrier, inc=1, device_id={"tp": other}, device_id_type=MESH)
    pl.semaphore_wait(barrier, 2)

    def at(owner, p):
        return out_ref.at[pl.ds(pl.multiple_of(owner * size + p * step, step), step)]

    def send(src, dst, sems, p, target):
        return pltpu.make_async_remote_copy(
            src_ref=src,
            dst_ref=dst,
            send_sem=sems[0].at[p],
            recv_sem=sems[1].at[p],
            device_id={"tp": target},
            device_id_type=MESH,
        )

    mine = [x_ref.at[pl.ds(p * step, step)] for p in range(pieces)]
    far_out = [send(mine[p], at(me, p), (far_send, far_recv), p, far) for p in range(pieces)]
    near_out = [send(mine[p], at(me, p), (near_send, near_recv), p, near) for p in range(pieces)]
    far_in = [send(mine[p], at(far, p), (far_send, far_recv), p, far) for p in range(pieces)]
    near_in = [send(mine[p], at(near, p), (near_send, near_recv), p, near) for p in range(pieces)]
    onward = [send(at(far, p), at(far, p), (on_send, on_recv), p, near) for p in range(pieces)]
    on_in = [
        send(at(opposite, p), at(opposite, p), (on_send, on_recv), p, near)
        for p in range(pieces)
    ]
    for p in range(pieces):
        far_out[p].start()
    for p in range(pieces):
        near_out[p].start()
    whole = pl.ds(pl.multiple_of(me * size, size), size)
    own = pltpu.make_async_copy(x_ref, out_ref.at[whole], own_sem)
    own.start()
    for p in range(pieces):
        far_in[p].wait_recv()
        onward[p].start()
    own.wait()
    for p in range(pieces):
        near_in[p].wait_recv()
        on_in[p].wait_recv()
    for p in range(pieces):
        far_out[p].wait_send()
        near_out[p].wait_send()
        onward[p].wait_send()


def gather_rows(x):
    if lax.axis_size("tp") != 4:
        return lax.all_gather(x, "tp", axis=0, tiled=True)
    pieces = 4
    vmem = pl.BlockSpec(memory_space=pltpu.VMEM)
    return pl.pallas_call(
        functools.partial(rows_kernel, pieces),
        out_shape=jax.ShapeDtypeStruct((4 * x.shape[0], x.shape[1]), x.dtype),
        in_specs=[vmem],
        out_specs=vmem,
        scratch_shapes=[pltpu.SemaphoreType.DMA] + [pltpu.SemaphoreType.DMA((pieces,))] * 6,
        compiler_params=pltpu.CompilerParams(
            collective_id=1, has_side_effects=True, vmem_limit_bytes=16 * 1024 * 1024
        ),
        cost_estimate=pl.CostEstimate(
            flops=30_000_000_000, bytes_accessed=4 * x.size, transcendentals=0
        ),
    )(x)


def product_kernel(
    pieces,
    x_ref,
    w_ref,
    out_ref,
    pair_out,
    pair_in,
    far_out,
    far_in,
    near_out,
    near_in,
    pair_send,
    pair_recv,
    far_send,
    far_recv,
    near_send,
    near_recv,
):
    me = lax.axis_index("tp")
    near = me + 1 - 2 * lax.rem(me, 2)
    far = lax.rem(me + 2, 4)
    opposite = lax.rem(near + 2, 4)
    size = out_ref.shape[0]
    step = out_ref.shape[1] // pieces
    barrier = pltpu.get_barrier_semaphore()
    for other in (near, far):
        pl.semaphore_signal(barrier, inc=1, device_id={"tp": other}, device_id_type=MESH)
    pl.semaphore_wait(barrier, 2)

    def columns(p):
        return pl.ds(pl.multiple_of(p * step, step), step)

    def term(owner, p):
        rows = pl.ds(pl.multiple_of(owner * size, size), size)
        return jnp.dot(x_ref[rows, :], w_ref[:, columns(p)], preferred_element_type=jnp.float32)

    def send(src, dst, sems, p, target):
        return pltpu.make_async_remote_copy(
            src_ref=src.at[p],
            dst_ref=dst.at[p],
            send_sem=sems[0].at[p],
            recv_sem=sems[1].at[p],
            device_id={"tp": target},
            device_id_type=MESH,
        )

    def pair(p):
        return send(pair_out, pair_in, (pair_send, pair_recv), p, near)

    def across(p):
        return send(far_out, far_in, (far_send, far_recv), p, far)

    def beside(p):
        return send(near_out, near_in, (near_send, near_recv), p, near)

    @pl.loop(0, pieces)
    def _(p):
        pair_out[p] = term(opposite, p).astype(jnp.bfloat16)
        pair(p).start()
        mine = term(far, p)
        pair(p).wait_recv()
        far_out[p] = (mine + pair_in[p].astype(jnp.float32)).astype(jnp.bfloat16)
        across(p).start()

    @pl.loop(0, pieces)
    def _(p):
        near_out[p] = term(near, p).astype(jnp.bfloat16)
        beside(p).start()

    @pl.loop(0, pieces)
    def _(p):
        own = term(me, p)
        beside(p).wait_recv()
        out_ref[:, columns(p)] = own + near_in[p].astype(jnp.float32)

    @pl.loop(0, pieces)
    def _(p):
        across(p).wait_recv()
        out_ref[:, columns(p)] += far_in[p].astype(jnp.float32)

    @pl.loop(0, pieces)
    def _(p):
        pair(p).wait_send()
        across(p).wait_send()
        beside(p).wait_send()


def product_rows(x, w, tag):
    if lax.axis_size("tp") != 4:
        partial = jnp.dot(x, w, preferred_element_type=jnp.float32).astype(jnp.bfloat16)
        return lax.psum_scatter(partial, "tp", scatter_dimension=0, tiled=True).astype(
            jnp.float32
        )
    pieces = 4
    rows, wide = x.shape[0] // 4, w.shape[1]
    vmem = pl.BlockSpec(memory_space=pltpu.VMEM)
    slots = pltpu.VMEM((pieces, rows, wide // pieces), jnp.bfloat16)
    return pl.pallas_call(
        functools.partial(product_kernel, pieces),
        out_shape=jax.ShapeDtypeStruct((rows, wide), jnp.float32),
        in_specs=[vmem] * 2,
        out_specs=vmem,
        scratch_shapes=[slots] * 6 + [pltpu.SemaphoreType.DMA((pieces,))] * 6,
        compiler_params=pltpu.CompilerParams(
            collective_id=tag, has_side_effects=True, vmem_limit_bytes=40 * 1024 * 1024
        ),
        cost_estimate=pl.CostEstimate(
            flops=30_000_000_000, bytes_accessed=2 * w.size, transcendentals=0
        ),
    )(x, w)


def walk_kernel(count, pieces, x_ref, out_ref, own_sem, send_sem, recv_sem):
    me = lax.axis_index("sp")
    odd = lax.rem(me, 2)
    place = me // 2 + odd * (count - 1 - 2 * (me // 2))
    size = x_ref.shape[0]
    step = size // (2 * pieces)

    def index(position):
        position = lax.rem(position + 2 * count, count)
        back = position // (count // 2)
        return (1 - back) * 2 * position + back * (2 * (count - 1 - position) + 1)

    ways = (1, -1)
    barrier = pltpu.get_barrier_semaphore()
    for way in ways:
        pl.semaphore_signal(
            barrier, inc=1, device_id={"sp": index(place + way)}, device_id_type=MESH
        )
    pl.semaphore_wait(barrier, 2)

    def hop(w, t, p, age, own=False):
        inner = (w * pieces + p) * step
        owner = index(place - ways[w] * age)
        dst = out_ref.at[pl.ds(pl.multiple_of(owner * size + inner, step), step)]
        return pltpu.make_async_remote_copy(
            src_ref=x_ref.at[pl.ds(inner, step)] if own else dst,
            dst_ref=dst,
            send_sem=send_sem.at[w, p, t],
            recv_sem=recv_sem.at[w, p, t],
            device_id={"sp": index(place + ways[w])},
            device_id_type=MESH,
        )

    for p in range(pieces):
        for w in range(2):
            hop(w, 0, p, 0, True).start()
    whole = pl.ds(pl.multiple_of(me * size, size), size)
    own = pltpu.make_async_copy(x_ref, out_ref.at[whole], own_sem)
    own.start()

    @pl.loop(1, count - 1)
    def _(t):
        for p in range(pieces):
            for w in range(2):
                hop(w, t - 1, p, t).wait_recv()
                hop(w, t, p, t).start()

    own.wait()
    for p in range(pieces):
        for w in range(2):
            hop(w, count - 2, p, count - 1).wait_recv()
            hop(w, 0, p, 0, True).wait_send()

    @pl.loop(1, count - 1)
    def _(t):
        for p in range(pieces):
            for w in range(2):
                hop(w, t, p, t).wait_send()


def walk_gather(x, pieces):
    count = lax.axis_size("sp")
    if count % 2 or count < 4 or x.shape[0] % (32 * pieces):
        return lax.all_gather(x, "sp", axis=0, tiled=True)
    vmem = pl.BlockSpec(memory_space=pltpu.VMEM)
    return pl.pallas_call(
        functools.partial(walk_kernel, count, pieces),
        out_shape=jax.ShapeDtypeStruct((count * x.shape[0], x.shape[1]), x.dtype),
        in_specs=[vmem],
        out_specs=vmem,
        scratch_shapes=[pltpu.SemaphoreType.DMA]
        + [pltpu.SemaphoreType.DMA((2, pieces, count - 1))] * 2,
        compiler_params=pltpu.CompilerParams(
            collective_id=4, has_side_effects=True, vmem_limit_bytes=16 * 1024 * 1024
        ),
        cost_estimate=pl.CostEstimate(
            flops=30_000_000_000, bytes_accessed=count * x.size, transcendentals=0
        ),
    )(x)


def layer_kernel(
    count,
    heads,
    up_pieces,
    down_pieces,
    input_logs_ref,
    forget_logs_ref,
    gain_ref,
    norm_gain_ref,
    gate_taps_ref,
    value_taps_ref,
    q_hbm,
    k_hbm,
    v_hbm,
    gate_hbm,
    residual_hbm,
    wo_ref,
    gate_w_ref,
    value_w_ref,
    down_w_ref,
    out_ref,
    q_ref,
    k_ref,
    v_ref,
    gate_ref,
    residual_ref,
    rows_ref,
    cols_ref,
    state_ref,
    held,
    memory,
    normer,
    running,
    pair_memory,
    pair_normer,
    pair_level,
    handed,
    gated,
    mine,
    wo_full,
    middle,
    give_up,
    give_down,
    full_up,
    full_down,
    total_rows,
    stream,
    group,
    up_tile,
    up_other,
    hidden,
    pair_out,
    pair_in,
    second_out,
    second_in,
    third_out,
    third_in,
    kept,
    blocks_of,
    load_sem,
    wo_sem,
    give_sem,
    state_send,
    state_recv,
    up_send,
    up_recv,
    down_send,
    down_recv,
    block_send,
    block_recv,
    rows_send,
    rows_recv,
    sum_send,
    sum_recv,
    edge_sem,
    out_sem,
):
    me = lax.axis_index("sp")
    tp = lax.axis_index("tp")
    core = lax.rem(tp, 2)
    chip = tp // 2
    near = tp + 1 - 2 * core
    far = lax.rem(tp + 2, 4)
    opposite = lax.rem(near + 2, 4)
    odd = lax.rem(me, 2)
    partner = me + 1 - 2 * odd
    line = count // 2
    place = me // 2
    model = full_up.shape[0]
    lane = 128
    up_rows = model // count
    up_step = 2 * up_rows // up_pieces
    half_width = full_down.shape[1]
    tiles = half_width // lane
    rest = half_width - tiles * lane
    wide = full_down.shape[2]
    down_step = 2 * half_width // down_pieces

    barrier = pltpu.get_barrier_semaphore()
    for other in (near, far, opposite):
        pl.semaphore_signal(barrier, inc=1, device_id={"tp": other}, device_id_type=MESH)
    for other in (partner, lax.rem(me + 2, count), lax.rem(me + count - 2, count)):
        pl.semaphore_signal(barrier, inc=1, device_id={"sp": other}, device_id_type=MESH)

    own_up = pl.ds(pl.multiple_of(me * up_rows, up_rows), up_rows)
    wo_rows = wo_ref.shape[0]
    wo_own = pl.ds(pl.multiple_of(tp * wo_rows, wo_rows), wo_rows)
    loads = []

    def load(src, dst):
        loads.append(pltpu.make_async_copy(src, dst, load_sem.at[len(loads)]))

    shift = tiles * lane + 2 * rest
    for i in range(tiles):
        for a, w_ref in enumerate((gate_w_ref, value_w_ref)):
            lanes = pl.ds((2 * i + a) * lane, lane)
            for to, y in ((full_up.at[own_up, lanes], odd), (give_up.at[:, lanes], 1 - odd)):
                at = pl.multiple_of(y * shift + i * lane, lane)
                load(w_ref.at[:, pl.ds(at, lane)], to)
    for a, w_ref in enumerate((gate_w_ref, value_w_ref)):
        load(w_ref.at[:, pl.ds(tiles * lane, lane)], middle.at[a])
    first_loads = len(loads)
    load(k_hbm, k_ref)
    load(v_hbm, v_ref)
    load(wo_ref, wo_full.at[wo_own])
    soon_loads = len(loads)
    for to, y in ((full_down.at[me], odd), (give_down, 1 - odd)):
        at = pl.multiple_of(y * shift, rest)
        load(down_w_ref.at[pl.ds(at, tiles * lane)], to.at[pl.ds(0, tiles * lane)])
        at = pl.multiple_of(tiles * lane + y * rest, rest)
        load(down_w_ref.at[pl.ds(at, rest)], to.at[pl.ds(tiles * lane, rest)])
    load(q_hbm, q_ref)
    load(gate_hbm, gate_ref)
    load(residual_hbm, residual_ref)
    for one in loads[:first_loads]:
        one.start()
    for one in loads[first_loads:]:
        one.start()
    for one in loads[:first_loads]:
        one.wait()

    def remote(src, dst, send_sem, recv_sem, **to):
        return pltpu.make_async_remote_copy(
            src_ref=src,
            dst_ref=dst,
            send_sem=send_sem,
            recv_sem=recv_sem,
            device_id=to,
            device_id_type=MESH,
        )

    at_lane = lax.broadcasted_iota(jnp.int32, (up_rows, lane), 1)
    first_half = at_lane < rest

    def halves_of(g, v, low):
        a = jnp.where(low, g, pltpu.roll(v, rest, 1))
        b = jnp.where(low, pltpu.roll(g, rest, 1), v)
        return a, b

    mid_a, mid_b = halves_of(
        middle[0].astype(jnp.float32), middle[1].astype(jnp.float32), first_half
    )
    tail = slice(2 * tiles * lane, 2 * tiles * lane + lane)
    full_up[own_up, tail] = jnp.where(odd == 0, mid_a, mid_b).astype(jnp.bfloat16)
    give_up[:, tail] = jnp.where(odd == 0, mid_b, mid_a).astype(jnp.bfloat16)

    give_step = up_rows // 2

    def give_rows(p):
        at = pl.multiple_of(me * up_rows + p * give_step, give_step)
        return remote(
            give_up.at[pl.ds(p * give_step, give_step)],
            full_up.at[pl.ds(at, give_step)],
            give_sem.at[0, p],
            give_sem.at[1, p],
            sp=partner,
        )

    give_cols = remote(give_down, full_down.at[me], give_sem.at[0, 2], give_sem.at[1, 2], sp=partner)
    wo_pieces = wo_sem.shape[2]
    wo_step = wo_rows // 2 // wo_pieces

    def wo_copy(kind, owner, y, s, **to):
        at = pl.multiple_of(owner * wo_rows + (y * wo_pieces + s) * wo_step, wo_step)
        part = wo_full.at[pl.ds(at, wo_step)]
        return remote(part, part, wo_sem.at[0, kind, s], wo_sem.at[1, kind, s], **to)

    def wo_shard(owner):
        part = wo_full.at[pl.ds(pl.multiple_of(owner * wo_rows, wo_rows), wo_rows)]
        return remote(part, part, wo_sem.at[0, 0, 0], wo_sem.at[1, 0, 0], tp=near)

    def wo_onward(s):
        wo_copy(1, far, odd, s, tp=far).wait_recv()
        wo_copy(2, far, odd, s, sp=partner).start()
        wo_copy(3, far, odd, s, tp=near).start()

    def source(w, t):
        return place - t if w == 0 else place + t

    def has(w, t):
        return place >= t if w == 0 else place + t < line

    def sends(w, t):
        onward = place + 1 < line if w == 0 else place > 0
        return has(w, t) & onward & (t < line - 1)

    def beyond(w):
        return lax.rem(me + 2, count) if w == 0 else lax.rem(me + count - 2, count)

    def up_hop(w, t, m):
        at = source(w, t) * 2 * up_rows + lax.rem(m + odd * (up_pieces // 2), up_pieces) * up_step
        part = full_up.at[pl.ds(pl.multiple_of(at, up_step), up_step)]
        return remote(part, part, up_send.at[w, t, m], up_recv.at[w, t, m], sp=beyond(w))

    def down_hop(w, t, m):
        each = down_pieces // 2
        owner = source(w, t) * 2 + m // each
        at = lax.rem(m, each) * down_step
        part = full_down.at[owner, pl.ds(pl.multiple_of(at, down_step), down_step)]
        return remote(part, part, down_send.at[w, t, m], down_recv.at[w, t, m], sp=beyond(w))

    up_ticks = line * up_pieces
    all_ticks = up_ticks + line * down_pieces

    at_end = (place == 0) | (place == line - 1)

    def move(hop, pieces, n):
        t = n // pieces
        m = lax.rem(n, pieces)
        for w in range(2):
            due = sends(w, t)
            if hop is down_hop:
                due = due & ((t > 0) | jnp.logical_not(at_end))

            @pl.when(has(w, t) & (t > 0))
            def _():
                hop(w, t - 1, m).wait_recv()

            @pl.when(due)
            def _():
                hop(w, t, m).start()

    def up_tick(n):
        for p in range(2):

            @pl.when(n == up_pieces // 2 + p * (up_pieces // 4))
            def _():
                give_rows(p).wait_recv()

        move(up_hop, up_pieces, n)

    def down_tick(n):
        @pl.when((n == 0) & jnp.logical_not(at_end))
        def _():
            give_cols.wait_recv()

        move(down_hop, down_pieces, n)

    def late_tick(n):
        @pl.when((n >= up_ticks) & (n < all_ticks))
        def _():
            down_tick(n - up_ticks)

    def tick(n):
        @pl.when((n < up_pieces) | jnp.logical_not(at_end))
        def _():
            @pl.when(n < up_ticks)
            def _():
                up_tick(n)

            late_tick(n)

    def up_sent(n):
        t = n // up_pieces
        for w in range(2):

            @pl.when(sends(w, t))
            def _():
                up_hop(w, t, lax.rem(n, up_pieces)).wait_send()

    pl.semaphore_wait(barrier, 6)
    for n in range(2):
        up_tick(n)
    give_rows(0).start()
    for one in loads[first_loads:soon_loads]:
        one.wait()
    for s in range(wo_pieces):
        wo_copy(1, tp, odd, s, tp=far).start()
    wo_shard(tp).start()

    key_width = memory.shape[1]
    value_width = memory.shape[2]
    span = key_width + STATE_PAD
    swap = remote(state_ref, held.at[0], state_send.at[0], state_recv.at[0], sp=partner)
    hand = remote(handed, held.at[1], state_send.at[1], state_recv.at[1], sp=beyond(0))

    def read_state(ref, h):
        low = h * span
        extra = ref[low + key_width : low + span, :].astype(jnp.float32)
        total = extra[2:3, :1] + extra[3:4, :1]
        level = extra[4:5, :1] + extra[5:6, :1]
        parts = extra[0:1, :key_width] + extra[1:2, :key_width]
        return ref[low : low + key_width, :].astype(jnp.float32), parts, level, total

    def join(first, second, total):
        mem_a, norm_a, level_a = first
        mem_b, norm_b, level_b = second
        after = jnp.maximum(total + level_a, level_b)
        one = jnp.exp(total + level_a - after)
        two = jnp.exp(level_b - after)
        return one * mem_a + two * mem_b, one * norm_a + two * norm_b, after

    def keep(refs, h, values):
        mem, norm, level = values
        refs[0][h] = mem
        refs[1][h, :1, :] = norm
        refs[2][h] = jnp.broadcast_to(level, refs[2].shape[1:])

    carried_refs = (memory, normer, running)

    def write_state(ref, h, mem, norm, level, total):
        low = h * span
        ref[low : low + key_width, :] = mem.astype(jnp.bfloat16)
        lines = jnp.zeros((STATE_PAD, value_width), jnp.float32)
        at_line = lax.broadcasted_iota(jnp.int32, lines.shape, 0)
        norm = jnp.concatenate([norm] * (value_width // key_width), axis=1)
        for i, part in enumerate((norm, total, level)):
            high = part.astype(jnp.bfloat16).astype(jnp.float32)
            lines = jnp.where(at_line == 2 * i, high, lines)
            lines = jnp.where(at_line == 2 * i + 1, part - high, lines)
        ref[low + key_width : low + span, :] = lines.astype(jnp.bfloat16)

    length = BLOCK
    blocks = q_ref.shape[0] // length
    at_row = lax.broadcasted_iota(jnp.int32, (length, length), 0)
    at_col = lax.broadcasted_iota(jnp.int32, (length, length), 1)

    def by_block(ref):
        return jnp.concatenate(
            [
                ref[:, b * length : (b + 1) * length]
                for b in range(blocks)
            ],
            axis=0,
        )

    within = jnp.dot(
        by_block(forget_logs_ref),
        jnp.where(at_row <= at_col, 1.0, 0.0),
        precision=lax.Precision.HIGHEST,
        preferred_element_type=jnp.float32,
    )
    shifted_all = by_block(input_logs_ref) - within
    each_all = within[:, length - 1 : length]
    after = jnp.zeros((heads, 1), jnp.float32)
    to_end = [None] * blocks
    for b in reversed(range(blocks)):
        part = slice(b * heads, (b + 1) * heads)
        after = after + each_all[part]
        to_end[b] = shifted_all[part] + after
    own_total = after
    own_level = functools.reduce(jnp.maximum, to_end)
    own_level = jnp.max(own_level, axis=1, keepdims=True)
    for b in range(blocks):
        part = slice(b * heads, (b + 1) * heads)
        rows_ref[b, 0 : 2 * heads, :] = jnp.concatenate(
            [shifted_all[part], jnp.broadcast_to(each_all[part], (heads, length))], axis=0
        )
        lines = [within[part], shifted_all[part], jnp.exp(to_end[b] - own_level)]
        lines.append(jnp.zeros((length - 3 * heads, length), jnp.float32))
        cols_ref[b * length : (b + 1) * length, :] = jnp.transpose(
            jnp.concatenate(lines, axis=0)
        )

    memory[...] = jnp.zeros_like(memory)
    normer[...] = jnp.zeros_like(normer)

    @pl.loop(0, blocks)
    def _(j):
        rows = pl.ds(pl.multiple_of(j * length, length), length)
        cols = cols_ref[rows, :]
        for h in range(heads):
            k = k_ref[rows, h * key_width : (h + 1) * key_width]
            v = v_ref[rows, h * value_width : (h + 1) * value_width]
            weighted = k.astype(jnp.float32) * cols[:, 2 * heads + h : 2 * heads + h + 1]
            memory[h] += lax.dot_general(
                weighted.astype(jnp.bfloat16),
                v,
                (((0,), (0,)), ((), ())),
                preferred_element_type=jnp.float32,
            )
            normer[h, :1, :] += jnp.sum(weighted, axis=0, keepdims=True)

    for h in range(heads):
        write_state(
            state_ref,
            h,
            memory[h],
            normer[h, :1, :],
            own_level[h : h + 1, :],
            own_total[h : h + 1, :],
        )
    swap.start()
    give_rows(1).start()
    for one in loads[soon_loads:]:
        one.wait()
    swap.wait_recv()
    for s in range(wo_pieces // 2):
        wo_onward(s)

    @pl.when(odd == 0)
    def _():
        for h in range(heads):
            mem_a, norm_a, level_a, total_a = read_state(state_ref, h)
            mem_b, norm_b, level_b, total_b = read_state(held.at[0], h)
            out = join((mem_a, norm_a, level_a), (mem_b, norm_b, level_b), total_b)
            keep((pair_memory, pair_normer, pair_level.at[0]), h, out)
            pair_level[1, h] = jnp.broadcast_to(total_a + total_b, pair_level.shape[2:])

    @pl.when(odd == 1)
    def _():
        for h in range(heads):
            mem_a, norm_a, level_a, total_a = read_state(held.at[0], h)
            mem_b, norm_b, level_b, total_b = read_state(state_ref, h)
            out = join((mem_a, norm_a, level_a), (mem_b, norm_b, level_b), total_b)
            keep((pair_memory, pair_normer, pair_level.at[0]), h, out)
            pair_level[1, h] = jnp.broadcast_to(total_a + total_b, pair_level.shape[2:])

    started = jnp.minimum(FIRST_TICKS + NEXT_TICKS * place, jnp.where(at_end, up_pieces, up_ticks))

    @pl.loop(2, started)
    def _(n):
        up_sent(n - 2)
        up_tick(n)

    memory[...] = jnp.zeros_like(memory)
    normer[...] = jnp.zeros_like(normer)
    running[...] = jnp.full(running.shape, neg_large, jnp.float32)

    @pl.when(place > 0)
    def _():
        hand.wait_recv()
        for h in range(heads):
            mem, parts, level, total = read_state(held.at[1], h)
            keep(carried_refs, h, (mem, parts, level))

    @pl.when(place + 1 < line)
    def _():
        for h in range(heads):
            mem, norm, level = join(
                (memory[h], normer[h, :1, :], running[h, :1, :1]),
                (pair_memory[h], pair_normer[h, :1, :], pair_level[0, h, :1, :1]),
                pair_level[1, h, :1, :1],
            )
            write_state(handed, h, mem, norm, level, jnp.zeros_like(level))
        hand.start()

    @pl.when(odd == 1)
    def _():
        for h in range(heads):
            mem, norm, level, total = read_state(held.at[0], h)
            out = join(
                (memory[h], normer[h, :1, :], running[h, :1, :1]), (mem, norm, level), total
            )
            keep(carried_refs, h, out)

    scale = key_width ** (-0.5)
    causal = at_col <= at_row
    size = residual_ref.shape[0]
    per = size // length

    def block_copy(j, sender):
        at = pl.multiple_of(lax.rem(j, per) * length, length)
        width = gated.shape[1]
        return remote(
            gated.at[pl.ds(pl.multiple_of(j * length, length), length)],
            mine.at[sender, pl.ds(at, length)],
            block_send.at[j],
            block_recv.at[sender, lax.rem(j, per)],
            tp=j // per,
        )

    @pl.loop(0, blocks)
    def _(j):
        tick(started + j)

        @pl.when(j < wo_pieces // 2)
        def _():
            wo_onward(wo_pieces // 2 + j)

        @pl.when(j == wo_pieces // 2)
        def _():
            give_cols.start()

        @pl.when(j >= blocks - wo_pieces)
        def _():
            s = j - (blocks - wo_pieces)
            wo_copy(2, far, 1 - odd, s, sp=partner).wait_recv()
            wo_copy(4, far, 1 - odd, s, tp=near).start()

        rows = pl.ds(pl.multiple_of(j * length, length), length)
        lanes = rows_ref[j]
        cols = cols_ref[rows, :]
        for h in range(heads):
            keys = slice(h * key_width, (h + 1) * key_width)
            vals = slice(h * value_width, (h + 1) * value_width)
            q = q_ref[rows, keys]
            k = k_ref[rows, keys]
            v = v_ref[rows, vals]
            before = running[h, :1, :1]
            total = lanes[heads + h : heads + h + 1, :1]
            shifted_log = jnp.where(causal, lanes[h : h + 1, :], -jnp.inf)
            top = jnp.maximum(jnp.max(shifted_log, axis=1, keepdims=True), before)
            raw = (
                lax.dot_general(
                    q, k, (((1,), (1,)), ((), ())), preferred_element_type=jnp.float32
                )
                * scale
            )
            scores = raw * jnp.exp(shifted_log - top)
            carry = jnp.exp(before - top) * scale
            state = memory[h]
            high = state.astype(jnp.bfloat16)
            low = (state - high.astype(jnp.float32)).astype(jnp.bfloat16)
            carried = jnp.dot(q, high, preferred_element_type=jnp.float32) + jnp.dot(
                q, low, preferred_element_type=jnp.float32
            )
            numerator = carry * carried + jnp.dot(
                scores.astype(jnp.bfloat16), v, preferred_element_type=jnp.float32
            )
            denominator = carry * jnp.sum(
                q.astype(jnp.float32) * normer[h, :1, :], axis=1, keepdims=True
            ) + jnp.sum(scores, axis=1, keepdims=True)
            level = cols[:, h : h + 1] + top
            value = numerator / jnp.maximum(jnp.abs(denominator), jnp.exp(-level))
            mean = jnp.mean(value * value, axis=1, keepdims=True)
            normed = value * lax.rsqrt(mean + eps) * gain_ref[h : h + 1, :]
            gate = normed * jax.nn.sigmoid(gate_ref[rows, vals].astype(jnp.float32))
            gated[rows, vals] = gate.astype(gated.dtype)
            last = jnp.max(jnp.maximum(lanes[h : h + 1, :], before), axis=1, keepdims=True)
            decay = jnp.exp(before - last)
            weighted = k.astype(jnp.float32) * jnp.exp(cols[:, heads + h : heads + h + 1] - last)
            memory[h] = decay * state + lax.dot_general(
                weighted.astype(jnp.bfloat16),
                v,
                (((0,), (0,)), ((), ())),
                preferred_element_type=jnp.float32,
            )
            normer[h, :1, :] = decay * normer[h, :1, :] + jnp.sum(
                weighted, axis=0, keepdims=True
            )
            running[h] = jnp.broadcast_to(last + total, running.shape[1:])

        @pl.when(j // per == tp)
        def _():
            at = pl.multiple_of(lax.rem(j, per) * length, length)
            mine[tp, pl.ds(at, length), :] = gated[rows, :]

        @pl.when(j // per != tp)
        def _():
            block_copy(j, tp).start()

    reached = started + blocks
    wo_shard(near).wait_recv()
    for s in range(wo_pieces):
        wo_copy(3, opposite, odd, s, tp=near).wait_recv()
        wo_copy(4, opposite, 1 - odd, s, tp=near).wait_recv()

    @pl.loop(0, 4)
    def _(s):
        tick(reached + s)

        @pl.when(s != tp)
        def _():
            for p in range(per):
                block_copy(tp * per + p, s).wait_recv()

    reached = reached + 4

    @pl.when(at_end)
    def _():
        give_cols.wait_recv()
        for w in range(2):

            @pl.when(sends(w, 0))
            def _():
                for m in range(down_pieces):
                    down_hop(w, 0, m).start()

    def columns(i):
        return pl.ds(pl.multiple_of(i * wide, wide), wide)

    @pl.loop(0, model // wide)
    def _(i):
        total = jnp.zeros((size, wide), jnp.float32)
        for s in range(4):
            total += jnp.dot(
                mine[s],
                wo_full[s * wo_rows : (s + 1) * wo_rows, columns(i)],
                preferred_element_type=jnp.float32,
            )
        total_rows[:, columns(i)] = total

    pad = PAD_ROWS
    tokens = 8 * size
    row_pieces = rows_send.shape[1]
    row_step = size // row_pieces

    def row_copy(kind, y, owner, p, **to):
        at = pad + (y * 4 + owner) * size + p * row_step
        part = group.at[pl.ds(pl.multiple_of(at, pad), row_step)]
        return remote(part, part, rows_send.at[kind, p], rows_recv.at[kind, p], **to)

    @pl.when(place == 0)
    def _():
        group[0:pad, :] = jnp.zeros((pad, model), group.dtype)

    @pl.loop(0, row_pieces)
    def _(p):
        rows = pl.ds(pl.multiple_of(p * row_step, row_step), row_step)
        rounded = (residual_ref[rows, :].astype(jnp.float32) + total_rows[rows, :]).astype(
            jnp.bfloat16
        )
        stream[rows, :] = rounded
        x = rounded.astype(jnp.float32)
        normed = x * lax.rsqrt(jnp.mean(x * x, axis=-1, keepdims=True) + eps) * norm_gain_ref[...]
        at = pl.multiple_of(pad + (odd * 4 + tp) * size + p * row_step, pad)
        group[pl.ds(at, row_step), :] = normed.astype(jnp.bfloat16)
        row_copy(0, odd, tp, p, tp=far).start()
        row_copy(2, odd, tp, p, sp=partner).start()
        row_copy(1, odd, tp, p, tp=near).start()

    @pl.loop(0, row_pieces)
    def _(p):
        tick(reached + 2 * p)
        row_copy(0, odd, far, p, tp=far).wait_recv()
        row_copy(3, odd, far, p, tp=near).start()

        @pl.when(lax.rem(p, 2) == 0)
        def _():
            row_copy(6, odd, far, p, sp=partner).start()

        tick(reached + 2 * p + 1)
        row_copy(2, 1 - odd, tp, p, sp=partner).wait_recv()
        row_copy(4, 1 - odd, tp, p, tp=near).start()

        @pl.when(lax.rem(p, 2) == 1)
        def _():
            row_copy(6, 1 - odd, tp, p, tp=far).start()

    reached = reached + 2 * row_pieces

    @pl.loop(0, row_pieces)
    def _(p):
        tick(reached + p)
        row_copy(6, 1 - odd, far, p, sp=partner).wait_recv()
        row_copy(5, 1 - odd, far, p, tp=near).start()
        row_copy(1, odd, near, p, tp=near).wait_recv()
        row_copy(3, odd, opposite, p, tp=near).wait_recv()
        row_copy(4, 1 - odd, near, p, tp=near).wait_recv()

    reached = reached + row_pieces

    @pl.loop(0, row_pieces)
    def _(p):
        row_copy(5, 1 - odd, opposite, p, tp=near).wait_recv()

    edge = remote(
        group.at[pl.ds(tokens, pad)],
        group.at[pl.ds(0, pad)],
        edge_sem.at[0],
        edge_sem.at[1],
        sp=beyond(0),
    )

    @pl.when(place + 1 < line)
    def _():
        edge.start()

    @pl.loop(jnp.where(at_end, up_pieces, jnp.minimum(reached, up_ticks)), up_ticks)
    def _(n):
        up_tick(n)

    reached = jnp.maximum(reached, up_ticks)
    early = up_ticks + jnp.where(at_end, 1, 2) * down_pieces
    parts = 4
    up_tiles = (up_tile, up_other)
    part_rows = tokens // parts

    def silu(a):
        return a * jax.nn.sigmoid(a)

    @pl.loop(0, parts)
    def _(b):
        part = lax.rem(b + 1, parts)
        at = pl.multiple_of(part * part_rows, part_rows)
        window = pl.ds(at, part_rows + pad)
        outs = pl.ds(at, part_rows)

        @pl.when((b == parts - 1) & (place > 0))
        def _():
            edge.wait_recv()

        for m in range(UPS_TICKS):
            n = reached + b * UPS_TICKS + m

            @pl.when(n < early)
            def _():
                tick(n)

        def conv(ref, taps, width):
            return (
                taps[0:1, :] * ref[pad - 2 : pad - 2 + part_rows, width]
                + taps[1:2, :] * ref[pad - 1 : pad - 1 + part_rows, width]
                + taps[2:3, :] * ref[pad : pad + part_rows, width]
            )

        def product(i):
            ref = up_tiles[i % 2]
            if i < tiles:
                ref[...] = jnp.dot(
                    group[window, :],
                    full_up[:, 2 * i * lane : 2 * (i + 1) * lane],
                    preferred_element_type=jnp.float32,
                )
            else:
                ref[:, 0:lane] = jnp.dot(
                    group[window, :], full_up[:, tail], preferred_element_type=jnp.float32
                )

        def finish(i):
            ref = up_tiles[i % 2]
            if i < tiles:
                taps_at = pl.ds(pl.multiple_of(odd * shift + i * lane, lane), lane)
                act = silu(conv(ref, gate_taps_ref[:, taps_at], slice(0, lane))) * conv(
                    ref, value_taps_ref[:, taps_at], slice(lane, 2 * lane)
                )
                hidden[outs, i * lane : (i + 1) * lane] = act.astype(jnp.bfloat16)
            else:
                mid = slice(tiles * lane, (tiles + 1) * lane)
                low = lax.broadcasted_iota(jnp.int32, (3, lane), 1) < rest
                taps_a, taps_b = halves_of(gate_taps_ref[:, mid], value_taps_ref[:, mid], low)
                both = conv(ref, jnp.where(odd == 0, taps_a, taps_b), slice(0, lane))
                act = silu(both) * pltpu.roll(both, rest, 1)
                hidden[outs, tiles * lane : tiles * lane + rest] = act[:, :rest].astype(
                    jnp.bfloat16
                )

        product(0)
        for i in range(tiles):
            product(i + 1)
            finish(i)
        finish(tiles)

    @pl.loop(jnp.minimum(reached + parts * UPS_TICKS, early), early)
    def _(n):
        tick(n)

    both_sides = jnp.minimum(place, line - 1 - place)

    def away(k):
        return jnp.where(k <= 2 * both_sides, (k + 1) // 2, k - both_sides)

    def unit(k):
        rising = jnp.where(place < line - 1 - place, 1, -1)
        way = jnp.where(k <= 2 * both_sides, 1 - 2 * lax.rem(k, 2), rising)
        return place + way * away(k)

    def sum_copy(kind, i):
        src, dst, to = (
            (pair_out.at[i], pair_in.at[i], {"tp": near}),
            (second_out.at[i, 0], second_in.at[i, 0], {"tp": far}),
            (second_out.at[i, 1], second_in.at[i, 1], {"sp": partner}),
            (third_out.at[i, 0], third_in.at[i, 0], {"sp": partner}),
            (third_out.at[i, 1], third_in.at[i, 1], {"tp": far}),
        )[kind]
        return remote(src, dst, sum_send.at[kind, i], sum_recv.at[kind, i], **to)

    part_wide = wide // 2
    cut = (slice(0, part_wide), slice(part_wide, wide))

    def term(i, a, b, side):
        y = lax.rem(odd + a, 2)
        x = lax.rem(chip + b, 2)
        owner = 2 * x + lax.rem(core + side, 2)
        rows = pl.ds(pl.multiple_of((y * 4 + owner) * size, size), size)
        return jnp.dot(hidden[rows, :], full_down[i], preferred_element_type=jnp.float32)

    def first_stage(i):
        for a in range(2):
            for b in range(2):
                pair_out[i, 2 * a + b] = term(i, a, b, 1).astype(jnp.bfloat16)
        sum_copy(0, i).start()
        for a in range(2):
            for b in range(2):
                blocks_of[2 * a + b] = term(i, a, b, 0)

    def second_stage(i):
        sum_copy(0, i).wait_recv()

        def block(a, b, side):
            at = 2 * a + b
            return blocks_of[at, :, cut[side]] + pair_in[i, at, :, cut[side]].astype(jnp.float32)

        for a in range(2):
            second_out[i, 0, a] = block(a, 1, 0).astype(jnp.bfloat16)
        sum_copy(1, i).start()
        for b in range(2):
            second_out[i, 1, b] = block(1, b, 1).astype(jnp.bfloat16)
        sum_copy(2, i).start()
        for a in range(2):
            kept[i, 0, a] = block(a, 0, 0)
        for b in range(2):
            kept[i, 1, b] = block(0, b, 1)

    def third_stage(i):
        for side in range(2):
            sum_copy(1 + side, i).wait_recv()
            third_out[i, side] = (
                kept[i, side, 1] + second_in[i, side, 1].astype(jnp.float32)
            ).astype(jnp.bfloat16)
            sum_copy(3 + side, i).start()
            kept[i, side, 0] += second_in[i, side, 0].astype(jnp.float32)

    def out_copy(i):
        return pltpu.make_async_copy(
            stream.at[:, columns(i)], out_ref.at[:, columns(i)], out_sem.at[i]
        )

    def last_stage(i):
        for side in range(2):
            sum_copy(3 + side, i).wait_recv()
            at = pl.multiple_of(i * wide + side * part_wide, part_wide)
            cols = pl.ds(at, part_wide)
            stream[:, cols] = (
                stream[:, cols].astype(jnp.float32)
                + (kept[i, side, 0] + third_in[i, side].astype(jnp.float32))
            ).astype(stream.dtype)
        out_copy(i).start()

    def slice_at(n):
        return 2 * unit(n // 2) + lax.rem(n, 2)

    def due(k, j):
        return up_ticks + down_pieces * away(k) + (j + 1) * (down_pieces // 2)

    def until(n):
        k = n // 2
        last = jnp.where(k > 0, due(jnp.maximum(k - 1, 0), 1), early)
        return jnp.maximum(jnp.maximum(due(k, lax.rem(n, 2)), last), early)

    @pl.loop(0, count)
    def _(n):
        @pl.when(n > 0)
        def _():
            @pl.loop(until(n - 1), until(n))
            def _(at):
                late_tick(at)

        first_stage(slice_at(n))

        @pl.when(n > 1)
        def _():
            third_stage(slice_at(n - 2))

        second_stage(slice_at(n))

        @pl.when(n > 3)
        def _():
            last_stage(slice_at(n - 4))

    third_stage(slice_at(count - 2))
    last_stage(slice_at(count - 4))
    last_stage(slice_at(count - 3))
    third_stage(slice_at(count - 1))
    last_stage(slice_at(count - 2))
    last_stage(slice_at(count - 1))

    @pl.loop(0, count)
    def _(n):
        out_copy(n).wait()

    swap.wait_send()

    @pl.when(place + 1 < line)
    def _():
        hand.wait_send()
        edge.wait_send()

    for p in range(2):
        give_rows(p).wait_send()
    wo_shard(tp).wait_send()
    for s in range(wo_pieces):
        for kind in range(1, 5):
            wo_copy(kind, tp, 0, s, tp=near).wait_send()
    give_cols.wait_send()

    @pl.loop(0, blocks)
    def _(j):
        @pl.when(j // per != tp)
        def _():
            block_copy(j, tp).wait_send()

    @pl.loop(0, row_pieces)
    def _(p):
        for kind in range(7):
            row_copy(kind, odd, tp, p, tp=near).wait_send()

    @pl.loop(0, count)
    def _(i):
        for kind in range(5):
            sum_copy(kind, i).wait_send()

    @pl.loop(started - 2, up_ticks)
    def _(n):
        up_sent(n)

    @pl.loop(0, line - 1)
    def _(t):
        for w in range(2):

            @pl.when(sends(w, t))
            def _():
                for m in range(down_pieces):
                    down_hop(w, t, m).wait_send()


FIRST_TICKS = 4
NEXT_TICKS = 2
UPS_TICKS = 1
UP_PIECES = 8
DOWN_PIECES = 4
PAD_ROWS = 16


def one_kernel_fits(rows, gate_w, down_w):
    count = lax.axis_size("sp")
    return (
        lax.axis_size("tp") == 4
        and count >= 4
        and count % 2 == 0
        and 2 * gate_w.shape[0] % (16 * UP_PIECES) == 0
        and gate_w.shape[1] % 256 == 128
        and down_w.shape[0] % (16 * DOWN_PIECES) == 0
        and down_w.shape[1] % 256 == 0
        and rows % (2 * BLOCK) == 0
        and 4 * rows >= 6 * BLOCK
    )


def layer(q, k, v, gates, input_log, forget_log, gain, wo, residual, norm_gain, gate_w, value_w, down_w, gate_taps, value_taps):
    count = lax.axis_size("sp")
    line = count // 2
    heads = input_log.shape[1]
    tokens = q.shape[0]
    key_width = q.shape[1] // heads
    value_width = v.shape[1] // heads
    span = key_width + STATE_PAD
    model = wo.shape[1]
    rows = residual.shape[0]
    lane = 128
    half_width = gate_w.shape[1] // 2
    tiles = half_width // lane
    wide = down_w.shape[1]
    row_pieces = 4
    blocks = tokens // BLOCK
    vmem = pl.BlockSpec(memory_space=pltpu.VMEM)
    hbm = pl.BlockSpec(memory_space=pl.ANY)
    low, full = jnp.bfloat16, jnp.float32
    dma = pltpu.SemaphoreType.DMA
    return pl.pallas_call(
        functools.partial(layer_kernel, count, heads, UP_PIECES, DOWN_PIECES),
        out_shape=jax.ShapeDtypeStruct(residual.shape, low),
        in_specs=[vmem] * 6 + [hbm] * 9,
        out_specs=hbm,
        scratch_shapes=[
            pltpu.VMEM(q.shape, low),
            pltpu.VMEM(k.shape, low),
            pltpu.VMEM(v.shape, low),
            pltpu.VMEM(gates.shape, low),
            pltpu.VMEM(residual.shape, low),
            pltpu.VMEM((blocks, 8, BLOCK), full),
            pltpu.VMEM((tokens, BLOCK), full),
            pltpu.VMEM((heads * span, value_width), low),
            pltpu.VMEM((2, heads * span, value_width), low),
            pltpu.VMEM((heads, key_width, value_width), full),
            pltpu.VMEM((heads, 8, key_width), full),
            pltpu.VMEM((heads, 8, 128), full),
            pltpu.VMEM((heads, key_width, value_width), full),
            pltpu.VMEM((heads, 8, key_width), full),
            pltpu.VMEM((2, heads, 8, 128), full),
            pltpu.VMEM((heads * span, value_width), low),
            pltpu.VMEM((tokens, v.shape[1]), low),
            pltpu.VMEM((4, rows, v.shape[1]), low),
            pltpu.VMEM((model, model), low),
            pltpu.VMEM((2, gate_w.shape[0], lane), low),
            pltpu.VMEM((gate_w.shape[0], 2 * half_width), low),
            pltpu.VMEM((half_width, wide), low),
            pltpu.VMEM((model, 2 * half_width), low),
            pltpu.VMEM((count, half_width, wide), low),
            pltpu.VMEM((rows, model), full),
            pltpu.VMEM((rows, model), low),
            pltpu.VMEM((PAD_ROWS + 2 * tokens, model), low),
            pltpu.VMEM((PAD_ROWS + tokens // 2, 2 * lane), full),
            pltpu.VMEM((PAD_ROWS + tokens // 2, 2 * lane), full),
            pltpu.VMEM((2 * tokens, half_width), low),
            pltpu.VMEM((count, 4, rows, wide), low),
            pltpu.VMEM((count, 4, rows, wide), low),
            pltpu.VMEM((count, 2, 2, rows, wide // 2), low),
            pltpu.VMEM((count, 2, 2, rows, wide // 2), low),
            pltpu.VMEM((count, 2, rows, wide // 2), low),
            pltpu.VMEM((count, 2, rows, wide // 2), low),
            pltpu.VMEM((count, 2, 2, rows, wide // 2), full),
            pltpu.VMEM((4, rows, wide), full),
            dma((4 * tiles + 12,)),
            dma((2, 5, 4)),
            dma((2, 3)),
            dma((2,)),
            dma((2,)),
            dma((2, line - 1, UP_PIECES)),
            dma((2, line - 1, UP_PIECES)),
            dma((2, line - 1, DOWN_PIECES)),
            dma((2, line - 1, DOWN_PIECES)),
            dma((blocks,)),
            dma((4, rows // BLOCK)),
            dma((7, row_pieces)),
            dma((7, row_pieces)),
            dma((5, count)),
            dma((5, count)),
            dma((2,)),
            dma((count,)),
        ],
        compiler_params=pltpu.CompilerParams(
            collective_id=0, has_side_effects=True, vmem_limit_bytes=63 * 1024 * 1024
        ),
        cost_estimate=pl.CostEstimate(
            flops=30_000_000_000, bytes_accessed=8 * v.size, transcendentals=0
        ),
    )(
        input_log.T,
        forget_log.T,
        gain,
        norm_gain[None, :],
        gate_taps,
        value_taps,
        q,
        k,
        v,
        gates,
        residual,
        wo,
        gate_w,
        value_w,
        down_w,
    )


def local(
    residual_entry_input,
    query_matrix_rows,
    key_matrix_rows,
    value_matrix_rows,
    output_gate_logits,
    input_gate_logits,
    forget_gate_logits,
    forget_decay_offset,
    head_norm_gain,
    cell_output_weight,
    feedforward_norm_gain,
    gate_up_weight,
    value_up_weight,
    gate_filter_taps,
    value_filter_taps,
    down_projection_weight,
):
    input_log, forget_log = gate_log_values(
        input_gate_logits, forget_gate_logits, forget_decay_offset
    )
    if one_kernel_fits(residual_entry_input.shape[0], gate_up_weight, down_projection_weight):
        return layer(
            query_matrix_rows,
            key_matrix_rows,
            value_matrix_rows,
            output_gate_logits,
            input_log,
            forget_log,
            head_norm_gain,
            cell_output_weight,
            residual_entry_input,
            feedforward_norm_gain,
            gate_up_weight,
            value_up_weight,
            down_projection_weight,
            gate_filter_taps,
            value_filter_taps,
        )
    whole_gate = lax.all_gather(gate_up_weight, "sp", axis=0, tiled=True)
    whole_down = lax.all_gather(down_projection_weight, "sp", axis=1, tiled=True)
    gated_rows = cell(
        query_matrix_rows,
        key_matrix_rows,
        value_matrix_rows,
        output_gate_logits,
        input_log,
        forget_log,
        head_norm_gain,
    )
    mixed_rows = product_rows(gated_rows, cell_output_weight, 2)
    stream_wide = residual_entry_input.astype(jnp.float32) + mixed_rows
    stream = stream_wide.astype(jnp.bfloat16)
    stream_wide = lax.optimization_barrier(stream).astype(jnp.float32)
    normed_rows = (
        stream_wide
        * lax.rsqrt(jnp.mean(stream_wide * stream_wide, axis=-1, keepdims=True) + eps)
        * feedforward_norm_gain[None, :]
    ).astype(jnp.bfloat16)
    group_rows = gather_rows(normed_rows)
    group_rows, value_shard = lax.optimization_barrier((group_rows, value_up_weight))
    whole_value = walk_gather(value_shard, 2)
    earlier_rows = shifted(group_rows[-2:], "sp", 1)
    window = jnp.concatenate([earlier_rows, group_rows], axis=0)
    up_gate = jnp.dot(
        window,
        whole_gate,
        preferred_element_type=jnp.float32,
    )
    up_value = jnp.dot(
        window,
        whole_value,
        preferred_element_type=jnp.float32,
    )
    conv_g = (
        gate_filter_taps[0][None, :] * up_gate[:-2]
        + gate_filter_taps[1][None, :] * up_gate[1:-1]
        + gate_filter_taps[2][None, :] * up_gate[2:]
    )
    conv_v = (
        value_filter_taps[0][None, :] * up_value[:-2]
        + value_filter_taps[1][None, :] * up_value[1:-1]
        + value_filter_taps[2][None, :] * up_value[2:]
    )
    hidden = (jax.nn.silu(conv_g) * conv_v).astype(jnp.bfloat16)
    ffn_rows = product_rows(hidden, whole_down, 3)
    return (stream_wide + ffn_rows).astype(jnp.bfloat16)


def solution(mesh):
    in_specs = (
        P(("sp", "tp"), None),
        P("sp", "tp"),
        P("sp", "tp"),
        P("sp", "tp"),
        P("sp", "tp"),
        P("sp", "tp"),
        P("sp", "tp"),
        P("sp", "tp"),
        P("tp", None),
        P("tp", None),
        P(),
        P("sp", "tp"),
        P("sp", "tp"),
        P(None, "tp"),
        P(None, "tp"),
        P("tp", "sp"),
    )
    out_specs = P(("sp", "tp"), None)
    return jax.shard_map(local, mesh=mesh, in_specs=in_specs, out_specs=out_specs, check_vma=False)
```
